32 devices in a mesh: grp: 2 (over y), sp: 4 (over z), tp: 4 (over x, core).
Axes of the slice: x: 2, y: 2, z: 4, core: 2. Of those that a mesh axis runs over, the one named last changes fastest.
Arguments:
- tokens: bfloat16 [2048, 4096], P(('grp', 'sp'), 'tp'), parts along dimension 0, may hold values from -45 to 45
- norm_gain: float32 [2, 4096], replicated, may hold values from 0.1 to 1.9
- value_weight: bfloat16 [2, 4096, 1024], P(None, 'sp', 'tp'), may hold values from -0.09375 to 0.09375
- gate_weight: bfloat16 [2, 4096, 1024], P(None, 'sp', 'tp'), may hold values from -0.09375 to 0.09375
- conv_taps: float32 [2, 31, 1024], P(None, None, 'tp'), may hold values from -4 to 4
- channel_gain: float32 [2, 1024], P(None, 'tp'), may hold values from 0.1 to 1.9
- out_weight: bfloat16 [2, 1024, 4096], P(None, 'sp', 'tp'), may hold values from -0.375 to 0.375
- final_gain: float32 [4096], P('tp'), may hold values from 0.1 to 1.9
Outputs:
- result: bfloat16 [2048, 4096], P(('grp', 'sp'), 'tp'), parts along dimension 0
The draws below stay inside these ranges and needn't reach their ends.
There are 2 independent parts, one for each index of `grp`. The reference program is written for one: setup_inputs(seed, part) draws one part's arguments, and reference() takes and returns one part's arrays. A program takes and returns all parts, laid end to end along the dimension named above; an argument that names none is the same for every part. Nothing has to cross between parts.
All inputs are finite; a program needn't handle non-finite values.
Results may differ from the reference program's by a relative error of at most 0.012.
Values may be sent and summed in bfloat16 or wider, within the bound.
A program may use at most 128 MiB of HBM per device.

```python
import jax
import jax.numpy as jnp
from jax import lax

D = 4096
C = 1024
KERNEL = 31
LAYERS = 2
TOKENS = 1024


def draw_tokens(key, part):
    key_base, key_cols, key_rows = jax.random.split(key, 3)
    cols = jnp.arange(D, dtype=jnp.float32) / D
    col_scale = jnp.exp(jnp.log(3.0) * cols) * jnp.exp(jax.random.uniform(key_cols, (D,), jnp.float32, -0.35, 0.35))
    row_scale = jnp.exp(jax.random.uniform(key_rows, (TOKENS, 1), jnp.float32, -0.69, 0.69))
    base = jnp.clip(jax.random.normal(key_base, (TOKENS, D), jnp.float32), -4.0, 4.0)
    return (base * col_scale[None, :] * row_scale).astype(jnp.bfloat16)


def draw_conv_taps(key, part):
    key_base, key_cols = jax.random.split(key, 2)
    cols = jnp.arange(C, dtype=jnp.float32) / C
    col_scale = jnp.exp(jnp.log(3.0) * cols) * jnp.exp(jax.random.uniform(key_cols, (LAYERS, 1, C), jnp.float32, -0.5, 0.5))
    base = jnp.clip(jax.random.normal(key_base, (LAYERS, KERNEL, C), jnp.float32), -4.0, 4.0)
    return base * col_scale * KERNEL ** (-0.5)


def levels(key, shape, cuts, low, top_value):
    factor_of, own = 1.0, jax.random.fold_in(key, 6)
    for position, parts in cuts:
        steps = jnp.exp(jax.random.uniform(jax.random.fold_in(own, position), (parts,), jnp.float32, low / len(cuts), top_value / len(cuts)))
        factor_of = factor_of * jnp.repeat(steps, shape[position] // parts).reshape([-1 if axis == position else 1 for axis in range(len(shape))])
    return factor_of


def noise(own_key, dims, scale, most, pieces=(), held_as=jnp.bfloat16):
    entries = scale * jax.random.normal(own_key, dims, jnp.float32)
    if pieces:
        entries = entries * levels(own_key, dims, pieces, -0.22, 0.18)
    return jnp.clip(entries, -most, most).astype(held_as)


def setup_inputs(seed: int = 0, part: int = 0) -> dict:
    keys = jax.random.split(jax.random.key(seed), 9)
    part_keys = jax.random.split(jax.random.fold_in(keys[8], part), 9)
    return {
        "tokens": draw_tokens(jax.random.fold_in(jax.random.fold_in(keys[8], part), 71), part),
        "norm_gain": jnp.clip(1.0 + 0.18 * jax.random.normal(keys[1], (LAYERS, D), jnp.float32), 0.1, 1.9),
        "value_weight": noise(keys[2], (LAYERS, D, C), D ** -0.5, 0.09375, ((1, 4), (2, 4))),
        "gate_weight": noise(keys[3], (LAYERS, D, C), D ** -0.5, 0.09375, ((1, 4), (2, 4))),
        "conv_taps": draw_conv_taps(jax.random.fold_in(keys[8], 71), part),
        "channel_gain": jnp.clip(1.0 + 0.18 * jax.random.normal(keys[5], (LAYERS, C), jnp.float32), 0.1, 1.9),
        "out_weight": noise(keys[6], (LAYERS, C, D), (C // 4) ** -0.5, 0.375, ((1, 4), (2, 4))),
        "final_gain": jnp.clip(1.0 + 0.18 * jax.random.normal(keys[7], (D,), jnp.float32), 0.1, 1.9),
    }


def depthwise(glu, taps):
    reach = taps.shape[0] // 2
    padded = jnp.pad(glu.astype(jnp.float32), ((reach, reach), (0, 0)))
    length = glu.shape[0]
    total = jnp.zeros(glu.shape, jnp.float32)
    for tap in range(taps.shape[0]):
        total = total + taps[tap][None, :] * padded[tap:tap + length]
    return total

def reference(tokens, norm_gain, value_weight, gate_weight, conv_taps, channel_gain, out_weight, final_gain):
    x_state = tokens
    for layer in range(LAYERS):
        xf = x_state.astype(jnp.float32)
        scale = lax.rsqrt(lax.optimization_barrier(jnp.mean(xf * xf, axis=1, keepdims=True)) + 1e-06)
        normed = (xf * scale * norm_gain[layer][None, :]).astype(jnp.bfloat16)
        value = jnp.dot(normed, value_weight[layer], preferred_element_type=jnp.float32)
        gate = jnp.dot(normed, gate_weight[layer], preferred_element_type=jnp.float32)
        glu = (value * jax.nn.sigmoid(gate)).astype(jnp.bfloat16)
        conv = depthwise(glu, conv_taps[layer])
        center = lax.optimization_barrier(jnp.mean(conv, axis=1, keepdims=True))
        shifted = conv - center
        spread = lax.optimization_barrier(jnp.mean(shifted * shifted, axis=1, keepdims=True))
        act = jax.nn.silu(shifted * lax.rsqrt(spread + 1e-05) * channel_gain[layer][None, :]).astype(jnp.bfloat16)
        branch = jnp.dot(act, out_weight[layer], preferred_element_type=jnp.float32)
        x_state = (xf + branch).astype(jnp.bfloat16)
    xf = x_state.astype(jnp.float32)
    scale = lax.rsqrt(lax.optimization_barrier(jnp.mean(xf * xf, axis=1, keepdims=True)) + 1e-06)
    return (xf * scale * final_gain[None, :]).astype(jnp.bfloat16)
```

```python
import functools

import jax
import jax.numpy as jnp
from jax import lax
from jax.experimental import pallas as pl
from jax.experimental.pallas import tpu as pltpu
from jax.sharding import PartitionSpec as P

MESH = pl.DeviceIdType.MESH
Q = 2
PAD = 16


def kernel(
    G, n, T, L,
    tokens, gain, value_w, gate_w, taps, cgain, out_w, fgain,
    result,
    wvg, wo, xg, xn, glu_out, acc, pad, padf, conv, stat, actg, x_state,
    local_sem, z_recv, right_send, left_send, y_send, y_recv,
    x_send, x_recv, a_send, a_recv, s_send, s_recv, h_send, h_recv, f_send, f_recv,
):
    g, s, t = lax.axis_index("grp"), lax.axis_index("sp"), lax.axis_index("tp")
    rows, width = tokens.shape
    depth, chans = value_w.shape[1:]
    out_rows = out_w.shape[1]
    half = chans // G
    out_half = width // G
    reach = taps.shape[1] // 2
    n_taps = taps.shape[1]
    D = width * T
    C = chans * T
    chunk = depth // Q
    pieces = Q + 1
    f32, bf16 = jnp.float32, jnp.bfloat16
    helped = n >= 4
    last = n - 1
    is_end = (s == 0) | (s == last)
    helper = (s == 1) | (s == last - 1)
    end = jnp.where(s == 1, 0, last)
    inward = jnp.where(s == 0, 1, last - 1)

    def ends_out(p):
        return helped and p < Q

    def to_right_ok(p):
        return s < last - 1 if ends_out(p) else s < last

    def to_left_ok(p):
        return s > 1 if ends_out(p) else s > 0

    def takes(p):
        return jnp.logical_not(is_end) if ends_out(p) else s >= 0

    def by_grp(p, j):
        ok = takes(p) & (j != s)
        if helped and p == 0:
            ok = ok & jnp.logical_not((s == 1) & (j == 0)) & jnp.logical_not((s == last - 1) & (j == last))
        return ok

    def piece(p, h, j):
        layer, q = p // pieces, p % pieces
        if q < Q:
            start = pl.multiple_of(j * depth + q * chunk, chunk)
            return wvg.at[layer, h, pl.ds(start, chunk), :]
        return wo.at[layer, h, pl.ds(pl.multiple_of(j * out_rows, out_rows), out_rows), :]

    locals_ = [pltpu.make_async_copy(tokens, xg.at[0, t], local_sem.at[0])]
    own_rows = pl.ds(pl.multiple_of(s * depth, depth), depth)
    own_out = pl.ds(pl.multiple_of(s * out_rows, out_rows), out_rows)
    count = 1
    per_layer = []
    for layer in range(L):
        group = []
        for h in range(G):
            for k, w in enumerate((value_w, gate_w)):
                group.append(pltpu.make_async_copy(
                    w.at[layer, :, pl.ds(h * half, half)],
                    wvg.at[layer, h, own_rows, pl.ds(k * half, half)],
                    local_sem.at[count]))
                count += 1
            group.append(pltpu.make_async_copy(
                out_w.at[layer, :, pl.ds(h * out_half, out_half)],
                wo.at[layer, h, own_out, :], local_sem.at[count]))
            count += 1
        per_layer.append(group)
    for c in locals_ + sum(per_layer, []):
        c.start()

    barrier = pltpu.get_barrier_semaphore()
    for d in range(1, T):
        pl.semaphore_signal(barrier, inc=1, device_id={"tp": lax.rem(t + d, T)}, device_id_type=MESH)
    for d in range(1, G):
        pl.semaphore_signal(barrier, inc=1, device_id={"grp": lax.rem(g + d, G)}, device_id_type=MESH)

    @pl.when(s > 0)
    def _():
        pl.semaphore_signal(barrier, inc=1, device_id={"sp": s - 1}, device_id_type=MESH)

    @pl.when(s < n - 1)
    def _():
        pl.semaphore_signal(barrier, inc=1, device_id={"sp": s + 1}, device_id_type=MESH)

    sides = jnp.where(s > 0, 1, 0) + jnp.where(s < n - 1, 1, 0)
    pl.semaphore_wait(barrier, (T - 1) + (G - 1) + sides)

    def right(p, j):
        r = piece(p, g, j)
        return pltpu.make_async_remote_copy(
            src_ref=r, dst_ref=r, send_sem=right_send.at[p, j], recv_sem=z_recv.at[p, j],
            device_id={"sp": s + 1}, device_id_type=MESH)

    def left(p, j):
        r = piece(p, g, j)
        return pltpu.make_async_remote_copy(
            src_ref=r, dst_ref=r, send_sem=left_send.at[p, j], recv_sem=z_recv.at[p, j],
            device_id={"sp": s - 1}, device_id_type=MESH)

    def across(p, j, d, h):
        r = piece(p, h, j)
        return pltpu.make_async_remote_copy(
            src_ref=r, dst_ref=r, send_sem=y_send.at[p, j, d - 1], recv_sem=y_recv.at[p, j, d - 1],
            device_id={"grp": lax.rem(g + d, G)}, device_id_type=MESH)

    batches = []
    for layer in range(L):
        base = layer * pieces
        batches += [list(range(base, base + Q)), [base + Q]]

    def own_right(ps):
        for p in ps:
            right(p, s).start()

    def own_left(ps):
        for p in ps:
            left(p, s).start()

    def end_rows(target):
        return pltpu.make_async_remote_copy(
            src_ref=xg.at[0, t], dst_ref=xg.at[L, t], send_sem=f_send.at[0], recv_sem=f_recv.at[0],
            device_id={"sp": target}, device_id_type=MESH)

    def end_piece(d, h, j, target):
        r = piece(0, h, j)
        return pltpu.make_async_remote_copy(
            src_ref=r, dst_ref=r, send_sem=f_send.at[d], recv_sem=f_recv.at[d],
            device_id={"sp": target}, device_id_type=MESH)

    def end_glu(target):
        return pltpu.make_async_remote_copy(
            src_ref=glu_out, dst_ref=pad.at[0, pl.ds(PAD, rows), :],
            send_sem=f_send.at[G], recv_sem=f_recv.at[G],
            device_id={"sp": target}, device_id_type=MESH)

    def relay(b, low, high):
        low, high = min(low, n - 1), min(high, n - 1)
        following = batches[b + 1] if b + 1 < len(batches) else []

        def step(k, carry):
            for p in batches[b]:
                from_left, from_right = s - 1 - k, s + 1 + k

                @pl.when((from_left >= 0) & takes(p))
                def _():
                    j = jnp.maximum(from_left, 0)
                    right(p, j).wait_recv()

                    @pl.when(to_right_ok(p))
                    def _():
                        right(p, j).start()

                    @pl.when(by_grp(p, j))
                    def _():
                        for d in range(1, G):
                            across(p, j, d, g).start()

                @pl.when((from_right < n) & takes(p))
                def _():
                    j = jnp.minimum(from_right, n - 1)
                    left(p, j).wait_recv()

                    @pl.when(to_left_ok(p))
                    def _():
                        left(p, j).start()

                    @pl.when(by_grp(p, j))
                    def _():
                        for d in range(1, G):
                            across(p, j, d, g).start()

            @pl.when((k == s - 1) & (s < (last - 1 if helped and b < 2 else last)))
            def _():
                own_right(following)

            @pl.when((k == n - 2 - s) & (s > (1 if helped and b < 2 else 0)))
            def _():
                own_left(following)

            return carry

        if high > low:
            lax.fori_loop(low, high, step, 0)

    def wait_across(b):
        for p in batches[b]:
            def step(j, carry):
                @pl.when(by_grp(p, j))
                def _():
                    for d in range(1, G):
                        across(p, j, d, lax.rem(g + G - d, G)).wait_recv()
                return carry
            lax.fori_loop(0, n, step, 0)

    def spread(buf, layer, send, recv):
        def copy(bit, m):
            block = buf.at[layer, t ^ m]
            return pltpu.make_async_remote_copy(
                src_ref=block, dst_ref=block, send_sem=send.at[layer, bit + m], recv_sem=recv.at[layer, bit + m],
                device_id={"tp": t ^ bit}, device_id_type=MESH)

        def arrival(bit, m):
            block = buf.at[layer, t ^ bit ^ m]
            return pltpu.make_async_remote_copy(
                src_ref=block, dst_ref=block, send_sem=send.at[layer, bit + m], recv_sem=recv.at[layer, bit + m],
                device_id={"tp": t ^ bit}, device_id_type=MESH)

        bits = []
        bit = T // 2
        while bit >= 1:
            bits.append(bit)
            bit //= 2

        def begin():
            for bit in bits:
                copy(bit, 0).start()

        def finish():
            have, sent = [0], []
            for i, bit in enumerate(bits):
                for m in have:
                    arrival(bit, m).wait_recv()
                    sent.append((bit, m))
                    for lower in bits[i + 1:]:
                        copy(lower, m ^ bit).start()
                have = have + [m ^ bit for m in have]
            return lambda: [copy(bit, m).wait_send() for bit, m in sent]

        return begin, finish

    def exchange(index, columns):
        lane = lax.broadcasted_iota(jnp.int32, (rows, 128), 1)
        tile = jnp.zeros((rows, 128), f32)
        for i, column in enumerate(columns):
            tile = jnp.where(lane == i, column, tile)
        stat[index, 0] = tile.T[:8, :]

        def copy(d):
            return pltpu.make_async_remote_copy(
                src_ref=stat.at[index, 0], dst_ref=stat.at[index, d],
                send_sem=s_send.at[index, d - 1], recv_sem=s_recv.at[index, d - 1],
                device_id={"tp": lax.rem(t + d, T)}, device_id_type=MESH)

        for d in range(1, T):
            copy(d).start()

        def total():
            for d in range(1, T):
                copy(d).wait_recv()
            sums = stat[index, 0]
            for d in range(1, T):
                sums = sums + stat[index, d]
            wide = jnp.concatenate([sums, jnp.zeros((120, rows), f32)], axis=0).T
            for d in range(1, T):
                copy(d).wait_send()
            return [wide[:, i:i + 1] for i in range(len(columns))]

        return total

    def normalize(layer, held, into):
        def squares(j, total):
            part = xg[held, j].astype(f32)
            return total + jnp.sum(part * part, axis=1, keepdims=True)
        mean = lax.fori_loop(0, T, squares, jnp.zeros((rows, 1), f32)) / D
        scale = lax.rsqrt(mean + 1e-06)

        def body(j, carry):
            xn[into, j] = (xg[held, j].astype(f32) * scale * gain[layer * T + j][None, :]).astype(bf16)
            return carry
        lax.fori_loop(0, T, body, 0)

    def project(layer, held, put):
        for h in range(G):
            def body(j, carry):
                block = wvg[layer, h, pl.ds(pl.multiple_of(j * width, width), width), :]
                part = jnp.dot(xn[held, j], block, preferred_element_type=f32)

                @pl.when(j == 0)
                def _():
                    acc[...] = part

                @pl.when(j > 0)
                def _():
                    acc[...] += part
                return carry
            lax.fori_loop(0, T, body, 0)
            glu = acc[:, :half] * jax.nn.sigmoid(acc[:, half:])
            put(h, glu.astype(bf16))

    for c in locals_:
        c.wait()
    spreads = [spread(xg, layer, x_send, x_recv) for layer in range(L)]
    spreads[0][0]()
    for c in sum(per_layer, []):
        c.wait()

    @pl.when(to_right_ok(0))
    def _():
        own_right(batches[0])

    @pl.when(to_left_ok(0))
    def _():
        own_left(batches[0])

    if helped:
        @pl.when(is_end)
        def _():
            end_rows(inward).start()
            for d in range(1, G):
                end_piece(d, lax.rem(g + d, G), s, inward).start()

        @pl.when(s == last - 1)
        def _():
            own_right(batches[1])
            if L > 1:
                own_right(batches[2])

        @pl.when(s == 1)
        def _():
            own_left(batches[1])
            if L > 1:
                own_left(batches[2])

    @pl.when((s == 0) & (s < n - 1))
    def _():
        for b in batches[1:]:
            own_right(b)

    @pl.when((s == n - 1) & (s > 0))
    def _():
        for b in batches[1:]:
            own_left(b)

    x_state[...] = tokens_f32(tokens, xg, t)
    drains = []

    for layer in range(L):
        first, second = 2 * layer, 2 * layer + 1
        if layer == 0:
            relay(first, 0, 1)
        else:
            relay(first, 1, 2)
        drains.append(spreads[layer][1]())
        if helped and layer == 0:
            @pl.when(jnp.logical_not(is_end))
            def _():
                normalize(layer, layer, 0)
        else:
            normalize(layer, layer, 0)
        relay(first, 1 if layer == 0 else 2, n)
        begin, finish = spread(xg, L, x_send, x_recv)
        if helped and layer == 0:
            @pl.when(helper)
            def _():
                end_rows(end).wait_recv()
                begin()

        relay(second, 0, 1)

        def put(h, value):
            pad[layer, PAD:PAD + rows, h * half:(h + 1) * half] = value

        def put_out(h, value):
            glu_out[:, h * half:(h + 1) * half] = value

        if helped and layer == 0:
            @pl.when(helper)
            def _():
                drain = finish()
                normalize(0, L, 1)
                for d in range(1, G):
                    end_piece(d, lax.rem(g + d, G), end, end).wait_recv()
                drain()

            wait_across(first)

            @pl.when(helper)
            def _():
                project(0, 1, put_out)
                end_glu(end).start()

            @pl.when(jnp.logical_not(is_end))
            def _():
                project(0, 0, put)

            @pl.when(helper)
            def _():
                end_glu(end).wait_send()

            @pl.when(is_end)
            def _():
                end_rows(inward).wait_send()
                for d in range(1, G):
                    end_piece(d, lax.rem(g + d, G), s, inward).wait_send()
                end_glu(inward).wait_recv()
        else:
            wait_across(first)
            project(layer, 0, put)

        def to_right():
            return pltpu.make_async_remote_copy(
                src_ref=pad.at[layer, pl.ds(rows, PAD), :], dst_ref=pad.at[layer, pl.ds(0, PAD), :],
                send_sem=h_send.at[layer, 0], recv_sem=h_recv.at[layer, 0],
                device_id={"sp": s + 1}, device_id_type=MESH)

        def to_left():
            return pltpu.make_async_remote_copy(
                src_ref=pad.at[layer, pl.ds(PAD, PAD), :], dst_ref=pad.at[layer, pl.ds(PAD + rows, PAD), :],
                send_sem=h_send.at[layer, 1], recv_sem=h_recv.at[layer, 1],
                device_id={"sp": s - 1}, device_id_type=MESH)

        @pl.when(s < n - 1)
        def _():
            to_right().start()

        @pl.when(s > 0)
        def _():
            to_left().start()

        @pl.when(s == 0)
        def _():
            pad[layer, 0:PAD, :] = jnp.zeros((PAD, chans), bf16)

        @pl.when(s == n - 1)
        def _():
            pad[layer, PAD + rows:, :] = jnp.zeros((PAD, chans), bf16)

        relay(second, 1, 2)

        @pl.when(s > 0)
        def _():
            to_right().wait_recv()

        @pl.when(s < n - 1)
        def _():
            to_left().wait_recv()

        padf[...] = pad[layer].astype(f32)
        block = 64
        sums, squares = [], []
        for r in range(0, rows, block):
            total = jnp.zeros((block, chans), f32)
            for k in range(n_taps):
                start = r + PAD - reach + k
                total = total + taps[layer, k][None, :] * padf[start:start + block, :]
            conv[r:r + block, :] = total
            sums.append(jnp.sum(total, axis=1, keepdims=True))
            squares.append(jnp.sum(total * total, axis=1, keepdims=True))
        totals = exchange(layer, [jnp.concatenate(sums, 0), jnp.concatenate(squares, 0)])
        relay(second, 2, n)
        if layer + 1 < L:
            relay(second + 1, 0, 1)
        total, square = totals()
        center = total / C
        spread_ = square / C - center * center
        normal = (conv[...] - center) * lax.rsqrt(spread_ + 1e-05)
        actg[layer, t] = jax.nn.silu(normal * cgain[layer][None, :]).astype(bf16)
        act_begin, act_finish = spread(actg, layer, a_send, a_recv)
        act_begin()
        drains.append(act_finish())
        wait_across(second)
        for h in range(G):
            part = None
            for j in range(T):
                term = jnp.dot(actg[layer, j], wo[layer, h, j * chans:(j + 1) * chans, :], preferred_element_type=f32)
                part = term if part is None else part + term
            cols = slice(h * out_half, (h + 1) * out_half)
            x_state[:, cols] = (x_state[:, cols] + part).astype(bf16).astype(f32)
        if layer + 1 < L:
            xg[layer + 1, t] = x_state[...].astype(bf16)
            spreads[layer + 1][0]()

        @pl.when(s < n - 1)
        def _():
            to_right().wait_send()

        @pl.when(s > 0)
        def _():
            to_left().wait_send()

    xf = x_state[...]
    totals = exchange(L, [jnp.sum(xf * xf, axis=1, keepdims=True)])

    for drain in drains:
        drain()

    def drain_step(j, carry):
        for p in range(L * pieces):
            came = (j == s) | takes(p)

            @pl.when((j <= s) & to_right_ok(p) & came)
            def _():
                right(p, j).wait_send()

            @pl.when((j >= s) & to_left_ok(p) & came)
            def _():
                left(p, j).wait_send()

            @pl.when(by_grp(p, j))
            def _():
                for d in range(1, G):
                    across(p, j, d, g).wait_send()
        return carry
    lax.fori_loop(0, n, drain_step, 0)

    (total,) = totals()
    scale = lax.rsqrt(total / D + 1e-06)
    result[...] = (x_state[...] * scale * fgain[...]).astype(bf16)


QC = 4
RC = 2


def quad_kernel(
    G, n, T, L,
    tokens, gain, value_w, gate_w, taps, cgain, out_w, fgain,
    result,
    wvg, wo, xg, xn, glu_out, acc, pad, padf, conv, stat, actg, x_state,
    local_sem, recv_z, recv_o, send_in, send_out, send_y, send_un,
    x_send, x_recv, e_send, e_recv, a_send, a_recv, s_send, s_recv, h_send, h_recv, f_send, f_recv,
):
    g, s, t = lax.axis_index("grp"), lax.axis_index("sp"), lax.axis_index("tp")
    rows, width = tokens.shape
    depth, chans = value_w.shape[1:]
    out_rows = out_w.shape[1]
    half = chans // G
    out_half = width // G
    reach = taps.shape[1] // 2
    n_taps = taps.shape[1]
    D = width * T
    C = chans * T
    pieces = QC + RC
    size = {"vg": depth // QC, "wo": out_rows // RC}
    count = {"vg": QC, "wo": RC}
    shared_from = QC // 2
    f32, bf16 = jnp.float32, jnp.bfloat16
    last = n - 1
    low = s < n // 2
    is_end = (s == 0) | (s == last)
    is_mid = jnp.logical_not(is_end)
    inner = jnp.where(low, s + 1, s - 1)
    outer = jnp.where(low, s - 1, s + 1)
    edge, mine, near, far = (jnp.where(low, a, last - a) for a in (0, 1, n - 2, n - 1))
    other = lax.rem(g + 1, G)
    x_chunks = QC
    x_rows = rows // x_chunks
    first_vg, first_wo, second_vg, second_wo = (0, "vg"), (0, "wo"), (1, "vg"), (1, "wo")
    after = (first_wo, second_vg, second_wo)

    def index(stage, q):
        layer, kind = stage
        return layer * pieces + (0 if kind == "vg" else QC) + q

    def piece(stage, q, h, j):
        layer, kind = stage
        step = size[kind]
        per = depth if kind == "vg" else out_rows
        ref = wvg if kind == "vg" else wo
        return ref.at[layer, h, pl.ds(pl.multiple_of(j * per + q * step, step), step), :]

    token_copy = pltpu.make_async_copy(tokens, xg.at[0, t], local_sem.at[0])
    own_rows = pl.ds(pl.multiple_of(s * depth, depth), depth)
    own_out = pl.ds(pl.multiple_of(s * out_rows, out_rows), out_rows)
    staged = {}
    slot = 1
    for layer in range(L):
        staged[layer, "vg"], staged[layer, "wo"] = [], []
        for h in range(G):
            for k, w in enumerate((value_w, gate_w)):
                staged[layer, "vg"].append(pltpu.make_async_copy(
                    w.at[layer, :, pl.ds(h * half, half)],
                    wvg.at[layer, h, own_rows, pl.ds(k * half, half)],
                    local_sem.at[slot]))
                slot += 1
        for h in range(G):
            staged[layer, "wo"].append(pltpu.make_async_copy(
                out_w.at[layer, :, pl.ds(h * out_half, out_half)],
                wo.at[layer, h, own_out, :], local_sem.at[slot]))
            slot += 1
    for c in staged[first_vg]:
        c.start()
    token_copy.start()
    for stage in after:
        for c in staged[stage]:
            c.start()

    barrier = pltpu.get_barrier_semaphore()
    for d in range(1, T):
        pl.semaphore_signal(barrier, inc=1, device_id={"tp": lax.rem(t + d, T)}, device_id_type=MESH)
    pl.semaphore_signal(barrier, inc=1, device_id={"grp": other}, device_id_type=MESH)

    @pl.when(s > 0)
    def _():
        pl.semaphore_signal(barrier, inc=1, device_id={"sp": s - 1}, device_id_type=MESH)

    @pl.when(s < last)
    def _():
        pl.semaphore_signal(barrier, inc=1, device_id={"sp": s + 1}, device_id_type=MESH)

    sides = jnp.where(s > 0, 1, 0) + jnp.where(s < last, 1, 0)
    pl.semaphore_wait(barrier, (T - 1) + (G - 1) + sides)

    def along(stage, q, j, target, send):
        r, p = piece(stage, q, g, j), index(stage, q)
        return pltpu.make_async_remote_copy(
            src_ref=r, dst_ref=r, send_sem=send.at[p, j], recv_sem=recv_z.at[p, j],
            device_id={"sp": target}, device_id_type=MESH)

    def inward(stage, q, j):
        return along(stage, q, j, inner, send_in)

    def outward(stage, q, j):
        return along(stage, q, j, outer, send_out)

    def across(stage, q, j, h):
        r, p = piece(stage, q, h, j), index(stage, q)
        return pltpu.make_async_remote_copy(
            src_ref=r, dst_ref=r, send_sem=send_y.at[p, j], recv_sem=recv_o.at[p, j],
            device_id={"grp": other}, device_id_type=MESH)

    def direct(stage, q):
        r, p = piece(stage, q, other, edge), index(stage, q)
        return pltpu.make_async_remote_copy(
            src_ref=r, dst_ref=r, send_sem=send_un.at[p], recv_sem=recv_o.at[p, edge],
            device_id={"sp": inner}, device_id_type=MESH)

    def end_rows(c, target):
        part = pl.ds(pl.multiple_of(c * x_rows, x_rows), x_rows)
        return pltpu.make_async_remote_copy(
            src_ref=xg.at[0, t, part], dst_ref=xg.at[L, t, part], send_sem=f_send.at[c], recv_sem=f_recv.at[c],
            device_id={"sp": target}, device_id_type=MESH)

    def end_glu(target):
        return pltpu.make_async_remote_copy(
            src_ref=glu_out, dst_ref=pad.at[0], send_sem=f_send.at[x_chunks], recv_sem=f_recv.at[x_chunks],
            device_id={"sp": target}, device_id_type=MESH)

    def each(low_, high_, body):
        def step(q, carry):
            body(q)
            return carry
        lax.fori_loop(low_, high_, step, 0)

    def on(condition, body):
        pl.when(condition)(body)

    def from_inner(stage, q, j):
        def serve():
            inward(stage, q, j).wait_recv()
            if stage != first_vg:
                @pl.when(is_mid)
                def _():
                    outward(stage, q, j).start()
            across(stage, q, j, g).start()
        if stage == first_vg:
            on(is_mid, serve)
        else:
            serve()

    def from_edge(stage, q):
        @pl.when(is_mid)
        def _():
            inward(stage, q, edge).wait_recv()
            inward(stage, q, edge).start()
            if stage == first_vg:
                @pl.when(q >= shared_from)
                def _():
                    across(stage, q, edge, g).start()

    def push_in(stage, lo, hi):
        @pl.when(is_mid)
        def _():
            each(lo, hi, lambda q: inward(stage, q, mine).start())

    def wait_other(stage):
        kind = stage[1]

        def body(j):
            @pl.when(j != s)
            def _():
                each(0, count[kind], lambda q: across(stage, q, j, other).wait_recv())
        each(0, n, body)

    def spread(view, send, recv):
        def copy(bit, m):
            block = view(t ^ m)
            return pltpu.make_async_remote_copy(
                src_ref=block, dst_ref=block, send_sem=send.at[bit + m], recv_sem=recv.at[bit + m],
                device_id={"tp": t ^ bit}, device_id_type=MESH)

        def arrival(bit, m):
            block = view(t ^ bit ^ m)
            return pltpu.make_async_remote_copy(
                src_ref=block, dst_ref=block, send_sem=send.at[bit + m], recv_sem=recv.at[bit + m],
                device_id={"tp": t ^ bit}, device_id_type=MESH)

        bits = []
        bit = T // 2
        while bit >= 1:
            bits.append(bit)
            bit //= 2

        def begin():
            for bit in bits:
                copy(bit, 0).start()

        def order():
            have = [0]
            for i, bit in enumerate(bits):
                for m in have:
                    yield bit, m, bits[i + 1:]
                have = have + [m ^ bit for m in have]

        def finish():
            for bit, m, lower in order():
                arrival(bit, m).wait_recv()
                for b in lower:
                    copy(b, m ^ bit).start()

        def drain():
            for bit, m, _ in order():
                copy(bit, m).wait_send()

        return begin, finish, drain

    def whole(buf, layer, send, recv):
        return spread(lambda j: buf.at[layer, j], send.at[layer], recv.at[layer])

    def edge_spread(c):
        part = pl.ds(pl.multiple_of(c * x_rows, x_rows), x_rows)
        return spread(lambda j: xg.at[L, j, part], e_send.at[c], e_recv.at[c])

    def exchange(index_, columns):
        lane = lax.broadcasted_iota(jnp.int32, (rows, 128), 1)
        tile = jnp.zeros((rows, 128), f32)
        for i, column in enumerate(columns):
            tile = jnp.where(lane == i, column, tile)
        stat[index_, 0] = tile.T[:8, :]

        def copy(d):
            return pltpu.make_async_remote_copy(
                src_ref=stat.at[index_, 0], dst_ref=stat.at[index_, d],
                send_sem=s_send.at[index_, d - 1], recv_sem=s_recv.at[index_, d - 1],
                device_id={"tp": lax.rem(t + d, T)}, device_id_type=MESH)

        for d in range(1, T):
            copy(d).start()

        def total():
            for d in range(1, T):
                copy(d).wait_recv()
            sums = stat[index_, 0]
            for d in range(1, T):
                sums = sums + stat[index_, d]
            wide = jnp.concatenate([sums, jnp.zeros((120, rows), f32)], axis=0).T
            for d in range(1, T):
                copy(d).wait_send()
            return [wide[:, i:i + 1] for i in range(len(columns))]

        return total

    def normalize(layer, held, into):
        def squares(j, total):
            part = xg[held, j].astype(f32)
            return total + jnp.sum(part * part, axis=1, keepdims=True)
        mean = lax.fori_loop(0, T, squares, jnp.zeros((rows, 1), f32)) / D
        scale = lax.rsqrt(mean + 1e-06)

        def body(j, carry):
            xn[into, j] = (xg[held, j].astype(f32) * scale * gain[layer * T + j][None, :]).astype(bf16)
            return carry
        lax.fori_loop(0, T, body, 0)

    def project(layer, held, put):
        for h in range(G):
            def body(j, carry):
                block = wvg[layer, h, pl.ds(pl.multiple_of(j * width, width), width), :]
                part = jnp.dot(xn[held, j], block, preferred_element_type=f32)

                @pl.when(j == 0)
                def _():
                    acc[...] = part

                @pl.when(j > 0)
                def _():
                    acc[...] += part
                return carry
            lax.fori_loop(0, T, body, 0)
            glu = acc[:, :half] * jax.nn.sigmoid(acc[:, half:])
            put(h, glu.astype(bf16))

    def to_right(layer):
        return pltpu.make_async_remote_copy(
            src_ref=pad.at[layer, pl.ds(rows, PAD), :], dst_ref=pad.at[layer, pl.ds(0, PAD), :],
            send_sem=h_send.at[layer, 0], recv_sem=h_recv.at[layer, 0],
            device_id={"sp": s + 1}, device_id_type=MESH)

    def to_left(layer):
        return pltpu.make_async_remote_copy(
            src_ref=pad.at[layer, pl.ds(PAD, PAD), :], dst_ref=pad.at[layer, pl.ds(PAD + rows, PAD), :],
            send_sem=h_send.at[layer, 1], recv_sem=h_recv.at[layer, 1],
            device_id={"sp": s - 1}, device_id_type=MESH)

    def sides_of(layer):
        if layer == 0:
            return s == 1, s == last - 1, s == last - 1, s == 1
        return s < last, s > 0, s > 0, s < last

    def convolve(layer):
        padf[...] = pad[layer].astype(f32)
        block = 64
        sums, squares = [], []
        for r in range(0, rows, block):
            total = jnp.zeros((block, chans), f32)
            for k in range(n_taps):
                start = r + PAD - reach + k
                total = total + taps[layer, k][None, :] * padf[start:start + block, :]
            conv[r:r + block, :] = total
            sums.append(jnp.sum(total, axis=1, keepdims=True))
            squares.append(jnp.sum(total * total, axis=1, keepdims=True))
        return exchange(layer, [jnp.concatenate(sums, 0), jnp.concatenate(squares, 0)])

    def activate(layer, totals):
        total, square = totals()
        center = total / C
        spread_ = square / C - center * center
        normal = (conv[...] - center) * lax.rsqrt(spread_ + 1e-05)
        actg[layer, t] = jax.nn.silu(normal * cgain[layer][None, :]).astype(bf16)

    def add_branch(layer):
        for h in range(G):
            part = None
            for j in range(T):
                term = jnp.dot(actg[layer, j], wo[layer, h, j * chans:(j + 1) * chans, :], preferred_element_type=f32)
                part = term if part is None else part + term
            cols = slice(h * out_half, (h + 1) * out_half)
            x_state[:, cols] = (x_state[:, cols] + part).astype(bf16).astype(f32)

    for c in staged[first_vg]:
        c.wait()
    on(s >= 0, lambda: each(0, QC, lambda q: inward(first_vg, q, s).start()))
    token_copy.wait()
    x_own = [whole(xg, layer, x_send, x_recv) for layer in range(L)]

    @pl.when(is_end)
    def _():
        each(0, x_chunks, lambda c: end_rows(c, inner).start())

    @pl.when(is_mid)
    def _():
        x_own[0][0]()

    for stage in after:
        for c in staged[stage]:
            c.wait()

    @pl.when(is_end)
    def _():
        each(0, shared_from, lambda q: direct(first_vg, q).start())
        for stage in after:
            each(0, count[stage[1]], lambda q: inward(stage, q, edge).start())
            each(0, count[stage[1]], lambda q: direct(stage, q).start())

    @pl.when(is_mid)
    def _():
        for stage in after:
            each(0, count[stage[1]], lambda q: outward(stage, q, mine).start())

    x_state[...] = xg[0, t].astype(f32)

    def first_chunks(q):
        from_edge(first_vg, q)
        from_inner(first_vg, q, near)
    each(0, QC, first_chunks)

    @pl.when(is_end)
    def _():
        def pass_on(stage):
            def body(q):
                outward(stage, q, mine).wait_recv()
                across(stage, q, mine, g).start()
            each(0, count[stage[1]], body)
        for stage in after:
            pass_on(stage)

    @pl.when(is_mid)
    def _():
        x_own[0][1]()
        normalize(0, 0, 0)

    def second_chunks(q):
        from_inner(first_vg, q, far)

        @pl.when(is_mid)
        def _():
            end_rows(q, edge).wait_recv()
            edge_spread(q)[0]()
    each(0, QC, second_chunks)
    push_in(first_wo, 0, RC)
    push_in(second_vg, 0, QC // 2)
    each(0, RC, lambda q: from_inner(first_wo, q, near))

    def put(layer):
        def store(h, value):
            pad[layer, PAD:PAD + rows, h * half:(h + 1) * half] = value
        return store

    def put_out(h, value):
        glu_out[PAD:PAD + rows, h * half:(h + 1) * half] = value

    @pl.when(is_mid)
    def _():
        each(0, x_chunks, lambda c: edge_spread(c)[1]())
        normalize(0, L, 1)
        wait_other(first_vg)
        project(0, 1, put_out)
        project(0, 0, put(0))

    sends_right, sends_left, from_left, from_right = sides_of(0)

    @pl.when(sends_right)
    def _():
        to_right(0).start()
        glu_out[0:PAD, :] = jnp.zeros((PAD, chans), bf16)
        glu_out[PAD + rows:, :] = pad[0, PAD:2 * PAD, :]
        pad[0, 0:PAD, :] = glu_out[rows:rows + PAD, :]

    @pl.when(sends_left)
    def _():
        to_left(0).start()
        glu_out[0:PAD, :] = pad[0, rows:rows + PAD, :]
        glu_out[PAD + rows:, :] = jnp.zeros((PAD, chans), bf16)
        pad[0, PAD + rows:, :] = glu_out[PAD:2 * PAD, :]

    @pl.when(is_mid)
    def _():
        end_glu(edge).start()
    each(0, RC, lambda q: from_edge(first_wo, q))
    each(0, QC // 2, lambda q: from_inner(second_vg, q, near))
    push_in(second_vg, QC // 2, QC)

    @pl.when(from_left)
    def _():
        to_right(0).wait_recv()

    @pl.when(from_right)
    def _():
        to_left(0).wait_recv()

    @pl.when(is_end)
    def _():
        end_glu(inner).wait_recv()

    totals = convolve(0)
    each(0, RC, lambda q: from_inner(first_wo, q, far))
    activate(0, totals)
    act = [whole(actg, layer, a_send, a_recv) for layer in range(L)]
    act[0][0]()
    act[0][1]()
    wait_other(first_wo)
    add_branch(0)
    xg[1, t] = x_state[...].astype(bf16)
    x_own[1][0]()
    each(QC // 2, QC, lambda q: from_inner(second_vg, q, near))

    def third_chunks(q):
        from_edge(second_vg, q)
        from_inner(second_vg, q, far)
    each(0, QC, third_chunks)
    push_in(second_wo, 0, RC)
    x_own[1][1]()
    normalize(1, 1, 0)
    each(0, RC, lambda q: from_inner(second_wo, q, near))
    wait_other(second_vg)
    project(1, 0, put(1))
    sends_right, sends_left, from_left, from_right = sides_of(1)

    @pl.when(sends_right)
    def _():
        to_right(1).start()

    @pl.when(sends_left)
    def _():
        to_left(1).start()

    @pl.when(jnp.logical_not(from_left))
    def _():
        pad[1, 0:PAD, :] = jnp.zeros((PAD, chans), bf16)

    @pl.when(jnp.logical_not(from_right))
    def _():
        pad[1, PAD + rows:, :] = jnp.zeros((PAD, chans), bf16)

    each(0, RC, lambda q: from_edge(second_wo, q))

    @pl.when(from_left)
    def _():
        to_right(1).wait_recv()

    @pl.when(from_right)
    def _():
        to_left(1).wait_recv()

    totals = convolve(1)
    each(0, RC, lambda q: from_inner(second_wo, q, far))
    activate(1, totals)
    act[1][0]()
    act[1][1]()
    wait_other(second_wo)
    add_branch(1)
    xf = x_state[...]
    totals = exchange(L, [jnp.sum(xf * xf, axis=1, keepdims=True)])

    for layer in range(L):
        sends_right, sends_left, _, _ = sides_of(layer)

        @pl.when(sends_right)
        def _():
            to_right(layer).wait_send()

        @pl.when(sends_left)
        def _():
            to_left(layer).wait_send()
    act[0][2]()
    act[1][2]()
    x_own[1][2]()

    @pl.when(is_mid)
    def _():
        x_own[0][2]()
        each(0, x_chunks, lambda c: edge_spread(c)[2]())
        end_glu(edge).wait_send()
        for stage in (first_vg,) + after:
            def body(q):
                inward(stage, q, mine).wait_send()
                inward(stage, q, edge).wait_send()
                if stage == first_vg:
                    @pl.when(q >= shared_from)
                    def _():
                        across(stage, q, edge, g).wait_send()
                for j in (near, far):
                    across(stage, q, j, g).wait_send()
                    if stage != first_vg:
                        outward(stage, q, j).wait_send()
                if stage != first_vg:
                    outward(stage, q, mine).wait_send()
            each(0, count[stage[1]], body)

    @pl.when(is_end)
    def _():
        each(0, x_chunks, lambda c: end_rows(c, inner).wait_send())
        each(0, shared_from, lambda q: direct(first_vg, q).wait_send())
        each(0, QC, lambda q: inward(first_vg, q, edge).wait_send())
        for stage in after:
            def body(q):
                inward(stage, q, edge).wait_send()
                direct(stage, q).wait_send()
                for j in (mine, near, far):
                    across(stage, q, j, g).wait_send()
            each(0, count[stage[1]], body)

    (total,) = totals()
    scale = lax.rsqrt(total / D + 1e-06)
    result[...] = (x_state[...] * scale * fgain[...]).astype(bf16)


def quad_on_device(G, n, T, tokens, norm_gain, value_w, gate_w, taps, cgain, out_w, fgain):
    L = norm_gain.shape[0]
    if L != 2:
        return on_device(G, n, T, tokens, norm_gain, value_w, gate_w, taps, cgain, out_w, fgain)
    rows, width = tokens.shape
    depth, chans = value_w.shape[1:]
    D, C = width * T, chans * T
    bf16, f32 = jnp.bfloat16, jnp.float32
    dma = pltpu.SemaphoreType.DMA
    vmem = pl.BlockSpec(memory_space=pltpu.VMEM)
    hbm = pl.BlockSpec(memory_space=pl.ANY)
    P_ = L * (QC + RC)
    return pl.pallas_call(
        functools.partial(quad_kernel, G, n, T, L),
        out_shape=jax.ShapeDtypeStruct((rows, width), bf16),
        in_specs=[hbm, vmem, hbm, hbm, vmem, vmem, hbm, vmem],
        out_specs=vmem,
        scratch_shapes=[
            pltpu.VMEM((L, G, D, 2 * chans // G), bf16),
            pltpu.VMEM((L, G, C, width // G), bf16),
            pltpu.VMEM((L + 1, T, rows, width), bf16),
            pltpu.VMEM((2, T, rows, width), bf16),
            pltpu.VMEM((rows + 2 * PAD, chans), bf16),
            pltpu.VMEM((rows, 2 * chans // G), f32),
            pltpu.VMEM((L, rows + 2 * PAD, chans), bf16),
            pltpu.VMEM((rows + 2 * PAD, chans), f32),
            pltpu.VMEM((rows, chans), f32),
            pltpu.VMEM((L + 1, T, 8, rows), f32),
            pltpu.VMEM((L, T, rows, chans), bf16),
            pltpu.VMEM((rows, width), f32),
            dma((1 + L * G * 3,)),
            dma((P_, n)), dma((P_, n)), dma((P_, n)), dma((P_, n)), dma((P_, n)), dma((P_,)),
            dma((L, T)), dma((L, T)), dma((QC, T)), dma((QC, T)), dma((L, T)), dma((L, T)),
            dma((L + 1, T)), dma((L + 1, T)),
            dma((L, 2)), dma((L, 2)),
            dma((QC + 1,)), dma((QC + 1,)),
        ],
        compiler_params=pltpu.CompilerParams(
            collective_id=0, has_side_effects=True, vmem_limit_bytes=56 * 2**20
        ),
    )(tokens, norm_gain.reshape(L * T, width), value_w, gate_w, taps, cgain, out_w, fgain.reshape(1, width))


def tokens_f32(tokens, xg, t):
    return xg[0, t].astype(jnp.float32)


def on_device(G, n, T, tokens, norm_gain, value_w, gate_w, taps, cgain, out_w, fgain):
    L = norm_gain.shape[0]
    rows, width = tokens.shape
    depth, chans = value_w.shape[1:]
    D, C = width * T, chans * T
    bf16, f32 = jnp.bfloat16, jnp.float32
    dma = pltpu.SemaphoreType.DMA
    vmem = pl.BlockSpec(memory_space=pltpu.VMEM)
    hbm = pl.BlockSpec(memory_space=pl.ANY)
    P_ = L * (Q + 1)
    peers = max(G - 1, 1)
    return pl.pallas_call(
        functools.partial(kernel, G, n, T, L),
        out_shape=jax.ShapeDtypeStruct((rows, width), bf16),
        in_specs=[hbm, vmem, hbm, hbm, vmem, vmem, hbm, vmem],
        out_specs=vmem,
        scratch_shapes=[
            pltpu.VMEM((L, G, D, 2 * chans // G), bf16),
            pltpu.VMEM((L, G, C, width // G), bf16),
            pltpu.VMEM((L + 1, T, rows, width), bf16),
            pltpu.VMEM((2, T, rows, width), bf16),
            pltpu.VMEM((rows, chans), bf16),
            pltpu.VMEM((rows, 2 * chans // G), f32),
            pltpu.VMEM((L, rows + 2 * PAD, chans), bf16),
            pltpu.VMEM((rows + 2 * PAD, chans), f32),
            pltpu.VMEM((rows, chans), f32),
            pltpu.VMEM((L + 1, T, 8, rows), f32),
            pltpu.VMEM((L, T, rows, chans), bf16),
            pltpu.VMEM((rows, width), f32),
            dma((1 + L * G * 3,)),
            dma((P_, n)), dma((P_, n)), dma((P_, n)),
            dma((P_, n, peers)), dma((P_, n, peers)),
            dma((L + 1, T)), dma((L + 1, T)), dma((L, T)), dma((L, T)),
            dma((L + 1, T)), dma((L + 1, T)),
            dma((L, 2)), dma((L, 2)),
            dma((G + 1,)), dma((G + 1,)),
        ],
        compiler_params=pltpu.CompilerParams(
            collective_id=0, has_side_effects=True, vmem_limit_bytes=56 * 2**20
        ),
    )(tokens, norm_gain.reshape(L * T, width), value_w, gate_w, taps, cgain, out_w, fgain.reshape(1, width))


def solution(mesh):
    placed = (
        P(("grp", "sp"), "tp"),
        P(),
        P(None, "sp", "tp"),
        P(None, "sp", "tp"),
        P(None, None, "tp"),
        P(None, "tp"),
        P(None, "sp", "tp"),
        P("tp"),
    )
    G, n, T = (mesh.shape[a] for a in ("grp", "sp", "tp"))
    paired = n - 2 == G == 2 and T & (T - 1) == 0
    return jax.shard_map(
        functools.partial(quad_on_device if paired else on_device, G, n, T),
        mesh=mesh, in_specs=placed, out_specs=P(("grp", "sp"), "tp"), check_vma=False,
    )
```

```python
import functools

import jax
import jax.numpy as jnp
from jax import lax
from jax.experimental import pallas as pl
from jax.experimental.pallas import tpu as pltpu
from jax.sharding import PartitionSpec as P

MESH = pl.DeviceIdType.MESH
Q = 2
PAD = 16


def kernel(
    G, n, T, L,
    tokens, gain, value_w, gate_w, taps, cgain, out_w, fgain,
    result,
    wvg, wo, xg, xn, glu_out, acc, pad, padf, conv, stat, actg, x_state,
    local_sem, z_recv, right_send, left_send, y_send, y_recv,
    x_send, x_recv, a_send, a_recv, s_send, s_recv, h_send, h_recv, f_send, f_recv,
):
    g, s, t = lax.axis_index("grp"), lax.axis_index("sp"), lax.axis_index("tp")
    rows, width = tokens.shape
    depth, chans = value_w.shape[1:]
    out_rows = out_w.shape[1]
    half = chans // G
    out_half = width // G
    reach = taps.shape[1] // 2
    n_taps = taps.shape[1]
    D = width * T
    C = chans * T
    chunk = depth // Q
    pieces = Q + 1
    f32, bf16 = jnp.float32, jnp.bfloat16
    helped = n >= 4
    last = n - 1
    is_end = (s == 0) | (s == last)
    helper = (s == 1) | (s == last - 1)
    end = jnp.where(s == 1, 0, last)
    inward = jnp.where(s == 0, 1, last - 1)

    def ends_out(p):
        return helped and p < Q

    def to_right_ok(p):
        return s < last - 1 if ends_out(p) else s < last

    def to_left_ok(p):
        return s > 1 if ends_out(p) else s > 0

    def takes(p):
        return jnp.logical_not(is_end) if ends_out(p) else s >= 0

    def by_grp(p, j):
        ok = takes(p) & (j != s)
        if helped and p == 0:
            ok = ok & jnp.logical_not((s == 1) & (j == 0)) & jnp.logical_not((s == last - 1) & (j == last))
        return ok

    def piece(p, h, j):
        layer, q = p // pieces, p % pieces
        if q < Q:
            start = pl.multiple_of(j * depth + q * chunk, chunk)
            return wvg.at[layer, h, pl.ds(start, chunk), :]
        return wo.at[layer, h, pl.ds(pl.multiple_of(j * out_rows, out_rows), out_rows), :]

    locals_ = [pltpu.make_async_copy(tokens, xg.at[0, t], local_sem.at[0])]
    own_rows = pl.ds(pl.multiple_of(s * depth, depth), depth)
    own_out = pl.ds(pl.multiple_of(s * out_rows, out_rows), out_rows)
    count = 1
    per_layer = []
    for layer in range(L):
        group = []
        for h in range(G):
            for k, w in enumerate((value_w, gate_w)):
                group.append(pltpu.make_async_copy(
                    w.at[layer, :, pl.ds(h * half, half)],
                    wvg.at[layer, h, own_rows, pl.ds(k * half, half)],
                    local_sem.at[count]))
                count += 1
            group.append(pltpu.make_async_copy(
                out_w.at[layer, :, pl.ds(h * out_half, out_half)],
                wo.at[layer, h, own_out, :], local_sem.at[count]))
            count += 1
        per_layer.append(group)
    for c in locals_ + sum(per_layer, []):
        c.start()

    barrier = pltpu.get_barrier_semaphore()
    for d in range(1, T):
        pl.semaphore_signal(barrier, inc=1, device_id={"tp": lax.rem(t + d, T)}, device_id_type=MESH)
    for d in range(1, G):
        pl.semaphore_signal(barrier, inc=1, device_id={"grp": lax.rem(g + d, G)}, device_id_type=MESH)

    @pl.when(s > 0)
    def _():
        pl.semaphore_signal(barrier, inc=1, device_id={"sp": s - 1}, device_id_type=MESH)

    @pl.when(s < n - 1)
    def _():
        pl.semaphore_signal(barrier, inc=1, device_id={"sp": s + 1}, device_id_type=MESH)

    sides = jnp.where(s > 0, 1, 0) + jnp.where(s < n - 1, 1, 0)
    pl.semaphore_wait(barrier, (T - 1) + (G - 1) + sides)

    def right(p, j):
        r = piece(p, g, j)
        return pltpu.make_async_remote_copy(
            src_ref=r, dst_ref=r, send_sem=right_send.at[p, j], recv_sem=z_recv.at[p, j],
            device_id={"sp": s + 1}, device_id_type=MESH)

    def left(p, j):
        r = piece(p, g, j)
        return pltpu.make_async_remote_copy(
            src_ref=r, dst_ref=r, send_sem=left_send.at[p, j], recv_sem=z_recv.at[p, j],
            device_id={"sp": s - 1}, device_id_type=MESH)

    def across(p, j, d, h):
        r = piece(p, h, j)
        return pltpu.make_async_remote_copy(
            src_ref=r, dst_ref=r, send_sem=y_send.at[p, j, d - 1], recv_sem=y_recv.at[p, j, d - 1],
            device_id={"grp": lax.rem(g + d, G)}, device_id_type=MESH)

    batches = []
    for layer in range(L):
        base = layer * pieces
        batches += [list(range(base, base + Q)), [base + Q]]

    def own_right(ps):
        for p in ps:
            right(p, s).start()

    def own_left(ps):
        for p in ps:
            left(p, s).start()

    def end_rows(target):
        return pltpu.make_async_remote_copy(
            src_ref=xg.at[0, t], dst_ref=xg.at[L, t], send_sem=f_send.at[0], recv_sem=f_recv.at[0],
            device_id={"sp": target}, device_id_type=MESH)

    def end_piece(d, h, j, target):
        r = piece(0, h, j)
        return pltpu.make_async_remote_copy(
            src_ref=r, dst_ref=r, send_sem=f_send.at[d], recv_sem=f_recv.at[d],
            device_id={"sp": target}, device_id_type=MESH)

    def end_glu(target):
        return pltpu.make_async_remote_copy(
            src_ref=glu_out, dst_ref=pad.at[0, pl.ds(PAD, rows), :],
            send_sem=f_send.at[G], recv_sem=f_recv.at[G],
            device_id={"sp": target}, device_id_type=MESH)

    def relay(b, low, high):
        low, high = min(low, n - 1), min(high, n - 1)
        following = batches[b + 1] if b + 1 < len(batches) else []

        def step(k, carry):
            for p in batches[b]:
                from_left, from_right = s - 1 - k, s + 1 + k

                @pl.when((from_left >= 0) & takes(p))
                def _():
                    j = jnp.maximum(from_left, 0)
                    right(p, j).wait_recv()

                    @pl.when(to_right_ok(p))
                    def _():
                        right(p, j).start()

                    @pl.when(by_grp(p, j))
                    def _():
                        for d in range(1, G):
                            across(p, j, d, g).start()

                @pl.when((from_right < n) & takes(p))
                def _():
                    j = jnp.minimum(from_right, n - 1)
                    left(p, j).wait_recv()

                    @pl.when(to_left_ok(p))
                    def _():
                        left(p, j).start()

                    @pl.when(by_grp(p, j))
                    def _():
                        for d in range(1, G):
                            across(p, j, d, g).start()

            @pl.when((k == s - 1) & (s < (last - 1 if helped and b < 2 else last)))
            def _():
                own_right(following)

            @pl.when((k == n - 2 - s) & (s > (1 if helped and b < 2 else 0)))
            def _():
                own_left(following)

            return carry

        if high > low:
            lax.fori_loop(low, high, step, 0)

    def wait_across(b):
        for p in batches[b]:
            def step(j, carry):
                @pl.when(by_grp(p, j))
                def _():
                    for d in range(1, G):
                        across(p, j, d, lax.rem(g + G - d, G)).wait_recv()
                return carry
            lax.fori_loop(0, n, step, 0)

    def spread(buf, layer, send, recv):
        def copy(bit, m):
            block = buf.at[layer, t ^ m]
            return pltpu.make_async_remote_copy(
                src_ref=block, dst_ref=block, send_sem=send.at[layer, bit + m], recv_sem=recv.at[layer, bit + m],
                device_id={"tp": t ^ bit}, device_id_type=MESH)

        def arrival(bit, m):
            block = buf.at[layer, t ^ bit ^ m]
            return pltpu.make_async_remote_copy(
                src_ref=block, dst_ref=block, send_sem=send.at[layer, bit + m], recv_sem=recv.at[layer, bit + m],
                device_id={"tp": t ^ bit}, device_id_type=MESH)

        bits = []
        bit = T // 2
        while bit >= 1:
            bits.append(bit)
            bit //= 2

        def begin():
            for bit in bits:
                copy(bit, 0).start()

        def finish():
            have, sent = [0], []
            for i, bit in enumerate(bits):
                for m in have:
                    arrival(bit, m).wait_recv()
                    sent.append((bit, m))
                    for lower in bits[i + 1:]:
                        copy(lower, m ^ bit).start()
                have = have + [m ^ bit for m in have]
            return lambda: [copy(bit, m).wait_send() for bit, m in sent]

        return begin, finish

    def exchange(index, columns):
        lane = lax.broadcasted_iota(jnp.int32, (rows, 128), 1)
        tile = jnp.zeros((rows, 128), f32)
        for i, column in enumerate(columns):
            tile = jnp.where(lane == i, column, tile)
        stat[index, 0] = tile.T[:8, :]

        def copy(d):
            return pltpu.make_async_remote_copy(
                src_ref=stat.at[index, 0], dst_ref=stat.at[index, d],
                send_sem=s_send.at[index, d - 1], recv_sem=s_recv.at[index, d - 1],
                device_id={"tp": lax.rem(t + d, T)}, device_id_type=MESH)

        for d in range(1, T):
            copy(d).start()

        def total():
            for d in range(1, T):
                copy(d).wait_recv()
            sums = stat[index, 0]
            for d in range(1, T):
                sums = sums + stat[index, d]
            wide = jnp.concatenate([sums, jnp.zeros((120, rows), f32)], axis=0).T
            for d in range(1, T):
                copy(d).wait_send()
            return [wide[:, i:i + 1] for i in range(len(columns))]

        return total

    def normalize(layer, held, into):
        def squares(j, total):
            part = xg[held, j].astype(f32)
            return total + jnp.sum(part * part, axis=1, keepdims=True)
        mean = lax.fori_loop(0, T, squares, jnp.zeros((rows, 1), f32)) / D
        scale = lax.rsqrt(mean + 1e-06)

        def body(j, carry):
            xn[into, j] = (xg[held, j].astype(f32) * scale * gain[layer * T + j][None, :]).astype(bf16)
            return carry
        lax.fori_loop(0, T, body, 0)

    def project(layer, held, put):
        for h in range(G):
            def body(j, carry):
                block = wvg[layer, h, pl.ds(pl.multiple_of(j * width, width), width), :]
                part = jnp.dot(xn[held, j], block, preferred_element_type=f32)

                @pl.when(j == 0)
                def _():
                    acc[...] = part

                @pl.when(j > 0)
                def _():
                    acc[...] += part
                return carry
            lax.fori_loop(0, T, body, 0)
            glu = acc[:, :half] * jax.nn.sigmoid(acc[:, half:])
            put(h, glu.astype(bf16))

    for c in locals_:
        c.wait()
    spreads = [spread(xg, layer, x_send, x_recv) for layer in range(L)]
    spreads[0][0]()
    for c in sum(per_layer, []):
        c.wait()

    @pl.when(to_right_ok(0))
    def _():
        own_right(batches[0])

    @pl.when(to_left_ok(0))
    def _():
        own_left(batches[0])

    if helped:
        @pl.when(is_end)
        def _():
            end_rows(inward).start()
            for d in range(1, G):
                end_piece(d, lax.rem(g + d, G), s, inward).start()

        @pl.when(s == last - 1)
        def _():
            own_right(batches[1])
            if L > 1:
                own_right(batches[2])

        @pl.when(s == 1)
        def _():
            own_left(batches[1])
            if L > 1:
                own_left(batches[2])

    @pl.when((s == 0) & (s < n - 1))
    def _():
        for b in batches[1:]:
            own_right(b)

    @pl.when((s == n - 1) & (s > 0))
    def _():
        for b in batches[1:]:
            own_left(b)

    x_state[...] = tokens_f32(tokens, xg, t)
    drains = []

    for layer in range(L):
        first, second = 2 * layer, 2 * layer + 1
        if layer == 0:
            relay(first, 0, 1)
        else:
            relay(first, 1, 2)
        drains.append(spreads[layer][1]())
        if helped and layer == 0:
            @pl.when(jnp.logical_not(is_end))
            def _():
                normalize(layer, layer, 0)
        else:
            normalize(layer, layer, 0)
        relay(first, 1 if layer == 0 else 2, n)
        begin, finish = spread(xg, L, x_send, x_recv)
        if helped and layer == 0:
            @pl.when(helper)
            def _():
                end_rows(end).wait_recv()
                begin()

        relay(second, 0, 1)

        def put(h, value):
            pad[layer, PAD:PAD + rows, h * half:(h + 1) * half] = value

        def put_out(h, value):
            glu_out[:, h * half:(h + 1) * half] = value

        if helped and layer == 0:
            @pl.when(helper)
            def _():
                drain = finish()
                normalize(0, L, 1)
                for d in range(1, G):
                    end_piece(d, lax.rem(g + d, G), end, end).wait_recv()
                drain()

            wait_across(first)

            @pl.when(helper)
            def _():
                project(0, 1, put_out)
                end_glu(end).start()

            @pl.when(jnp.logical_not(is_end))
            def _():
                project(0, 0, put)

            @pl.when(helper)
            def _():
                end_glu(end).wait_send()

            @pl.when(is_end)
            def _():
                end_rows(inward).wait_send()
                for d in range(1, G):
                    end_piece(d, lax.rem(g + d, G), s, inward).wait_send()
                end_glu(inward).wait_recv()
        else:
            wait_across(first)
            project(layer, 0, put)

        def to_right():
            return pltpu.make_async_remote_copy(
                src_ref=pad.at[layer, pl.ds(rows, PAD), :], dst_ref=pad.at[layer, pl.ds(0, PAD), :],
                send_sem=h_send.at[layer, 0], recv_sem=h_recv.at[layer, 0],
                device_id={"sp": s + 1}, device_id_type=MESH)

        def to_left():
            return pltpu.make_async_remote_copy(
                src_ref=pad.at[layer, pl.ds(PAD, PAD), :], dst_ref=pad.at[layer, pl.ds(PAD + rows, PAD), :],
                send_sem=h_send.at[layer, 1], recv_sem=h_recv.at[layer, 1],
                device_id={"sp": s - 1}, device_id_type=MESH)

        @pl.when(s < n - 1)
        def _():
            to_right().start()

        @pl.when(s > 0)
        def _():
            to_left().start()

        @pl.when(s == 0)
        def _():
            pad[layer, 0:PAD, :] = jnp.zeros((PAD, chans), bf16)

        @pl.when(s == n - 1)
        def _():
            pad[layer, PAD + rows:, :] = jnp.zeros((PAD, chans), bf16)

        relay(second, 1, 2)

        @pl.when(s > 0)
        def _():
            to_right().wait_recv()

        @pl.when(s < n - 1)
        def _():
            to_left().wait_recv()

        padf[...] = pad[layer].astype(f32)
        block = 64
        sums, squares = [], []
        for r in range(0, rows, block):
            total = jnp.zeros((block, chans), f32)
            for k in range(n_taps):
                start = r + PAD - reach + k
                total = total + taps[layer, k][None, :] * padf[start:start + block, :]
            conv[r:r + block, :] = total
            sums.append(jnp.sum(total, axis=1, keepdims=True))
            squares.append(jnp.sum(total * total, axis=1, keepdims=True))
        totals = exchange(layer, [jnp.concatenate(sums, 0), jnp.concatenate(squares, 0)])
        relay(second, 2, n)
        if layer + 1 < L:
            relay(second + 1, 0, 1)
        total, square = totals()
        center = total / C
        spread_ = square / C - center * center
        normal = (conv[...] - center) * lax.rsqrt(spread_ + 1e-05)
        actg[layer, t] = jax.nn.silu(normal * cgain[layer][None, :]).astype(bf16)
        act_begin, act_finish = spread(actg, layer, a_send, a_recv)
        act_begin()
        drains.append(act_finish())
        wait_across(second)
        for h in range(G):
            part = None
            for j in range(T):
                term = jnp.dot(actg[layer, j], wo[layer, h, j * chans:(j + 1) * chans, :], preferred_element_type=f32)
                part = term if part is None else part + term
            cols = slice(h * out_half, (h + 1) * out_half)
            x_state[:, cols] = (x_state[:, cols] + part).astype(bf16).astype(f32)
        if layer + 1 < L:
            xg[layer + 1, t] = x_state[...].astype(bf16)
            spreads[layer + 1][0]()

        @pl.when(s < n - 1)
        def _():
            to_right().wait_send()

        @pl.when(s > 0)
        def _():
            to_left().wait_send()

    xf = x_state[...]
    totals = exchange(L, [jnp.sum(xf * xf, axis=1, keepdims=True)])

    for drain in drains:
        drain()

    def drain_step(j, carry):
        for p in range(L * pieces):
            came = (j == s) | takes(p)

            @pl.when((j <= s) & to_right_ok(p) & came)
            def _():
                right(p, j).wait_send()

            @pl.when((j >= s) & to_left_ok(p) & came)
            def _():
                left(p, j).wait_send()

            @pl.when(by_grp(p, j))
            def _():
                for d in range(1, G):
                    across(p, j, d, g).wait_send()
        return carry
    lax.fori_loop(0, n, drain_step, 0)

    (total,) = totals()
    scale = lax.rsqrt(total / D + 1e-06)
    result[...] = (x_state[...] * scale * fgain[...]).astype(bf16)


QC = 4
RC = 2


def quad_kernel(
    G, n, T, L,
    tokens, gain_hbm, value_w, gate_w, taps_hbm, cgain_hbm, out_w, fgain_hbm,
    result,
    wvg, wo, xg, xn, glu_out, acc, pad, padf, convg, stat, x_state, gain, taps, cgain, fgain,
    local_sem, recv_z, recv_o, send_w, x_sem, e_sem, c_sem, s_sem, h_sem, hs_sem, g_sem, f_sem,
):
    g, s, t = lax.axis_index("grp"), lax.axis_index("sp"), lax.axis_index("tp")
    rows, width = tokens.shape
    depth, chans = value_w.shape[1:]
    out_rows = out_w.shape[1]
    half = chans // G
    out_half = width // G
    n_taps = taps.shape[0]
    reach = n_taps // 2
    D = width * T
    C = chans * T
    full = rows + 2 * PAD
    pieces = QC + RC
    size = {"vg": depth // QC, "wo": out_rows // RC}
    count = {"vg": QC, "wo": RC}
    shared_from = QC - 1
    f32, bf16 = jnp.float32, jnp.bfloat16
    last = n - 1
    low = s < n // 2
    is_end = (s == 0) | (s == last)
    is_mid = jnp.logical_not(is_end)
    inner = jnp.where(low, s + 1, s - 1)
    outer = jnp.where(low, s - 1, s + 1)
    edge, mine, near, far = (jnp.where(low, a, last - a) for a in (0, 1, n - 2, n - 1))
    other = lax.rem(g + 1, G)
    x_chunks = QC
    x_rows = rows // x_chunks
    own = pl.ds(PAD, rows)
    first_vg, first_wo, second_vg, second_wo = (0, "vg"), (0, "wo"), (1, "vg"), (1, "wo")
    after = (first_wo, second_vg, second_wo)
    scope = jax.named_scope
    IN, OUT, Y, YE, UN = range(5)

    def index(stage, q):
        layer, kind = stage
        return layer * pieces + (0 if kind == "vg" else QC) + q

    def order_of(stage):
        return stage[0] * 2 + (0 if stage[1] == "vg" else 1)

    def place(j):
        return jnp.where(j == near, 1, jnp.where(j == far, 2, 0))

    def piece(stage, q, h, j):
        layer, kind = stage
        step = size[kind]
        per = depth if kind == "vg" else out_rows
        ref = wvg if kind == "vg" else wo
        return ref.at[layer, h, pl.ds(pl.multiple_of(j * per + q * step, step), step), :]

    def wait_bytes(ref, sem):
        pltpu.make_async_copy(ref, ref, sem).wait()

    own_rows = pl.ds(pl.multiple_of(s * depth, depth), depth)
    own_out = pl.ds(pl.multiple_of(s * out_rows, out_rows), out_rows)

    def stage_in(stage):
        layer, kind = stage
        sem = local_sem.at[order_of(stage)]
        for h in range(G):
            if kind == "vg":
                for k, w in enumerate((value_w, gate_w)):
                    pltpu.make_async_copy(
                        w.at[layer, :, pl.ds(h * half, half)],
                        wvg.at[layer, h, own_rows, pl.ds(k * half, half)], sem).start()
            else:
                pltpu.make_async_copy(
                    out_w.at[layer, :, pl.ds(h * out_half, out_half)],
                    wo.at[layer, h, own_out, :], sem).start()

    def staged(stage):
        layer, kind = stage
        ref = wvg.at[layer, :, own_rows] if kind == "vg" else wo.at[layer, :, own_out]
        wait_bytes(ref, local_sem.at[order_of(stage)])

    token_copy = pltpu.make_async_copy(tokens, xg.at[0, t, own], local_sem.at[2 * L])
    gain_copy = pltpu.make_async_copy(cgain_hbm, cgain.at[t], local_sem.at[2 * L + 1])
    small = [
        pltpu.make_async_copy(gain_hbm, gain, local_sem.at[2 * L + 2]),
        pltpu.make_async_copy(taps_hbm, taps, local_sem.at[2 * L + 3]),
        pltpu.make_async_copy(fgain_hbm, fgain, local_sem.at[2 * L + 4]),
    ]
    stage_in(first_vg)
    token_copy.start()
    gain_copy.start()
    for stage in after:
        stage_in(stage)
    for c in small:
        c.start()

    barrier = pltpu.get_barrier_semaphore()
    for d in range(1, T):
        pl.semaphore_signal(barrier, inc=1, device_id={"tp": lax.rem(t + d, T)}, device_id_type=MESH)
    pl.semaphore_signal(barrier, inc=1, device_id={"grp": other}, device_id_type=MESH)

    @pl.when(s > 0)
    def _():
        pl.semaphore_signal(barrier, inc=1, device_id={"sp": s - 1}, device_id_type=MESH)

    @pl.when(s < last)
    def _():
        pl.semaphore_signal(barrier, inc=1, device_id={"sp": s + 1}, device_id_type=MESH)

    blank = jnp.zeros((T, PAD, width), bf16)

    @pl.when(s < n // 2)
    def _():
        xg[0, :, 0:PAD, :] = blank

    @pl.when(s >= n // 2)
    def _():
        xg[0, :, PAD + rows:, :] = blank

    @pl.when(s == 0)
    def _():
        xg[1, :, 0:PAD, :] = blank

    @pl.when(s == last)
    def _():
        xg[1, :, PAD + rows:, :] = blank

    sides = jnp.where(s > 0, 1, 0) + jnp.where(s < last, 1, 0)
    pl.semaphore_wait(barrier, (T - 1) + (G - 1) + sides)

    def arrived(stage, q, j):
        wait_bytes(piece(stage, q, g, j), recv_z.at[index(stage, q), place(j)])

    def inward(stage, q, j):
        r, p = piece(stage, q, g, j), index(stage, q)
        there = jnp.where(is_end, 0, jnp.where(j == mine, 1, 2))
        return pltpu.make_async_remote_copy(
            src_ref=r, dst_ref=r, send_sem=send_w.at[IN], recv_sem=recv_z.at[p, there],
            device_id={"sp": inner}, device_id_type=MESH)

    def outward(stage, q, j):
        r, p = piece(stage, q, g, j), index(stage, q)
        return pltpu.make_async_remote_copy(
            src_ref=r, dst_ref=r, send_sem=send_w.at[OUT], recv_sem=recv_z.at[p, place(j)],
            device_id={"sp": outer}, device_id_type=MESH)

    def across(stage, q, j, send=Y):
        r = piece(stage, q, g, j)
        return pltpu.make_async_remote_copy(
            src_ref=r, dst_ref=r, send_sem=send_w.at[send], recv_sem=recv_o.at[order_of(stage)],
            device_id={"grp": other}, device_id_type=MESH)

    def direct(stage, q):
        r = piece(stage, q, other, edge)
        return pltpu.make_async_remote_copy(
            src_ref=r, dst_ref=r, send_sem=send_w.at[UN], recv_sem=recv_o.at[order_of(stage)],
            device_id={"sp": inner}, device_id_type=MESH)

    def others_arrived(stage):
        layer, kind = stage
        per = depth if kind == "vg" else out_rows
        ref = wvg if kind == "vg" else wo
        wait_bytes(ref.at[layer, 0, pl.ds(0, (n - 1) * per)], recv_o.at[order_of(stage)])

    def end_rows(c, target):
        src = pl.ds(pl.multiple_of(PAD + c * x_rows, PAD), x_rows)
        return pltpu.make_async_remote_copy(
            src_ref=xg.at[0, t, src], dst_ref=xg.at[L, t, src], send_sem=f_sem.at[0], recv_sem=f_sem.at[2 + c],
            device_id={"sp": target}, device_id_type=MESH)

    def end_glu(target):
        return pltpu.make_async_remote_copy(
            src_ref=glu_out, dst_ref=pad.at[0], send_sem=f_sem.at[1], recv_sem=f_sem.at[2 + x_chunks],
            device_id={"sp": target}, device_id_type=MESH)

    def each(low_, high_, body):
        def step(q, carry):
            body(q)
            return carry
        lax.fori_loop(low_, high_, step, 0)

    def from_inner(stage, q, j):
        def serve():
            arrived(stage, q, j)
            if stage != first_vg:
                @pl.when(is_mid)
                def _():
                    outward(stage, q, j).start()
            across(stage, q, j).start()
        if stage == first_vg:
            pl.when(is_mid)(serve)
        else:
            serve()

    def from_edge(stage, q):
        @pl.when(is_mid)
        def _():
            arrived(stage, q, edge)
            inward(stage, q, edge).start()
            if stage == first_vg:
                @pl.when(q >= shared_from)
                def _():
                    across(stage, q, edge, YE).start()

    def push_in(stage, lo, hi):
        @pl.when(is_mid)
        def _():
            each(lo, hi, lambda q: inward(stage, q, mine).start())

    class Spread:
        def __init__(self, view, three, two, sems):
            self.view, self.three, self.two, self.sems = view, three, two, sems

        def copy(self, j, bit, k):
            block = self.view(j)
            return pltpu.make_async_remote_copy(
                src_ref=block, dst_ref=block, send_sem=self.sems(2), recv_sem=self.sems(k),
                device_id={"tp": t ^ bit}, device_id_type=MESH)

        def begin(self):
            self.copy(t, T // 2, 0).start()
            self.copy(t, 1, 1).start()

        def relay(self):
            wait_bytes(self.view(t), self.sems(0))
            self.copy(t ^ (T // 2), 1, 1).start()

        def complete(self):
            wait_bytes(self.two, self.sems(1))

        def drain(self):
            wait_bytes(self.three, self.sems(2))

    def x_spread(layer):
        return Spread(lambda j: xg.at[layer, j, own], xg.at[layer, pl.ds(0, 3), own], xg.at[layer, pl.ds(0, 2), own],
                      lambda k: x_sem.at[layer, k])

    def edge_spread(c):
        part = pl.ds(pl.multiple_of(PAD + c * x_rows, PAD), x_rows)
        return Spread(lambda j: xg.at[L, j, part], xg.at[L, pl.ds(0, 3), part], xg.at[L, pl.ds(0, 2), part],
                      lambda k: e_sem.at[c, k])

    def halo_spread(layer, side):
        part = pl.ds(0 if side == 0 else PAD + rows, PAD)
        return Spread(lambda j: xg.at[layer, j, part], xg.at[layer, pl.ds(0, 3), part], xg.at[layer, pl.ds(0, 2), part],
                      lambda k: hs_sem.at[layer, side, k])

    def conv_spread(layer, part_):
        part = pl.ds(part_ * (rows // 2), rows // 2)
        return Spread(lambda j: convg.at[layer, j, part], convg.at[layer, pl.ds(0, 3), part],
                      convg.at[layer, pl.ds(0, 2), part], lambda k: c_sem.at[layer, part_, k])

    def to_peers(buf, sem, k):
        for d in range(1, T):
            pltpu.make_async_remote_copy(
                src_ref=buf.at[0], dst_ref=buf.at[d], send_sem=sem.at[k], recv_sem=sem.at[k + 1],
                device_id={"tp": lax.rem(t + d, T)}, device_id_type=MESH).start()

    def columns_of(index_):
        wait_bytes(stat.at[index_, pl.ds(0, T - 1)], s_sem.at[2 * index_ + 1])
        got = jnp.concatenate([stat[index_, d] for d in range(T)] + [jnp.zeros((128 - 8 * T, rows), f32)], axis=0)
        return got.T

    def share(index_, columns):
        lane = lax.broadcasted_iota(jnp.int32, (rows, 128), 1)
        tile = jnp.zeros((rows, 128), f32)
        for i, column in enumerate(columns):
            tile = jnp.where(lane == i, column, tile)
        stat[index_, 0] = tile.T[:8, :]
        to_peers(stat.at[index_], s_sem, 2 * index_)

    def normalize(layer, held, into, start, size_):
        def squares(j, total):
            part = xg[held, j, start:start + size_, :].astype(f32)
            return total + jnp.sum(part * part, axis=1, keepdims=True)
        mean = lax.fori_loop(0, T, squares, jnp.zeros((size_, 1), f32)) / D
        scale = lax.rsqrt(mean + 1e-06)

        def body(j, carry):
            by = gain[pl.ds(layer, 1), pl.ds(pl.multiple_of(j * width, width), width)]
            xn[into, j, start:start + size_, :] = (
                xg[held, j, start:start + size_, :].astype(f32) * scale * by).astype(bf16)
            return carry
        lax.fori_loop(0, T, body, 0)

    def project(layer, held, start, size_, into):
        for h in range(G):
            def body(j, carry):
                block = wvg[layer, h, pl.ds(pl.multiple_of(j * width, width), width), :]
                part = jnp.dot(xn[held, j, start:start + size_, :], block, preferred_element_type=f32)

                @pl.when(j == 0)
                def _():
                    acc[start:start + size_, :] = part

                @pl.when(j > 0)
                def _():
                    acc[start:start + size_, :] += part
                return carry
            lax.fori_loop(0, T, body, 0)
            glu = acc[start:start + size_, :half] * jax.nn.sigmoid(acc[start:start + size_, half:])
            into[start:start + size_, h * half:(h + 1) * half] = glu.astype(bf16)

    def x_right(layer):
        return pltpu.make_async_remote_copy(
            src_ref=xg.at[layer, t, pl.ds(rows, PAD)], dst_ref=xg.at[layer, t, pl.ds(0, PAD)],
            send_sem=h_sem.at[layer, 0], recv_sem=h_sem.at[layer, 2],
            device_id={"sp": s + 1}, device_id_type=MESH)

    def x_left(layer):
        return pltpu.make_async_remote_copy(
            src_ref=xg.at[layer, t, pl.ds(PAD, PAD)], dst_ref=xg.at[layer, t, pl.ds(PAD + rows, PAD)],
            send_sem=h_sem.at[layer, 1], recv_sem=h_sem.at[layer, 3],
            device_id={"sp": s - 1}, device_id_type=MESH)

    def sides_of(layer):
        if layer == 0:
            return s == 1, s == last - 1, s == last - 1, s == 1
        return s < last, s > 0, s > 0, s < last

    def halo(layer, do):
        sends_right, sends_left, from_left, from_right = sides_of(layer)
        if do == "send":
            pl.when(sends_right)(lambda: x_right(layer).start())
            pl.when(sends_left)(lambda: x_left(layer).start())
        elif do == "begin":
            @pl.when(from_left)
            def _():
                wait_bytes(xg.at[layer, t, pl.ds(0, PAD)], h_sem.at[layer, 2])
                halo_spread(layer, 0).begin()

            @pl.when(from_right)
            def _():
                wait_bytes(xg.at[layer, t, pl.ds(0, PAD)], h_sem.at[layer, 3])
                halo_spread(layer, 1).begin()
        elif do == "drain":
            @pl.when(sends_right)
            def _():
                wait_bytes(xg.at[layer, t, pl.ds(0, PAD)], h_sem.at[layer, 0])

            @pl.when(sends_left)
            def _():
                wait_bytes(xg.at[layer, t, pl.ds(0, PAD)], h_sem.at[layer, 1])
            pl.when(from_left)(lambda: halo_spread(layer, 0).drain())
            pl.when(from_right)(lambda: halo_spread(layer, 1).drain())
        else:
            pl.when(from_left)(lambda: getattr(halo_spread(layer, 0), do)())
            pl.when(from_right)(lambda: getattr(halo_spread(layer, 1), do)())

    def convolve(layer):
        padf[...] = pad[layer].astype(f32)
        block = 64
        sums, squares = [], []
        for r in range(0, rows, block):
            total = jnp.zeros((block, chans), f32)
            for k in range(n_taps):
                start = r + PAD - reach + k
                total = total + taps[k, layer:layer + 1, :] * padf[start:start + block, :]
            mean = jnp.sum(total, axis=1, keepdims=True) / chans
            shifted = total - mean
            convg[layer, t, r:r + block, :] = shifted.astype(bf16)
            sums.append(mean)
            squares.append(jnp.sum(shifted * shifted, axis=1, keepdims=True))
            if r + block == rows // 2:
                conv_spread(layer, 0).begin()
        share(layer, [jnp.concatenate(sums, 0), jnp.concatenate(squares, 0)])
        conv_spread(layer, 1).begin()

    def add_branch(layer):
        got = columns_of(layer)
        means = [got[:, 8 * d:8 * d + 1] for d in range(T)]
        center = sum(means[1:], means[0]) / T
        apart = [m - center for m in means]
        square = sum((got[:, 8 * d + 1:8 * d + 2] + chans * (apart[d] * apart[d]) for d in range(T)), jnp.zeros((rows, 1), f32))
        scale = lax.rsqrt(square / C + 1e-05)
        parts = [None] * G
        for d in range(T):
            j = lax.rem(t + T - d, T)
            by = cgain[j, layer:layer + 1, :]
            normal = (convg[layer, j].astype(f32) + apart[d]) * scale
            act = jax.nn.silu(normal * by).astype(bf16)
            for h in range(G):
                block = wo[layer, h, pl.ds(pl.multiple_of(j * chans, chans), chans), :]
                term = jnp.dot(act, block, preferred_element_type=f32)
                parts[h] = term if parts[h] is None else parts[h] + term
        for h in range(G):
            cols = slice(h * out_half, (h + 1) * out_half)
            x_state[:, cols] = (x_state[:, cols] + parts[h]).astype(bf16).astype(f32)

    with scope("stage_wait"):
        staged(first_vg)
    token_copy.wait()
    halo(0, "send")
    each(0, QC, lambda q: inward(first_vg, q, s).start())

    @pl.when(is_end)
    def _():
        each(0, x_chunks, lambda c: end_rows(c, inner).start())

    @pl.when(is_mid)
    def _():
        x_spread(0).begin()

    with scope("stage_wait2"):
        for stage in after:
            staged(stage)

    def end_sends(what, stage, lo, hi):
        @pl.when(is_end)
        def _():
            if what == "in":
                each(lo, hi, lambda q: inward(stage, q, edge).start())
            else:
                each(lo, hi, lambda q: direct(stage, q).start())

    end_sends("direct", first_vg, 0, shared_from)

    @pl.when(is_mid)
    def _():
        for stage in after:
            each(0, count[stage[1]], lambda q: outward(stage, q, mine).start())

    gain_copy.wait()
    for c in small:
        c.wait()
    for d in range(1, T):
        pltpu.make_async_remote_copy(
            src_ref=cgain.at[t], dst_ref=cgain.at[t], send_sem=g_sem.at[0], recv_sem=g_sem.at[1],
            device_id={"tp": lax.rem(t + d, T)}, device_id_type=MESH).start()
    x_state[...] = xg[0, t, own, :].astype(f32)
    with scope("halo0_begin"):
        halo(0, "begin")

    def first_chunks(q):
        from_inner(first_vg, q, near)
        from_edge(first_vg, q)
    with scope("A_vg0_near_edge"):
        each(0, QC, first_chunks)
    push_in(first_wo, 0, RC)
    push_in(second_vg, 0, QC // 2)

    @pl.when(is_end)
    def _():
        def pass_on(stage):
            def body(q):
                arrived(stage, q, mine)
                across(stage, q, mine).start()
            each(0, count[stage[1]], body)
        for stage in after:
            with scope("end_pass_on"):
                pass_on(stage)
            if stage == first_wo:
                end_sends("in", first_wo, 0, RC)
                end_sends("direct", first_wo, 0, RC)
            elif stage == second_vg:
                end_sends("in", second_vg, 0, QC // 2)

    halo(0, "relay")
    @pl.when(is_mid)
    def _():
        with scope("x0_finish"):
            x_spread(0).relay()
            x_spread(0).complete()
    halo(0, "complete")

    @pl.when(is_mid)
    def _():
        with scope("norm0"):
            normalize(0, 0, 0, 0, full)

    def second_chunks(q):
        from_inner(first_vg, q, far)

        @pl.when(is_mid)
        def _():
            wait_bytes(xg.at[0, t, pl.ds(0, x_rows)], f_sem.at[2 + q])
            edge_spread(q).begin()

            @pl.when(q > 0)
            def _():
                edge_spread(q - 1).relay()
    with scope("B_vg0_far"):
        each(0, QC, second_chunks)

    @pl.when(is_mid)
    def _():
        with scope("edge_spread"):
            edge_spread(x_chunks - 1).relay()
            each(0, x_chunks - 1, lambda c: edge_spread(c).complete())
    with scope("C1_wo0_near"):
        from_inner(first_wo, 0, near)
    end_sends("in", second_vg, QC // 2, QC)

    @pl.when(is_mid)
    def _():
        with scope("edge_spread"):
            edge_spread(x_chunks - 1).complete()
        with scope("norm_e"):
            normalize(0, L, 1, PAD, rows)

    with scope("C1_wo0_near"):
        each(1, RC, lambda q: from_inner(first_wo, q, near))

    @pl.when(is_mid)
    def _():
        with scope("wait_vg0"):
            others_arrived(first_vg)
        with scope("proj0e"):
            project(0, 1, PAD, rows, glu_out)

    with scope("C2_wo0_edge"):
        each(0, RC, lambda q: from_edge(first_wo, q))
    push_in(second_vg, QC // 2, QC)
    with scope("D1_vg1_near"):
        from_inner(second_vg, 0, near)
    end_sends("direct", second_vg, 0, QC // 2)

    @pl.when(is_mid)
    def _():
        with scope("proj0"):
            project(0, 0, 0, full, pad.at[0])

    sends_right, sends_left, _, _ = sides_of(0)

    @pl.when(sends_right)
    def _():
        glu_out[0:PAD, :] = jnp.zeros((PAD, chans), bf16)
        glu_out[PAD + rows:, :] = pad[0, PAD:2 * PAD, :]
        pad[0, 0:PAD, :] = glu_out[rows:rows + PAD, :]

    @pl.when(sends_left)
    def _():
        glu_out[0:PAD, :] = pad[0, rows:rows + PAD, :]
        glu_out[PAD + rows:, :] = jnp.zeros((PAD, chans), bf16)
        pad[0, PAD + rows:, :] = glu_out[PAD:2 * PAD, :]

    @pl.when(is_mid)
    def _():
        end_glu(edge).start()

    with scope("C3_wo0_far"):
        from_inner(first_wo, 0, far)

    @pl.when(is_end)
    def _():
        with scope("end_glu_wait"):
            wait_bytes(glu_out, f_sem.at[2 + x_chunks])
    with scope("conv0"):
        convolve(0)
    with scope("C3_wo0_far"):
        each(1, RC, lambda q: from_inner(first_wo, q, far))
    with scope("D2_vg1_near"):
        from_inner(second_vg, 1, near)
    with scope("D2_vg1_edge"):
        from_edge(second_vg, 0)
    with scope("conv0_relay"):
        conv_spread(0, 0).relay()
        conv_spread(0, 1).relay()
    with scope("D2_vg1_near"):
        from_inner(second_vg, QC // 2, near)
    with scope("conv0_complete"):
        conv_spread(0, 0).complete()
        conv_spread(0, 1).complete()
        wait_bytes(cgain.at[pl.ds(0, T - 1)], g_sem.at[1])
    with scope("wait_wo0"):
        others_arrived(first_wo)
    with scope("out0"):
        add_branch(0)
    xg[1, t, own, :] = x_state[...].astype(bf16)
    x_spread(1).begin()
    halo(1, "send")
    end_sends("in", second_wo, 0, RC)
    end_sends("direct", second_vg, QC // 2, QC)
    end_sends("direct", second_wo, 0, RC)
    with scope("D3_vg1_edge"):
        each(1, QC // 2, lambda q: from_edge(second_vg, q))
    with scope("D3_vg1_near"):
        each(QC // 2 + 1, QC, lambda q: from_inner(second_vg, q, near))
    with scope("D3_vg1_edge"):
        each(QC // 2, QC, lambda q: from_edge(second_vg, q))
    push_in(second_wo, 0, RC)
    with scope("D4_vg1_far"):
        each(0, QC // 2, lambda q: from_inner(second_vg, q, far))
    with scope("halo1_begin"):
        halo(1, "begin")
    with scope("D4_vg1_far"):
        each(QC // 2, QC, lambda q: from_inner(second_vg, q, far))
    with scope("x1_relay"):
        x_spread(1).relay()
    with scope("E1_wo1_near"):
        each(0, RC, lambda q: from_inner(second_wo, q, near))
    with scope("halo1_relay"):
        halo(1, "relay")
    with scope("E1_wo1_edge"):
        from_edge(second_wo, 0)
    with scope("x1_complete"):
        x_spread(1).complete()
        halo(1, "complete")
    with scope("norm1"):
        normalize(1, 1, 0, 0, full)
    with scope("E1_wo1_edge"):
        each(1, RC, lambda q: from_edge(second_wo, q))
    with scope("wait_vg1"):
        others_arrived(second_vg)
    with scope("proj1"):
        project(1, 0, 0, full, pad.at[1])
    with scope("E2_wo1_far"):
        from_inner(second_wo, 0, far)
    with scope("conv1"):
        convolve(1)
    with scope("E3_wo1_far"):
        each(1, RC, lambda q: from_inner(second_wo, q, far))
    with scope("conv1_gather"):
        conv_spread(1, 0).relay()
        conv_spread(1, 1).relay()
        conv_spread(1, 0).complete()
        conv_spread(1, 1).complete()
    with scope("wait_wo1"):
        others_arrived(second_wo)
    with scope("out1"):
        add_branch(1)
    xf = x_state[...]
    share(L, [jnp.sum(xf * xf, axis=1, keepdims=True)])

    halo(0, "drain")
    halo(1, "drain")
    for layer in range(L):
        for part_ in range(2):
            conv_spread(layer, part_).drain()
    x_spread(1).drain()
    wait_bytes(cgain.at[pl.ds(0, T - 1)], g_sem.at[0])
    chunk_rows = size["vg"]
    stages = L * pieces
    later = stages - QC

    def sent(chunks, k):
        wait_bytes(wvg.at[0, 0, pl.ds(0, chunks * chunk_rows)], send_w.at[k])

    def sent_twice(chunks, k):
        wait_bytes(wvg.at[0, :, pl.ds(0, chunks * chunk_rows)], send_w.at[k])

    def sent_all(k):
        sent_twice(later * (n - 1) // G, k)

    @pl.when(is_mid)
    def _():
        x_spread(0).drain()
        each(0, x_chunks, lambda c: edge_spread(c).drain())
        wait_bytes(glu_out, f_sem.at[1])
        sent_twice(stages, IN)
        sent_all(OUT)
        sent(QC - shared_from, YE)
        sent_twice(later + QC, Y)

    @pl.when(is_end)
    def _():
        wait_bytes(xg.at[0, t, own], f_sem.at[0])
        sent(stages, IN)
        sent(later + shared_from, UN)
        sent_all(Y)

    with scope("final_stat"):
        got = columns_of(L)
        for index_ in range(L + 1):
            wait_bytes(stat.at[index_, pl.ds(0, T - 1)], s_sem.at[2 * index_])
    total = sum((got[:, 8 * d:8 * d + 1] for d in range(1, T)), got[:, 0:1])
    scale = lax.rsqrt(total / D + 1e-06)
    result[...] = (x_state[...] * scale * fgain[...]).astype(bf16)


def quad_on_device(G, n, T, tokens, norm_gain, value_w, gate_w, taps, cgain, out_w, fgain):
    L = norm_gain.shape[0]
    if L != 2:
        return on_device(G, n, T, tokens, norm_gain, value_w, gate_w, taps, cgain, out_w, fgain)
    rows, width = tokens.shape
    depth, chans = value_w.shape[1:]
    D, C = width * T, chans * T
    bf16, f32 = jnp.bfloat16, jnp.float32
    dma = pltpu.SemaphoreType.DMA
    vmem = pl.BlockSpec(memory_space=pltpu.VMEM)
    hbm = pl.BlockSpec(memory_space=pl.ANY)
    full = rows + 2 * PAD
    return pl.pallas_call(
        functools.partial(quad_kernel, G, n, T, L),
        out_shape=jax.ShapeDtypeStruct((rows, width), bf16),
        in_specs=[hbm] * 8,
        out_specs=vmem,
        scratch_shapes=[
            pltpu.VMEM((L, G, D, 2 * chans // G), bf16),
            pltpu.VMEM((L, G, C, width // G), bf16),
            pltpu.VMEM((L + 1, T, full, width), bf16),
            pltpu.VMEM((2, T, full, width), bf16),
            pltpu.VMEM((full, chans), bf16),
            pltpu.VMEM((full, 2 * chans // G), f32),
            pltpu.VMEM((L, full, chans), bf16),
            pltpu.VMEM((full, chans), f32),
            pltpu.VMEM((L, T, rows, chans), bf16),
            pltpu.VMEM((L + 1, T, 8, rows), f32),
            pltpu.VMEM((rows, width), f32),
            pltpu.VMEM(norm_gain.shape, f32),
            pltpu.VMEM((taps.shape[1], L, chans), f32),
            pltpu.VMEM((T,) + cgain.shape, f32),
            pltpu.VMEM((1, width), f32),
            dma((2 * L + 5,)),
            dma((L * (QC + RC), 3)), dma((2 * L,)), dma((5,)),
            dma((L, 3)), dma((QC, 3)), dma((L, 2, 3)), dma((2 * (L + 1),)),
            dma((L, 4)), dma((L, 2, 3)), dma((2,)), dma((QC + 3,)),
        ],
        compiler_params=pltpu.CompilerParams(
            collective_id=0, has_side_effects=True, vmem_limit_bytes=56 * 2**20
        ),
    )(tokens, norm_gain, value_w, gate_w, taps.transpose(1, 0, 2), cgain, out_w, fgain.reshape(1, width))


def tokens_f32(tokens, xg, t):
    return xg[0, t].astype(jnp.float32)


def on_device(G, n, T, tokens, norm_gain, value_w, gate_w, taps, cgain, out_w, fgain):
    L = norm_gain.shape[0]
    rows, width = tokens.shape
    depth, chans = value_w.shape[1:]
    D, C = width * T, chans * T
    bf16, f32 = jnp.bfloat16, jnp.float32
    dma = pltpu.SemaphoreType.DMA
    vmem = pl.BlockSpec(memory_space=pltpu.VMEM)
    hbm = pl.BlockSpec(memory_space=pl.ANY)
    P_ = L * (Q + 1)
    peers = max(G - 1, 1)
    return pl.pallas_call(
        functools.partial(kernel, G, n, T, L),
        out_shape=jax.ShapeDtypeStruct((rows, width), bf16),
        in_specs=[hbm, vmem, hbm, hbm, vmem, vmem, hbm, vmem],
        out_specs=vmem,
        scratch_shapes=[
            pltpu.VMEM((L, G, D, 2 * chans // G), bf16),
            pltpu.VMEM((L, G, C, width // G), bf16),
            pltpu.VMEM((L + 1, T, rows, width), bf16),
            pltpu.VMEM((2, T, rows, width), bf16),
            pltpu.VMEM((rows, chans), bf16),
            pltpu.VMEM((rows, 2 * chans // G), f32),
            pltpu.VMEM((L, rows + 2 * PAD, chans), bf16),
            pltpu.VMEM((rows + 2 * PAD, chans), f32),
            pltpu.VMEM((rows, chans), f32),
            pltpu.VMEM((L + 1, T, 8, rows), f32),
            pltpu.VMEM((L, T, rows, chans), bf16),
            pltpu.VMEM((rows, width), f32),
            dma((1 + L * G * 3,)),
            dma((P_, n)), dma((P_, n)), dma((P_, n)),
            dma((P_, n, peers)), dma((P_, n, peers)),
            dma((L + 1, T)), dma((L + 1, T)), dma((L, T)), dma((L, T)),
            dma((L + 1, T)), dma((L + 1, T)),
            dma((L, 2)), dma((L, 2)),
            dma((G + 1,)), dma((G + 1,)),
        ],
        compiler_params=pltpu.CompilerParams(
            collective_id=0, has_side_effects=True, vmem_limit_bytes=56 * 2**20
        ),
    )(tokens, norm_gain.reshape(L * T, width), value_w, gate_w, taps, cgain, out_w, fgain.reshape(1, width))


def solution(mesh):
    placed = (
        P(("grp", "sp"), "tp"),
        P(),
        P(None, "sp", "tp"),
        P(None, "sp", "tp"),
        P(None, None, "tp"),
        P(None, "tp"),
        P(None, "sp", "tp"),
        P("tp"),
    )
    G, n, T = (mesh.shape[a] for a in ("grp", "sp", "tp"))
    paired = G == 2 and n == T == 2 * G
    return jax.shard_map(
        functools.partial(quad_on_device if paired else on_device, G, n, T),
        mesh=mesh, in_specs=placed, out_specs=P(("grp", "sp"), "tp"), check_vma=False,
    )
```

```python
import functools

import jax
import jax.numpy as jnp
from jax import lax
from jax.experimental import pallas as pl
from jax.experimental.pallas import tpu as pltpu
from jax.sharding import PartitionSpec as P

MESH = pl.DeviceIdType.MESH
Q = 2
PAD = 16


def kernel(
    G, n, T, L,
    tokens, gain, value_w, gate_w, taps, cgain, out_w, fgain,
    result,
    wvg, wo, xg, xn, glu_out, acc, pad, padf, conv, stat, actg, x_state,
    local_sem, z_recv, right_send, left_send, y_send, y_recv,
    x_send, x_recv, a_send, a_recv, s_send, s_recv, h_send, h_recv, f_send, f_recv,
):
    g, s, t = lax.axis_index("grp"), lax.axis_index("sp"), lax.axis_index("tp")
    rows, width = tokens.shape
    depth, chans = value_w.shape[1:]
    out_rows = out_w.shape[1]
    half = chans // G
    out_half = width // G
    reach = taps.shape[1] // 2
    n_taps = taps.shape[1]
    D = width * T
    C = chans * T
    chunk = depth // Q
    pieces = Q + 1
    f32, bf16 = jnp.float32, jnp.bfloat16
    helped = n >= 4
    last = n - 1
    is_end = (s == 0) | (s == last)
    helper = (s == 1) | (s == last - 1)
    end = jnp.where(s == 1, 0, last)
    inward = jnp.where(s == 0, 1, last - 1)

    def ends_out(p):
        return helped and p < Q

    def to_right_ok(p):
        return s < last - 1 if ends_out(p) else s < last

    def to_left_ok(p):
        return s > 1 if ends_out(p) else s > 0

    def takes(p):
        return jnp.logical_not(is_end) if ends_out(p) else s >= 0

    def by_grp(p, j):
        ok = takes(p) & (j != s)
        if helped and p == 0:
            ok = ok & jnp.logical_not((s == 1) & (j == 0)) & jnp.logical_not((s == last - 1) & (j == last))
        return ok

    def piece(p, h, j):
        layer, q = p // pieces, p % pieces
        if q < Q:
            start = pl.multiple_of(j * depth + q * chunk, chunk)
            return wvg.at[layer, h, pl.ds(start, chunk), :]
        return wo.at[layer, h, pl.ds(pl.multiple_of(j * out_rows, out_rows), out_rows), :]

    locals_ = [pltpu.make_async_copy(tokens, xg.at[0, t], local_sem.at[0])]
    own_rows = pl.ds(pl.multiple_of(s * depth, depth), depth)
    own_out = pl.ds(pl.multiple_of(s * out_rows, out_rows), out_rows)
    count = 1
    per_layer = []
    for layer in range(L):
        group = []
        for h in range(G):
            for k, w in enumerate((value_w, gate_w)):
                group.append(pltpu.make_async_copy(
                    w.at[layer, :, pl.ds(h * half, half)],
                    wvg.at[layer, h, own_rows, pl.ds(k * half, half)],
                    local_sem.at[count]))
                count += 1
            group.append(pltpu.make_async_copy(
                out_w.at[layer, :, pl.ds(h * out_half, out_half)],
                wo.at[layer, h, own_out, :], local_sem.at[count]))
            count += 1
        per_layer.append(group)
    for c in locals_ + sum(per_layer, []):
        c.start()

    barrier = pltpu.get_barrier_semaphore()
    for d in range(1, T):
        pl.semaphore_signal(barrier, inc=1, device_id={"tp": lax.rem(t + d, T)}, device_id_type=MESH)
    for d in range(1, G):
        pl.semaphore_signal(barrier, inc=1, device_id={"grp": lax.rem(g + d, G)}, device_id_type=MESH)

    @pl.when(s > 0)
    def _():
        pl.semaphore_signal(barrier, inc=1, device_id={"sp": s - 1}, device_id_type=MESH)

    @pl.when(s < n - 1)
    def _():
        pl.semaphore_signal(barrier, inc=1, device_id={"sp": s + 1}, device_id_type=MESH)

    sides = jnp.where(s > 0, 1, 0) + jnp.where(s < n - 1, 1, 0)
    pl.semaphore_wait(barrier, (T - 1) + (G - 1) + sides)

    def right(p, j):
        r = piece(p, g, j)
        return pltpu.make_async_remote_copy(
            src_ref=r, dst_ref=r, send_sem=right_send.at[p, j], recv_sem=z_recv.at[p, j],
            device_id={"sp": s + 1}, device_id_type=MESH)

    def left(p, j):
        r = piece(p, g, j)
        return pltpu.make_async_remote_copy(
            src_ref=r, dst_ref=r, send_sem=left_send.at[p, j], recv_sem=z_recv.at[p, j],
            device_id={"sp": s - 1}, device_id_type=MESH)

    def across(p, j, d, h):
        r = piece(p, h, j)
        return pltpu.make_async_remote_copy(
            src_ref=r, dst_ref=r, send_sem=y_send.at[p, j, d - 1], recv_sem=y_recv.at[p, j, d - 1],
            device_id={"grp": lax.rem(g + d, G)}, device_id_type=MESH)

    batches = []
    for layer in range(L):
        base = layer * pieces
        batches += [list(range(base, base + Q)), [base + Q]]

    def own_right(ps):
        for p in ps:
            right(p, s).start()

    def own_left(ps):
        for p in ps:
            left(p, s).start()

    def end_rows(target):
        return pltpu.make_async_remote_copy(
            src_ref=xg.at[0, t], dst_ref=xg.at[L, t], send_sem=f_send.at[0], recv_sem=f_recv.at[0],
            device_id={"sp": target}, device_id_type=MESH)

    def end_piece(d, h, j, target):
        r = piece(0, h, j)
        return pltpu.make_async_remote_copy(
            src_ref=r, dst_ref=r, send_sem=f_send.at[d], recv_sem=f_recv.at[d],
            device_id={"sp": target}, device_id_type=MESH)

    def end_glu(target):
        return pltpu.make_async_remote_copy(
            src_ref=glu_out, dst_ref=pad.at[0, pl.ds(PAD, rows), :],
            send_sem=f_send.at[G], recv_sem=f_recv.at[G],
            device_id={"sp": target}, device_id_type=MESH)

    def relay(b, low, high):
        low, high = min(low, n - 1), min(high, n - 1)
        following = batches[b + 1] if b + 1 < len(batches) else []

        def step(k, carry):
            for p in batches[b]:
                from_left, from_right = s - 1 - k, s + 1 + k

                @pl.when((from_left >= 0) & takes(p))
                def _():
                    j = jnp.maximum(from_left, 0)
                    right(p, j).wait_recv()

                    @pl.when(to_right_ok(p))
                    def _():
                        right(p, j).start()

                    @pl.when(by_grp(p, j))
                    def _():
                        for d in range(1, G):
                            across(p, j, d, g).start()

                @pl.when((from_right < n) & takes(p))
                def _():
                    j = jnp.minimum(from_right, n - 1)
                    left(p, j).wait_recv()

                    @pl.when(to_left_ok(p))
                    def _():
                        left(p, j).start()

                    @pl.when(by_grp(p, j))
                    def _():
                        for d in range(1, G):
                            across(p, j, d, g).start()

            @pl.when((k == s - 1) & (s < (last - 1 if helped and b < 2 else last)))
            def _():
                own_right(following)

            @pl.when((k == n - 2 - s) & (s > (1 if helped and b < 2 else 0)))
            def _():
                own_left(following)

            return carry

        if high > low:
            lax.fori_loop(low, high, step, 0)

    def wait_across(b):
        for p in batches[b]:
            def step(j, carry):
                @pl.when(by_grp(p, j))
                def _():
                    for d in range(1, G):
                        across(p, j, d, lax.rem(g + G - d, G)).wait_recv()
                return carry
            lax.fori_loop(0, n, step, 0)

    def spread(buf, layer, send, recv):
        def copy(bit, m):
            block = buf.at[layer, t ^ m]
            return pltpu.make_async_remote_copy(
                src_ref=block, dst_ref=block, send_sem=send.at[layer, bit + m], recv_sem=recv.at[layer, bit + m],
                device_id={"tp": t ^ bit}, device_id_type=MESH)

        def arrival(bit, m):
            block = buf.at[layer, t ^ bit ^ m]
            return pltpu.make_async_remote_copy(
                src_ref=block, dst_ref=block, send_sem=send.at[layer, bit + m], recv_sem=recv.at[layer, bit + m],
                device_id={"tp": t ^ bit}, device_id_type=MESH)

        bits = []
        bit = T // 2
        while bit >= 1:
            bits.append(bit)
            bit //= 2

        def begin():
            for bit in bits:
                copy(bit, 0).start()

        def finish():
            have, sent = [0], []
            for i, bit in enumerate(bits):
                for m in have:
                    arrival(bit, m).wait_recv()
                    sent.append((bit, m))
                    for lower in bits[i + 1:]:
                        copy(lower, m ^ bit).start()
                have = have + [m ^ bit for m in have]
            return lambda: [copy(bit, m).wait_send() for bit, m in sent]

        return begin, finish

    def exchange(index, columns):
        lane = lax.broadcasted_iota(jnp.int32, (rows, 128), 1)
        tile = jnp.zeros((rows, 128), f32)
        for i, column in enumerate(columns):
            tile = jnp.where(lane == i, column, tile)
        stat[index, 0] = tile.T[:8, :]

        def copy(d):
            return pltpu.make_async_remote_copy(
                src_ref=stat.at[index, 0], dst_ref=stat.at[index, d],
                send_sem=s_send.at[index, d - 1], recv_sem=s_recv.at[index, d - 1],
                device_id={"tp": lax.rem(t + d, T)}, device_id_type=MESH)

        for d in range(1, T):
            copy(d).start()

        def total():
            for d in range(1, T):
                copy(d).wait_recv()
            sums = stat[index, 0]
            for d in range(1, T):
                sums = sums + stat[index, d]
            wide = jnp.concatenate([sums, jnp.zeros((120, rows), f32)], axis=0).T
            for d in range(1, T):
                copy(d).wait_send()
            return [wide[:, i:i + 1] for i in range(len(columns))]

        return total

    def normalize(layer, held, into):
        def squares(j, total):
            part = xg[held, j].astype(f32)
            return total + jnp.sum(part * part, axis=1, keepdims=True)
        mean = lax.fori_loop(0, T, squares, jnp.zeros((rows, 1), f32)) / D
        scale = lax.rsqrt(mean + 1e-06)

        def body(j, carry):
            xn[into, j] = (xg[held, j].astype(f32) * scale * gain[layer * T + j][None, :]).astype(bf16)
            return carry
        lax.fori_loop(0, T, body, 0)

    def project(layer, held, put):
        for h in range(G):
            def body(j, carry):
                block = wvg[layer, h, pl.ds(pl.multiple_of(j * width, width), width), :]
                part = jnp.dot(xn[held, j], block, preferred_element_type=f32)

                @pl.when(j == 0)
                def _():
                    acc[...] = part

                @pl.when(j > 0)
                def _():
                    acc[...] += part
                return carry
            lax.fori_loop(0, T, body, 0)
            glu = acc[:, :half] * jax.nn.sigmoid(acc[:, half:])
            put(h, glu.astype(bf16))

    for c in locals_:
        c.wait()
    spreads = [spread(xg, layer, x_send, x_recv) for layer in range(L)]
    spreads[0][0]()
    for c in sum(per_layer, []):
        c.wait()

    @pl.when(to_right_ok(0))
    def _():
        own_right(batches[0])

    @pl.when(to_left_ok(0))
    def _():
        own_left(batches[0])

    if helped:
        @pl.when(is_end)
        def _():
            end_rows(inward).start()
            for d in range(1, G):
                end_piece(d, lax.rem(g + d, G), s, inward).start()

        @pl.when(s == last - 1)
        def _():
            own_right(batches[1])
            if L > 1:
                own_right(batches[2])

        @pl.when(s == 1)
        def _():
            own_left(batches[1])
            if L > 1:
                own_left(batches[2])

    @pl.when((s == 0) & (s < n - 1))
    def _():
        for b in batches[1:]:
            own_right(b)

    @pl.when((s == n - 1) & (s > 0))
    def _():
        for b in batches[1:]:
            own_left(b)

    x_state[...] = tokens_f32(tokens, xg, t)
    drains = []

    for layer in range(L):
        first, second = 2 * layer, 2 * layer + 1
        if layer == 0:
            relay(first, 0, 1)
        else:
            relay(first, 1, 2)
        drains.append(spreads[layer][1]())
        if helped and layer == 0:
            @pl.when(jnp.logical_not(is_end))
            def _():
                normalize(layer, layer, 0)
        else:
            normalize(layer, layer, 0)
        relay(first, 1 if layer == 0 else 2, n)
        begin, finish = spread(xg, L, x_send, x_recv)
        if helped and layer == 0:
            @pl.when(helper)
            def _():
                end_rows(end).wait_recv()
                begin()

        relay(second, 0, 1)

        def put(h, value):
            pad[layer, PAD:PAD + rows, h * half:(h + 1) * half] = value

        def put_out(h, value):
            glu_out[:, h * half:(h + 1) * half] = value

        if helped and layer == 0:
            @pl.when(helper)
            def _():
                drain = finish()
                normalize(0, L, 1)
                for d in range(1, G):
                    end_piece(d, lax.rem(g + d, G), end, end).wait_recv()
                drain()

            wait_across(first)

            @pl.when(helper)
            def _():
                project(0, 1, put_out)
                end_glu(end).start()

            @pl.when(jnp.logical_not(is_end))
            def _():
                project(0, 0, put)

            @pl.when(helper)
            def _():
                end_glu(end).wait_send()

            @pl.when(is_end)
            def _():
                end_rows(inward).wait_send()
                for d in range(1, G):
                    end_piece(d, lax.rem(g + d, G), s, inward).wait_send()
                end_glu(inward).wait_recv()
        else:
            wait_across(first)
            project(layer, 0, put)

        def to_right():
            return pltpu.make_async_remote_copy(
                src_ref=pad.at[layer, pl.ds(rows, PAD), :], dst_ref=pad.at[layer, pl.ds(0, PAD), :],
                send_sem=h_send.at[layer, 0], recv_sem=h_recv.at[layer, 0],
                device_id={"sp": s + 1}, device_id_type=MESH)

        def to_left():
            return pltpu.make_async_remote_copy(
                src_ref=pad.at[layer, pl.ds(PAD, PAD), :], dst_ref=pad.at[layer, pl.ds(PAD + rows, PAD), :],
                send_sem=h_send.at[layer, 1], recv_sem=h_recv.at[layer, 1],
                device_id={"sp": s - 1}, device_id_type=MESH)

        @pl.when(s < n - 1)
        def _():
            to_right().start()

        @pl.when(s > 0)
        def _():
            to_left().start()

        @pl.when(s == 0)
        def _():
            pad[layer, 0:PAD, :] = jnp.zeros((PAD, chans), bf16)

        @pl.when(s == n - 1)
        def _():
            pad[layer, PAD + rows:, :] = jnp.zeros((PAD, chans), bf16)

        relay(second, 1, 2)

        @pl.when(s > 0)
        def _():
            to_right().wait_recv()

        @pl.when(s < n - 1)
        def _():
            to_left().wait_recv()

        padf[...] = pad[layer].astype(f32)
        block = 64
        sums, squares = [], []
        for r in range(0, rows, block):
            total = jnp.zeros((block, chans), f32)
            for k in range(n_taps):
                start = r + PAD - reach + k
                total = total + taps[layer, k][None, :] * padf[start:start + block, :]
            conv[r:r + block, :] = total
            sums.append(jnp.sum(total, axis=1, keepdims=True))
            squares.append(jnp.sum(total * total, axis=1, keepdims=True))
        totals = exchange(layer, [jnp.concatenate(sums, 0), jnp.concatenate(squares, 0)])
        relay(second, 2, n)
        if layer + 1 < L:
            relay(second + 1, 0, 1)
        total, square = totals()
        center = total / C
        spread_ = square / C - center * center
        normal = (conv[...] - center) * lax.rsqrt(spread_ + 1e-05)
        actg[layer, t] = jax.nn.silu(normal * cgain[layer][None, :]).astype(bf16)
        act_begin, act_finish = spread(actg, layer, a_send, a_recv)
        act_begin()
        drains.append(act_finish())
        wait_across(second)
        for h in range(G):
            part = None
            for j in range(T):
                term = jnp.dot(actg[layer, j], wo[layer, h, j * chans:(j + 1) * chans, :], preferred_element_type=f32)
                part = term if part is None else part + term
            cols = slice(h * out_half, (h + 1) * out_half)
            x_state[:, cols] = (x_state[:, cols] + part).astype(bf16).astype(f32)
        if layer + 1 < L:
            xg[layer + 1, t] = x_state[...].astype(bf16)
            spreads[layer + 1][0]()

        @pl.when(s < n - 1)
        def _():
            to_right().wait_send()

        @pl.when(s > 0)
        def _():
            to_left().wait_send()

    xf = x_state[...]
    totals = exchange(L, [jnp.sum(xf * xf, axis=1, keepdims=True)])

    for drain in drains:
        drain()

    def drain_step(j, carry):
        for p in range(L * pieces):
            came = (j == s) | takes(p)

            @pl.when((j <= s) & to_right_ok(p) & came)
            def _():
                right(p, j).wait_send()

            @pl.when((j >= s) & to_left_ok(p) & came)
            def _():
                left(p, j).wait_send()

            @pl.when(by_grp(p, j))
            def _():
                for d in range(1, G):
                    across(p, j, d, g).wait_send()
        return carry
    lax.fori_loop(0, n, drain_step, 0)

    (total,) = totals()
    scale = lax.rsqrt(total / D + 1e-06)
    result[...] = (x_state[...] * scale * fgain[...]).astype(bf16)


QC = 4
RC = 2


def quad_kernel(
    G, n, T, L,
    tokens, gain_hbm, value_w, gate_w, taps_hbm, cgain_hbm, out_w, fgain_hbm,
    result,
    wvg, wo, xg, xn, glu_out, acc, pad, padf, convg, act, stat, x_state, gain, taps, cgain, fgain,
    local_sem, recv_z, recv_o, send_w, x_sem, e_sem, c_sem, s_sem, h_sem, hs_sem, g_sem, f_sem,
):
    g, s, t = lax.axis_index("grp"), lax.axis_index("sp"), lax.axis_index("tp")
    rows, width = tokens.shape
    depth, chans = value_w.shape[1:]
    out_rows = out_w.shape[1]
    half = chans // G
    out_half = width // G
    n_taps = taps.shape[0]
    reach = n_taps // 2
    D = width * T
    C = chans * T
    full = rows + 2 * PAD
    pieces = QC + RC
    size = {"vg": depth // QC, "wo": out_rows // RC}
    count = {"vg": QC, "wo": RC}
    shared_from = QC - 1
    f32, bf16 = jnp.float32, jnp.bfloat16
    last = n - 1
    low = s < n // 2
    is_end = (s == 0) | (s == last)
    is_mid = jnp.logical_not(is_end)
    inner = jnp.where(low, s + 1, s - 1)
    outer = jnp.where(low, s - 1, s + 1)
    edge, mine, near, far = (jnp.where(low, a, last - a) for a in (0, 1, n - 2, n - 1))
    other = lax.rem(g + 1, G)
    x_chunks = QC
    x_rows = rows // x_chunks
    own = pl.ds(PAD, rows)
    first_vg, first_wo, second_vg, second_wo = (0, "vg"), (0, "wo"), (1, "vg"), (1, "wo")
    after = (first_wo, second_vg, second_wo)
    scope = jax.named_scope
    IN, OUT, Y, YE, UN = range(5)

    def index(stage, q):
        layer, kind = stage
        return layer * pieces + (0 if kind == "vg" else QC) + q

    def order_of(stage):
        return stage[0] * 2 + (0 if stage[1] == "vg" else 1)

    def place(j):
        return jnp.where(j == near, 1, jnp.where(j == far, 2, 0))

    def piece(stage, q, h, j):
        layer, kind = stage
        step = size[kind]
        per = depth if kind == "vg" else out_rows
        ref = wvg if kind == "vg" else wo
        return ref.at[layer, h, pl.ds(pl.multiple_of(j * per + q * step, step), step), :]

    def wait_bytes(ref, sem):
        pltpu.make_async_copy(ref, ref, sem).wait()

    own_rows = pl.ds(pl.multiple_of(s * depth, depth), depth)
    own_out = pl.ds(pl.multiple_of(s * out_rows, out_rows), out_rows)

    def stage_in(stage):
        layer, kind = stage
        sem = local_sem.at[order_of(stage)]
        for h in range(G):
            if kind == "vg":
                for k, w in enumerate((value_w, gate_w)):
                    pltpu.make_async_copy(
                        w.at[layer, :, pl.ds(h * half, half)],
                        wvg.at[layer, h, own_rows, pl.ds(k * half, half)], sem).start()
            else:
                pltpu.make_async_copy(
                    out_w.at[layer, :, pl.ds(h * out_half, out_half)],
                    wo.at[layer, h, own_out, :], sem).start()

    def staged(stage):
        layer, kind = stage
        ref = wvg.at[layer, :, own_rows] if kind == "vg" else wo.at[layer, :, own_out]
        wait_bytes(ref, local_sem.at[order_of(stage)])

    token_copy = pltpu.make_async_copy(tokens, xg.at[0, t, own], local_sem.at[2 * L])
    gain_copy = pltpu.make_async_copy(cgain_hbm, cgain.at[t], local_sem.at[2 * L + 1])
    small = [
        pltpu.make_async_copy(gain_hbm, gain, local_sem.at[2 * L + 2]),
        pltpu.make_async_copy(taps_hbm, taps, local_sem.at[2 * L + 3]),
        pltpu.make_async_copy(fgain_hbm, fgain, local_sem.at[2 * L + 4]),
    ]
    stage_in(first_vg)
    token_copy.start()
    gain_copy.start()
    for stage in after:
        stage_in(stage)
    for c in small:
        c.start()

    barrier = pltpu.get_barrier_semaphore()
    for d in range(1, T):
        pl.semaphore_signal(barrier, inc=1, device_id={"tp": lax.rem(t + d, T)}, device_id_type=MESH)
    pl.semaphore_signal(barrier, inc=1, device_id={"grp": other}, device_id_type=MESH)

    @pl.when(s > 0)
    def _():
        pl.semaphore_signal(barrier, inc=1, device_id={"sp": s - 1}, device_id_type=MESH)

    @pl.when(s < last)
    def _():
        pl.semaphore_signal(barrier, inc=1, device_id={"sp": s + 1}, device_id_type=MESH)

    blank = jnp.zeros((T, PAD, width), bf16)

    @pl.when(s < n // 2)
    def _():
        xg[0, :, 0:PAD, :] = blank

    @pl.when(s >= n // 2)
    def _():
        xg[0, :, PAD + rows:, :] = blank

    @pl.when(s == 0)
    def _():
        xg[1, :, 0:PAD, :] = blank

    @pl.when(s == last)
    def _():
        xg[1, :, PAD + rows:, :] = blank

    sides = jnp.where(s > 0, 1, 0) + jnp.where(s < last, 1, 0)
    pl.semaphore_wait(barrier, (T - 1) + (G - 1) + sides)

    def arrived(stage, q, j):
        wait_bytes(piece(stage, q, g, j), recv_z.at[index(stage, q), place(j)])

    def inward(stage, q, j):
        r, p = piece(stage, q, g, j), index(stage, q)
        there = jnp.where(is_end, 0, jnp.where(j == mine, 1, 2))
        return pltpu.make_async_remote_copy(
            src_ref=r, dst_ref=r, send_sem=send_w.at[IN], recv_sem=recv_z.at[p, there],
            device_id={"sp": inner}, device_id_type=MESH)

    def outward(stage, q, j):
        r, p = piece(stage, q, g, j), index(stage, q)
        return pltpu.make_async_remote_copy(
            src_ref=r, dst_ref=r, send_sem=send_w.at[OUT], recv_sem=recv_z.at[p, place(j)],
            device_id={"sp": outer}, device_id_type=MESH)

    def across(stage, q, j, send=Y):
        r = piece(stage, q, g, j)
        return pltpu.make_async_remote_copy(
            src_ref=r, dst_ref=r, send_sem=send_w.at[send], recv_sem=recv_o.at[order_of(stage)],
            device_id={"grp": other}, device_id_type=MESH)

    def direct(stage, q):
        r = piece(stage, q, other, edge)
        return pltpu.make_async_remote_copy(
            src_ref=r, dst_ref=r, send_sem=send_w.at[UN], recv_sem=recv_o.at[order_of(stage)],
            device_id={"sp": inner}, device_id_type=MESH)

    def others_arrived(stage):
        layer, kind = stage
        per = depth if kind == "vg" else out_rows
        ref = wvg if kind == "vg" else wo
        wait_bytes(ref.at[layer, 0, pl.ds(0, (n - 1) * per)], recv_o.at[order_of(stage)])

    def end_rows(c, target):
        src = pl.ds(pl.multiple_of(PAD + c * x_rows, PAD), x_rows)
        return pltpu.make_async_remote_copy(
            src_ref=xg.at[0, t, src], dst_ref=xg.at[L, t, src], send_sem=f_sem.at[0], recv_sem=f_sem.at[2 + c],
            device_id={"sp": target}, device_id_type=MESH)

    def end_glu(target):
        return pltpu.make_async_remote_copy(
            src_ref=glu_out, dst_ref=pad.at[0], send_sem=f_sem.at[1], recv_sem=f_sem.at[2 + x_chunks],
            device_id={"sp": target}, device_id_type=MESH)

    def each(low_, high_, body):
        def step(q, carry):
            body(q)
            return carry
        lax.fori_loop(low_, high_, step, 0)

    def from_inner(stage, q, j, over_y=True):
        def serve():
            with scope("w_inner"):
                arrived(stage, q, j)
            if stage != first_vg:
                @pl.when(is_mid)
                def _():
                    outward(stage, q, j).start()
            if over_y:
                across(stage, q, j).start()
        if stage == first_vg:
            pl.when(is_mid)(serve)
        else:
            serve()

    def from_edge(stage, q):
        @pl.when(is_mid)
        def _():
            with scope("w_edge"):
                arrived(stage, q, edge)
            inward(stage, q, edge).start()
            if stage == first_vg:
                @pl.when(q >= shared_from)
                def _():
                    across(stage, q, edge, YE).start()

    def push_in(stage, lo, hi):
        @pl.when(is_mid)
        def _():
            each(lo, hi, lambda q: inward(stage, q, mine).start())

    class Spread:
        def __init__(self, view, three, two, sems):
            self.view, self.three, self.two, self.sems = view, three, two, sems

        def copy(self, j, bit, k):
            block = self.view(j)
            return pltpu.make_async_remote_copy(
                src_ref=block, dst_ref=block, send_sem=self.sems(2), recv_sem=self.sems(k),
                device_id={"tp": t ^ bit}, device_id_type=MESH)

        def begin(self):
            self.copy(t, T // 2, 0).start()
            self.copy(t, 1, 1).start()

        def relay(self):
            wait_bytes(self.view(t), self.sems(0))
            self.copy(t ^ (T // 2), 1, 1).start()

        def complete(self):
            wait_bytes(self.two, self.sems(1))

        def drain(self):
            wait_bytes(self.three, self.sems(2))

    def half_columns(h):
        return pl.ds(pl.multiple_of(h * out_half, out_half), out_half)

    def x_spread():
        return Spread(lambda j: xg.at[0, j, own], xg.at[0, pl.ds(0, 3), own], xg.at[0, pl.ds(0, 2), own],
                      lambda k: x_sem.at[0, k])

    def half_spread(h, turn):
        cols = half_columns(h)
        return Spread(lambda j: xg.at[1, j, own, cols], xg.at[1, pl.ds(0, 3), own, cols],
                      xg.at[1, pl.ds(0, 2), own, cols], lambda k: x_sem.at[1 + turn, k])

    def edge_spread(c):
        part = pl.ds(pl.multiple_of(PAD + c * x_rows, PAD), x_rows)
        return Spread(lambda j: xg.at[L, j, part], xg.at[L, pl.ds(0, 3), part], xg.at[L, pl.ds(0, 2), part],
                      lambda k: e_sem.at[c, k])

    def halo_spread(layer, side):
        part = pl.ds(0 if side == 0 else PAD + rows, PAD)
        return Spread(lambda j: xg.at[layer, j, part], xg.at[layer, pl.ds(0, 3), part], xg.at[layer, pl.ds(0, 2), part],
                      lambda k: hs_sem.at[layer, side, k])

    def conv_spread(layer, part_):
        part = pl.ds(part_ * (rows // 2), rows // 2)
        return Spread(lambda j: convg.at[layer, j, part], convg.at[layer, pl.ds(0, 3), part],
                      convg.at[layer, pl.ds(0, 2), part], lambda k: c_sem.at[layer, part_, k])

    def to_peers(buf, sem, k):
        for d in range(1, T):
            pltpu.make_async_remote_copy(
                src_ref=buf.at[0], dst_ref=buf.at[d], send_sem=sem.at[k], recv_sem=sem.at[k + 1],
                device_id={"tp": lax.rem(t + d, T)}, device_id_type=MESH).start()

    def columns_of(index_):
        wait_bytes(stat.at[index_, pl.ds(0, T - 1)], s_sem.at[2 * index_ + 1])
        got = jnp.concatenate([stat[index_, d] for d in range(T)] + [jnp.zeros((128 - 8 * T, rows), f32)], axis=0)
        return got.T

    def share(index_, columns):
        lane = lax.broadcasted_iota(jnp.int32, (rows, 128), 1)
        tile = jnp.zeros((rows, 128), f32)
        for i, column in enumerate(columns):
            tile = jnp.where(lane == i, column, tile)
        stat[index_, 0] = tile.T[:8, :]
        to_peers(stat.at[index_], s_sem, 2 * index_)

    def normalize(layer, held, into, start, size_):
        def squares(j, total):
            part = xg[held, j, start:start + size_, :].astype(f32)
            return total + jnp.sum(part * part, axis=1, keepdims=True)
        mean = lax.fori_loop(0, T, squares, jnp.zeros((size_, 1), f32)) / D
        scale = lax.rsqrt(mean + 1e-06)

        def body(j, carry):
            by = gain[pl.ds(layer, 1), pl.ds(pl.multiple_of(j * width, width), width)]
            xn[into, j, start:start + size_, :] = (
                xg[held, j, start:start + size_, :].astype(f32) * scale * by).astype(bf16)
            return carry
        lax.fori_loop(0, T, body, 0)

    def project(layer, held, start, size_, into, h):
        def body(j, carry):
            block = wvg[layer, h, pl.ds(pl.multiple_of(j * width, width), width), :]
            part = jnp.dot(xn[held, j, start:start + size_, :], block, preferred_element_type=f32)

            @pl.when(j == 0)
            def _():
                acc[start:start + size_, :] = part

            @pl.when(j > 0)
            def _():
                acc[start:start + size_, :] += part
            return carry
        lax.fori_loop(0, T, body, 0)
        glu = acc[start:start + size_, :half] * jax.nn.sigmoid(acc[start:start + size_, half:])
        into[start:start + size_, pl.ds(pl.multiple_of(h * half, half), half)] = glu.astype(bf16)

    def x_right(layer):
        return pltpu.make_async_remote_copy(
            src_ref=xg.at[layer, t, pl.ds(rows, PAD)], dst_ref=xg.at[layer, t, pl.ds(0, PAD)],
            send_sem=h_sem.at[layer, 0], recv_sem=h_sem.at[layer, 2],
            device_id={"sp": s + 1}, device_id_type=MESH)

    def x_left(layer):
        return pltpu.make_async_remote_copy(
            src_ref=xg.at[layer, t, pl.ds(PAD, PAD)], dst_ref=xg.at[layer, t, pl.ds(PAD + rows, PAD)],
            send_sem=h_sem.at[layer, 1], recv_sem=h_sem.at[layer, 3],
            device_id={"sp": s - 1}, device_id_type=MESH)

    def sides_of(layer):
        if layer == 0:
            return s == 1, s == last - 1, s == last - 1, s == 1
        return s < last, s > 0, s > 0, s < last

    def halo(layer, do):
        sends_right, sends_left, from_left, from_right = sides_of(layer)
        if do == "send":
            pl.when(sends_right)(lambda: x_right(layer).start())
            pl.when(sends_left)(lambda: x_left(layer).start())
        elif do == "begin":
            @pl.when(from_left)
            def _():
                wait_bytes(xg.at[layer, t, pl.ds(0, PAD)], h_sem.at[layer, 2])
                halo_spread(layer, 0).begin()

            @pl.when(from_right)
            def _():
                wait_bytes(xg.at[layer, t, pl.ds(0, PAD)], h_sem.at[layer, 3])
                halo_spread(layer, 1).begin()
        elif do == "drain":
            @pl.when(sends_right)
            def _():
                wait_bytes(xg.at[layer, t, pl.ds(0, PAD)], h_sem.at[layer, 0])

            @pl.when(sends_left)
            def _():
                wait_bytes(xg.at[layer, t, pl.ds(0, PAD)], h_sem.at[layer, 1])
            pl.when(from_left)(lambda: halo_spread(layer, 0).drain())
            pl.when(from_right)(lambda: halo_spread(layer, 1).drain())
        else:
            pl.when(from_left)(lambda: getattr(halo_spread(layer, 0), do)())
            pl.when(from_right)(lambda: getattr(halo_spread(layer, 1), do)())

    def convolve(layer, between):
        padf[...] = pad[layer].astype(f32)
        block = 64
        sums, squares = [], []
        for r in range(0, rows, block):
            total = jnp.zeros((block, chans), f32)
            for k in range(n_taps):
                start = r + PAD - reach + k
                total = total + taps[k, layer:layer + 1, :] * padf[start:start + block, :]
            mean = jnp.sum(total, axis=1, keepdims=True) / chans
            shifted = total - mean
            convg[layer, t, r:r + block, :] = shifted.astype(bf16)
            sums.append(mean)
            squares.append(jnp.sum(shifted * shifted, axis=1, keepdims=True))
            if r + block == rows // 2:
                conv_spread(layer, 0).begin()
                between()
        share(layer, [jnp.concatenate(sums, 0), jnp.concatenate(squares, 0)])
        conv_spread(layer, 1).begin()

    def activate(layer):
        got = columns_of(layer)
        means = [got[:, 8 * d:8 * d + 1] for d in range(T)]
        center = sum(means[1:], means[0]) / T
        apart = [m - center for m in means]
        square = sum((got[:, 8 * d + 1:8 * d + 2] + chans * (apart[d] * apart[d]) for d in range(T)), jnp.zeros((rows, 1), f32))
        scale = lax.rsqrt(square / C + 1e-05)
        for d in range(T):
            j = lax.rem(t + T - d, T)
            by = cgain[j, layer:layer + 1, :]
            normal = (convg[layer, j].astype(f32) + apart[d]) * scale
            act[j] = jax.nn.silu(normal * by).astype(bf16)

    def add_branch(layer, h):
        part = None
        for j in range(T):
            term = jnp.dot(act[j], wo[layer, h, j * chans:(j + 1) * chans, :], preferred_element_type=f32)
            part = term if part is None else part + term
        cols = half_columns(h)
        x_state[:, cols] = (x_state[:, cols] + part).astype(bf16).astype(f32)

    with scope("stage_wait"):
        staged(first_vg)
    token_copy.wait()
    halo(0, "send")
    each(0, QC, lambda q: inward(first_vg, q, s).start())

    @pl.when(is_end)
    def _():
        each(0, x_chunks, lambda c: end_rows(c, inner).start())

    @pl.when(is_mid)
    def _():
        x_spread().begin()

    with scope("stage_wait2"):
        for stage in after:
            staged(stage)

    def end_sends(what, stage, lo, hi):
        @pl.when(is_end)
        def _():
            if what == "in":
                each(lo, hi, lambda q: inward(stage, q, edge).start())
            else:
                each(lo, hi, lambda q: direct(stage, q).start())

    end_sends("direct", first_vg, 0, shared_from)

    @pl.when(is_mid)
    def _():
        for stage in after:
            each(0, count[stage[1]], lambda q: outward(stage, q, mine).start())

    gain_copy.wait()
    for c in small:
        c.wait()
    for d in range(1, T):
        pltpu.make_async_remote_copy(
            src_ref=cgain.at[t], dst_ref=cgain.at[t], send_sem=g_sem.at[0], recv_sem=g_sem.at[1],
            device_id={"tp": lax.rem(t + d, T)}, device_id_type=MESH).start()
    x_state[...] = xg[0, t, own, :].astype(f32)
    with scope("halo0_begin"):
        halo(0, "begin")

    def first_chunks(q):
        from_inner(first_vg, q, near)
        from_edge(first_vg, q)
    with scope("A_vg0_near_edge"):
        each(0, QC, first_chunks)
    push_in(first_wo, 0, RC)
    push_in(second_vg, 0, QC // 2)

    @pl.when(is_end)
    def _():
        def pass_on(stage):
            def body(q):
                arrived(stage, q, mine)
                across(stage, q, mine).start()
            each(0, count[stage[1]], body)
        for stage in after:
            with scope("end_pass_on"):
                pass_on(stage)
            if stage == first_wo:
                end_sends("in", first_wo, 0, RC)
                end_sends("in", second_vg, 0, QC // 2)
            elif stage == second_vg:
                end_sends("direct", first_wo, 0, RC)

    def edge_relays(lo, hi):
        @pl.when(is_mid)
        def _():
            with scope("edge_relay"):
                each(lo, hi, lambda c: edge_spread(c).relay())

    halo(0, "relay")

    @pl.when(is_mid)
    def _():
        with scope("x0_finish"):
            x_spread().relay()
            x_spread().complete()
    halo(0, "complete")

    @pl.when(is_mid)
    def _():
        with scope("norm0"):
            normalize(0, 0, 0, 0, full)

    def second_chunks(q):
        from_inner(first_vg, q, far)

        @pl.when(is_mid)
        def _():
            wait_bytes(xg.at[0, t, pl.ds(0, x_rows)], f_sem.at[2 + q])
            edge_spread(q).begin()
    with scope("B_vg0_far"):
        each(0, QC, second_chunks)

    @pl.when(is_mid)
    def _():
        with scope("proj0_g"):
            project(0, 0, 0, full, pad.at[0], g)
    edge_relays(0, x_chunks // 2)
    with scope("C1_wo0_near"):
        from_inner(first_wo, 0, near)
    edge_relays(x_chunks // 2, x_chunks - 1)
    with scope("C1_wo0_near"):
        each(1, RC, lambda q: from_inner(first_wo, q, near))
    edge_relays(x_chunks - 1, x_chunks)
    push_in(second_vg, QC // 2, QC // 2 + 1)
    end_sends("in", second_vg, QC // 2, QC)

    @pl.when(is_mid)
    def _():
        with scope("edge_complete"):
            each(0, x_chunks, lambda c: edge_spread(c).complete())
        with scope("norm_e"):
            normalize(0, L, 1, PAD, rows)
        with scope("proj0e_g"):
            project(0, 1, PAD, rows, glu_out, g)

    with scope("D1_vg1_near"):
        from_inner(second_vg, 0, near)

    @pl.when(is_mid)
    def _():
        with scope("wait_vg0"):
            others_arrived(first_vg)
        with scope("proj0e"):
            project(0, 1, PAD, rows, glu_out, other)
    with scope("C2_wo0_edge"):
        from_edge(first_wo, 0)

    @pl.when(is_mid)
    def _():
        with scope("proj0"):
            project(0, 0, 0, full, pad.at[0], other)

    sends_right, sends_left, _, _ = sides_of(0)

    @pl.when(sends_right)
    def _():
        glu_out[0:PAD, :] = jnp.zeros((PAD, chans), bf16)
        glu_out[PAD + rows:, :] = pad[0, PAD:2 * PAD, :]
        pad[0, 0:PAD, :] = glu_out[rows:rows + PAD, :]

    @pl.when(sends_left)
    def _():
        glu_out[0:PAD, :] = pad[0, rows:rows + PAD, :]
        glu_out[PAD + rows:, :] = jnp.zeros((PAD, chans), bf16)
        pad[0, PAD + rows:, :] = glu_out[PAD:2 * PAD, :]

    @pl.when(is_mid)
    def _():
        end_glu(edge).start()

    with scope("D1_vg1_near"):
        each(1, QC // 2, lambda q: from_inner(second_vg, q, near))
    with scope("C2_wo0_edge"):
        each(1, RC, lambda q: from_edge(first_wo, q))
    push_in(second_vg, QC // 2 + 1, QC)
    end_sends("in", second_wo, 0, RC)

    @pl.when(is_end)
    def _():
        with scope("end_glu_wait"):
            wait_bytes(glu_out, f_sem.at[2 + x_chunks])

    with scope("conv0"):
        convolve(0, lambda: None)
    with scope("D2_vg1_edge"):
        from_edge(second_vg, 0)
    with scope("C3_wo0_far"):
        from_inner(first_wo, 0, far)
    with scope("conv0_relay"):
        conv_spread(0, 0).relay()
    with scope("C3_wo0_far"):
        pl.when(is_end)(lambda: each(1, RC, lambda q: from_inner(first_wo, q, far)))
    with scope("conv0_relay"):
        conv_spread(0, 1).relay()
    with scope("C3_wo0_far"):
        pl.when(is_mid)(lambda: each(1, RC, lambda q: from_inner(first_wo, q, far)))
    with scope("conv0_complete"):
        conv_spread(0, 0).complete()
        conv_spread(0, 1).complete()
        wait_bytes(cgain.at[pl.ds(0, T - 1)], g_sem.at[1])
    with scope("act0"):
        activate(0)
    with scope("D2_vg1_edge"):
        from_edge(second_vg, 1)

    def next_x(h, turn):
        add_branch(0, h)
        cols = half_columns(h)
        xg[1, t, own, cols] = x_state[:, cols].astype(bf16)
        half_spread(h, turn).begin()
    with scope("out0_g"):
        next_x(g, 0)
    with scope("D2_vg1_near"):
        from_inner(second_vg, QC // 2, near)
    with scope("wait_wo0"):
        others_arrived(first_wo)
    with scope("out0"):
        next_x(other, 1)
    halo(1, "send")
    end_sends("direct", second_vg, 0, QC)
    end_sends("direct", second_wo, 0, RC)
    with scope("D3_vg1_near"):
        each(QC // 2 + 1, QC, lambda q: from_inner(second_vg, q, near))
    with scope("D3_vg1_edge"):
        from_edge(second_vg, 2)
    with scope("D4_vg1_far"):
        from_inner(second_vg, 0, far)
    with scope("D3_vg1_edge"):
        each(3, QC, lambda q: from_edge(second_vg, q))
    push_in(second_wo, 0, RC)
    with scope("D4_vg1_far"):
        from_inner(second_vg, 1, far)
    with scope("x1_relay"):
        half_spread(g, 0).relay()
    with scope("D4_vg1_far"):
        from_inner(second_vg, 2, far)
    with scope("E1_wo1_edge"):
        from_edge(second_wo, 0)
    with scope("D4_vg1_far"):
        each(3, QC, lambda q: from_inner(second_vg, q, far))
    with scope("E1_wo1_edge"):
        each(1, RC, lambda q: from_edge(second_wo, q))
    with scope("halo1_begin"):
        halo(1, "begin")
    with scope("x1_relay"):
        half_spread(other, 1).relay()
    with scope("E1_wo1_near"):
        from_inner(second_wo, 0, near)
    with scope("halo1_relay"):
        halo(1, "relay")
    with scope("x1_complete"):
        half_spread(g, 0).complete()
        half_spread(other, 1).complete()
        halo(1, "complete")
    with scope("norm1"):
        normalize(1, 1, 0, 0, full)
    with scope("E1_wo1_near"):
        each(1, RC, lambda q: from_inner(second_wo, q, near))
    with scope("proj1_g"):
        project(1, 0, 0, full, pad.at[1], g)
    with scope("E2_wo1_far_m"):
        pl.when(is_mid)(lambda: from_inner(second_wo, 0, far))
    with scope("wait_vg1"):
        others_arrived(second_vg)
    with scope("proj1"):
        project(1, 0, 0, full, pad.at[1], other)
    with scope("E2_wo1_far_e"):
        pl.when(is_end)(lambda: from_inner(second_wo, 0, far))
    with scope("conv1"):
        convolve(1, lambda: pl.when(is_mid)(lambda: each(1, RC, lambda q: from_inner(second_wo, q, far))))
    with scope("conv1_gather"):
        conv_spread(1, 0).relay()
        pl.when(is_end)(lambda: each(1, RC, lambda q: from_inner(second_wo, q, far)))
        conv_spread(1, 1).relay()
        conv_spread(1, 0).complete()
        conv_spread(1, 1).complete()
    with scope("act1"):
        activate(1)
    with scope("out1_g"):
        add_branch(1, g)
    with scope("wait_wo1"):
        others_arrived(second_wo)
    with scope("out1"):
        add_branch(1, other)
    xf = x_state[...]
    share(L, [jnp.sum(xf * xf, axis=1, keepdims=True)])

    halo(0, "drain")
    halo(1, "drain")
    for layer in range(L):
        for part_ in range(2):
            conv_spread(layer, part_).drain()
    half_spread(g, 0).drain()
    half_spread(other, 1).drain()
    wait_bytes(cgain.at[pl.ds(0, T - 1)], g_sem.at[0])
    chunk_rows = size["vg"]
    stages = L * pieces
    later = stages - QC

    def sent(chunks, k):
        wait_bytes(wvg.at[0, 0, pl.ds(0, chunks * chunk_rows)], send_w.at[k])

    def sent_twice(chunks, k):
        wait_bytes(wvg.at[0, :, pl.ds(0, chunks * chunk_rows)], send_w.at[k])

    def sent_all(k):
        sent_twice(later * (n - 1) // G, k)

    @pl.when(is_mid)
    def _():
        x_spread().drain()
        each(0, x_chunks, lambda c: edge_spread(c).drain())
        wait_bytes(glu_out, f_sem.at[1])
        sent_twice(stages, IN)
        sent_all(OUT)
        sent(QC - shared_from, YE)
        sent_twice(later + QC, Y)

    @pl.when(is_end)
    def _():
        wait_bytes(xg.at[0, t, own], f_sem.at[0])
        sent(stages, IN)
        sent(later + shared_from, UN)
        sent_all(Y)

    with scope("final_stat"):
        got = columns_of(L)
        for index_ in range(L + 1):
            wait_bytes(stat.at[index_, pl.ds(0, T - 1)], s_sem.at[2 * index_])
    total = sum((got[:, 8 * d:8 * d + 1] for d in range(1, T)), got[:, 0:1])
    scale = lax.rsqrt(total / D + 1e-06)
    result[...] = (x_state[...] * scale * fgain[...]).astype(bf16)


def quad_on_device(G, n, T, tokens, norm_gain, value_w, gate_w, taps, cgain, out_w, fgain):
    L = norm_gain.shape[0]
    if L != 2:
        return on_device(G, n, T, tokens, norm_gain, value_w, gate_w, taps, cgain, out_w, fgain)
    rows, width = tokens.shape
    depth, chans = value_w.shape[1:]
    D, C = width * T, chans * T
    bf16, f32 = jnp.bfloat16, jnp.float32
    dma = pltpu.SemaphoreType.DMA
    vmem = pl.BlockSpec(memory_space=pltpu.VMEM)
    hbm = pl.BlockSpec(memory_space=pl.ANY)
    full = rows + 2 * PAD
    return pl.pallas_call(
        functools.partial(quad_kernel, G, n, T, L),
        out_shape=jax.ShapeDtypeStruct((rows, width), bf16),
        in_specs=[hbm] * 8,
        out_specs=vmem,
        scratch_shapes=[
            pltpu.VMEM((L, G, D, 2 * chans // G), bf16),
            pltpu.VMEM((L, G, C, width // G), bf16),
            pltpu.VMEM((L + 1, T, full, width), bf16),
            pltpu.VMEM((2, T, full, width), bf16),
            pltpu.VMEM((full, chans), bf16),
            pltpu.VMEM((full, 2 * chans // G), f32),
            pltpu.VMEM((L, full, chans), bf16),
            pltpu.VMEM((full, chans), f32),
            pltpu.VMEM((L, T, rows, chans), bf16),
            pltpu.VMEM((T, rows, chans), bf16),
            pltpu.VMEM((L + 1, T, 8, rows), f32),
            pltpu.VMEM((rows, width), f32),
            pltpu.VMEM(norm_gain.shape, f32),
            pltpu.VMEM((taps.shape[1], L, chans), f32),
            pltpu.VMEM((T,) + cgain.shape, f32),
            pltpu.VMEM((1, width), f32),
            dma((2 * L + 5,)),
            dma((L * (QC + RC), 3)), dma((2 * L,)), dma((5,)),
            dma((1 + G, 3)), dma((QC, 3)), dma((L, 2, 3)), dma((2 * (L + 1),)),
            dma((L, 4)), dma((L, 2, 3)), dma((2,)), dma((QC + 3,)),
        ],
        compiler_params=pltpu.CompilerParams(
            collective_id=0, has_side_effects=True, vmem_limit_bytes=56 * 2**20
        ),
    )(tokens, norm_gain, value_w, gate_w, taps.transpose(1, 0, 2), cgain, out_w, fgain.reshape(1, width))


def tokens_f32(tokens, xg, t):
    return xg[0, t].astype(jnp.float32)


def on_device(G, n, T, tokens, norm_gain, value_w, gate_w, taps, cgain, out_w, fgain):
    L = norm_gain.shape[0]
    rows, width = tokens.shape
    depth, chans = value_w.shape[1:]
    D, C = width * T, chans * T
    bf16, f32 = jnp.bfloat16, jnp.float32
    dma = pltpu.SemaphoreType.DMA
    vmem = pl.BlockSpec(memory_space=pltpu.VMEM)
    hbm = pl.BlockSpec(memory_space=pl.ANY)
    P_ = L * (Q + 1)
    peers = max(G - 1, 1)
    return pl.pallas_call(
        functools.partial(kernel, G, n, T, L),
        out_shape=jax.ShapeDtypeStruct((rows, width), bf16),
        in_specs=[hbm, vmem, hbm, hbm, vmem, vmem, hbm, vmem],
        out_specs=vmem,
        scratch_shapes=[
            pltpu.VMEM((L, G, D, 2 * chans // G), bf16),
            pltpu.VMEM((L, G, C, width // G), bf16),
            pltpu.VMEM((L + 1, T, rows, width), bf16),
            pltpu.VMEM((2, T, rows, width), bf16),
            pltpu.VMEM((rows, chans), bf16),
            pltpu.VMEM((rows, 2 * chans // G), f32),
            pltpu.VMEM((L, rows + 2 * PAD, chans), bf16),
            pltpu.VMEM((rows + 2 * PAD, chans), f32),
            pltpu.VMEM((rows, chans), f32),
            pltpu.VMEM((L + 1, T, 8, rows), f32),
            pltpu.VMEM((L, T, rows, chans), bf16),
            pltpu.VMEM((rows, width), f32),
            dma((1 + L * G * 3,)),
            dma((P_, n)), dma((P_, n)), dma((P_, n)),
            dma((P_, n, peers)), dma((P_, n, peers)),
            dma((L + 1, T)), dma((L + 1, T)), dma((L, T)), dma((L, T)),
            dma((L + 1, T)), dma((L + 1, T)),
            dma((L, 2)), dma((L, 2)),
            dma((G + 1,)), dma((G + 1,)),
        ],
        compiler_params=pltpu.CompilerParams(
            collective_id=0, has_side_effects=True, vmem_limit_bytes=56 * 2**20
        ),
    )(tokens, norm_gain.reshape(L * T, width), value_w, gate_w, taps, cgain, out_w, fgain.reshape(1, width))


def solution(mesh):
    placed = (
        P(("grp", "sp"), "tp"),
        P(),
        P(None, "sp", "tp"),
        P(None, "sp", "tp"),
        P(None, None, "tp"),
        P(None, "tp"),
        P(None, "sp", "tp"),
        P("tp"),
    )
    G, n, T = (mesh.shape[a] for a in ("grp", "sp", "tp"))
    paired = G == 2 and n == T == 2 * G
    return jax.shard_map(
        functools.partial(quad_on_device if paired else on_device, G, n, T),
        mesh=mesh, in_specs=placed, out_specs=P(("grp", "sp"), "tp"), check_vma=False,
    )
```

```python
import functools

import jax
import jax.numpy as jnp
from jax import lax
from jax.experimental import pallas as pl
from jax.experimental.pallas import tpu as pltpu
from jax.sharding import PartitionSpec as P

MESH = pl.DeviceIdType.MESH
Q = 2
PAD = 16


def kernel(
    G, n, T, L,
    tokens, gain, value_w, gate_w, taps, cgain, out_w, fgain,
    result,
    wvg, wo, xg, xn, glu_out, acc, pad, padf, conv, stat, actg, x_state,
    local_sem, z_recv, right_send, left_send, y_send, y_recv,
    x_send, x_recv, a_send, a_recv, s_send, s_recv, h_send, h_recv, f_send, f_recv,
):
    g, s, t = lax.axis_index("grp"), lax.axis_index("sp"), lax.axis_index("tp")
    rows, width = tokens.shape
    depth, chans = value_w.shape[1:]
    out_rows = out_w.shape[1]
    half = chans // G
    out_half = width // G
    reach = taps.shape[1] // 2
    n_taps = taps.shape[1]
    D = width * T
    C = chans * T
    chunk = depth // Q
    pieces = Q + 1
    f32, bf16 = jnp.float32, jnp.bfloat16
    helped = n >= 4
    last = n - 1
    is_end = (s == 0) | (s == last)
    helper = (s == 1) | (s == last - 1)
    end = jnp.where(s == 1, 0, last)
    inward = jnp.where(s == 0, 1, last - 1)

    def ends_out(p):
        return helped and p < Q

    def to_right_ok(p):
        return s < last - 1 if ends_out(p) else s < last

    def to_left_ok(p):
        return s > 1 if ends_out(p) else s > 0

    def takes(p):
        return jnp.logical_not(is_end) if ends_out(p) else s >= 0

    def by_grp(p, j):
        ok = takes(p) & (j != s)
        if helped and p == 0:
            ok = ok & jnp.logical_not((s == 1) & (j == 0)) & jnp.logical_not((s == last - 1) & (j == last))
        return ok

    def piece(p, h, j):
        layer, q = p // pieces, p % pieces
        if q < Q:
            start = pl.multiple_of(j * depth + q * chunk, chunk)
            return wvg.at[layer, h, pl.ds(start, chunk), :]
        return wo.at[layer, h, pl.ds(pl.multiple_of(j * out_rows, out_rows), out_rows), :]

    locals_ = [pltpu.make_async_copy(tokens, xg.at[0, t], local_sem.at[0])]
    own_rows = pl.ds(pl.multiple_of(s * depth, depth), depth)
    own_out = pl.ds(pl.multiple_of(s * out_rows, out_rows), out_rows)
    count = 1
    per_layer = []
    for layer in range(L):
        group = []
        for h in range(G):
            for k, w in enumerate((value_w, gate_w)):
                group.append(pltpu.make_async_copy(
                    w.at[layer, :, pl.ds(h * half, half)],
                    wvg.at[layer, h, own_rows, pl.ds(k * half, half)],
                    local_sem.at[count]))
                count += 1
            group.append(pltpu.make_async_copy(
                out_w.at[layer, :, pl.ds(h * out_half, out_half)],
                wo.at[layer, h, own_out, :], local_sem.at[count]))
            count += 1
        per_layer.append(group)
    for c in locals_ + sum(per_layer, []):
        c.start()

    barrier = pltpu.get_barrier_semaphore()
    for d in range(1, T):
        pl.semaphore_signal(barrier, inc=1, device_id={"tp": lax.rem(t + d, T)}, device_id_type=MESH)
    for d in range(1, G):
        pl.semaphore_signal(barrier, inc=1, device_id={"grp": lax.rem(g + d, G)}, device_id_type=MESH)

    @pl.when(s > 0)
    def _():
        pl.semaphore_signal(barrier, inc=1, device_id={"sp": s - 1}, device_id_type=MESH)

    @pl.when(s < n - 1)
    def _():
        pl.semaphore_signal(barrier, inc=1, device_id={"sp": s + 1}, device_id_type=MESH)

    sides = jnp.where(s > 0, 1, 0) + jnp.where(s < n - 1, 1, 0)
    pl.semaphore_wait(barrier, (T - 1) + (G - 1) + sides)

    def right(p, j):
        r = piece(p, g, j)
        return pltpu.make_async_remote_copy(
            src_ref=r, dst_ref=r, send_sem=right_send.at[p, j], recv_sem=z_recv.at[p, j],
            device_id={"sp": s + 1}, device_id_type=MESH)

    def left(p, j):
        r = piece(p, g, j)
        return pltpu.make_async_remote_copy(
            src_ref=r, dst_ref=r, send_sem=left_send.at[p, j], recv_sem=z_recv.at[p, j],
            device_id={"sp": s - 1}, device_id_type=MESH)

    def across(p, j, d, h):
        r = piece(p, h, j)
        return pltpu.make_async_remote_copy(
            src_ref=r, dst_ref=r, send_sem=y_send.at[p, j, d - 1], recv_sem=y_recv.at[p, j, d - 1],
            device_id={"grp": lax.rem(g + d, G)}, device_id_type=MESH)

    batches = []
    for layer in range(L):
        base = layer * pieces
        batches += [list(range(base, base + Q)), [base + Q]]

    def own_right(ps):
        for p in ps:
            right(p, s).start()

    def own_left(ps):
        for p in ps:
            left(p, s).start()

    def end_rows(target):
        return pltpu.make_async_remote_copy(
            src_ref=xg.at[0, t], dst_ref=xg.at[L, t], send_sem=f_send.at[0], recv_sem=f_recv.at[0],
            device_id={"sp": target}, device_id_type=MESH)

    def end_piece(d, h, j, target):
        r = piece(0, h, j)
        return pltpu.make_async_remote_copy(
            src_ref=r, dst_ref=r, send_sem=f_send.at[d], recv_sem=f_recv.at[d],
            device_id={"sp": target}, device_id_type=MESH)

    def end_glu(target):
        return pltpu.make_async_remote_copy(
            src_ref=glu_out, dst_ref=pad.at[0, pl.ds(PAD, rows), :],
            send_sem=f_send.at[G], recv_sem=f_recv.at[G],
            device_id={"sp": target}, device_id_type=MESH)

    def relay(b, low, high):
        low, high = min(low, n - 1), min(high, n - 1)
        following = batches[b + 1] if b + 1 < len(batches) else []

        def step(k, carry):
            for p in batches[b]:
                from_left, from_right = s - 1 - k, s + 1 + k

                @pl.when((from_left >= 0) & takes(p))
                def _():
                    j = jnp.maximum(from_left, 0)
                    right(p, j).wait_recv()

                    @pl.when(to_right_ok(p))
                    def _():
                        right(p, j).start()

                    @pl.when(by_grp(p, j))
                    def _():
                        for d in range(1, G):
                            across(p, j, d, g).start()

                @pl.when((from_right < n) & takes(p))
                def _():
                    j = jnp.minimum(from_right, n - 1)
                    left(p, j).wait_recv()

                    @pl.when(to_left_ok(p))
                    def _():
                        left(p, j).start()

                    @pl.when(by_grp(p, j))
                    def _():
                        for d in range(1, G):
                            across(p, j, d, g).start()

            @pl.when((k == s - 1) & (s < (last - 1 if helped and b < 2 else last)))
            def _():
                own_right(following)

            @pl.when((k == n - 2 - s) & (s > (1 if helped and b < 2 else 0)))
            def _():
                own_left(following)

            return carry

        if high > low:
            lax.fori_loop(low, high, step, 0)

    def wait_across(b):
        for p in batches[b]:
            def step(j, carry):
                @pl.when(by_grp(p, j))
                def _():
                    for d in range(1, G):
                        across(p, j, d, lax.rem(g + G - d, G)).wait_recv()
                return carry
            lax.fori_loop(0, n, step, 0)

    def spread(buf, layer, send, recv):
        def copy(bit, m):
            block = buf.at[layer, t ^ m]
            return pltpu.make_async_remote_copy(
                src_ref=block, dst_ref=block, send_sem=send.at[layer, bit + m], recv_sem=recv.at[layer, bit + m],
                device_id={"tp": t ^ bit}, device_id_type=MESH)

        def arrival(bit, m):
            block = buf.at[layer, t ^ bit ^ m]
            return pltpu.make_async_remote_copy(
                src_ref=block, dst_ref=block, send_sem=send.at[layer, bit + m], recv_sem=recv.at[layer, bit + m],
                device_id={"tp": t ^ bit}, device_id_type=MESH)

        bits = []
        bit = T // 2
        while bit >= 1:
            bits.append(bit)
            bit //= 2

        def begin():
            for bit in bits:
                copy(bit, 0).start()

        def finish():
            have, sent = [0], []
            for i, bit in enumerate(bits):
                for m in have:
                    arrival(bit, m).wait_recv()
                    sent.append((bit, m))
                    for lower in bits[i + 1:]:
                        copy(lower, m ^ bit).start()
                have = have + [m ^ bit for m in have]
            return lambda: [copy(bit, m).wait_send() for bit, m in sent]

        return begin, finish

    def exchange(index, columns):
        lane = lax.broadcasted_iota(jnp.int32, (rows, 128), 1)
        tile = jnp.zeros((rows, 128), f32)
        for i, column in enumerate(columns):
            tile = jnp.where(lane == i, column, tile)
        stat[index, 0] = tile.T[:8, :]

        def copy(d):
            return pltpu.make_async_remote_copy(
                src_ref=stat.at[index, 0], dst_ref=stat.at[index, d],
                send_sem=s_send.at[index, d - 1], recv_sem=s_recv.at[index, d - 1],
                device_id={"tp": lax.rem(t + d, T)}, device_id_type=MESH)

        for d in range(1, T):
            copy(d).start()

        def total():
            for d in range(1, T):
                copy(d).wait_recv()
            sums = stat[index, 0]
            for d in range(1, T):
                sums = sums + stat[index, d]
            wide = jnp.concatenate([sums, jnp.zeros((120, rows), f32)], axis=0).T
            for d in range(1, T):
                copy(d).wait_send()
            return [wide[:, i:i + 1] for i in range(len(columns))]

        return total

    def normalize(layer, held, into):
        def squares(j, total):
            part = xg[held, j].astype(f32)
            return total + jnp.sum(part * part, axis=1, keepdims=True)
        mean = lax.fori_loop(0, T, squares, jnp.zeros((rows, 1), f32)) / D
        scale = lax.rsqrt(mean + 1e-06)

        def body(j, carry):
            xn[into, j] = (xg[held, j].astype(f32) * scale * gain[layer * T + j][None, :]).astype(bf16)
            return carry
        lax.fori_loop(0, T, body, 0)

    def project(layer, held, put):
        for h in range(G):
            def body(j, carry):
                block = wvg[layer, h, pl.ds(pl.multiple_of(j * width, width), width), :]
                part = jnp.dot(xn[held, j], block, preferred_element_type=f32)

                @pl.when(j == 0)
                def _():
                    acc[...] = part

                @pl.when(j > 0)
                def _():
                    acc[...] += part
                return carry
            lax.fori_loop(0, T, body, 0)
            glu = acc[:, :half] * jax.nn.sigmoid(acc[:, half:])
            put(h, glu.astype(bf16))

    for c in locals_:
        c.wait()
    spreads = [spread(xg, layer, x_send, x_recv) for layer in range(L)]
    spreads[0][0]()
    for c in sum(per_layer, []):
        c.wait()

    @pl.when(to_right_ok(0))
    def _():
        own_right(batches[0])

    @pl.when(to_left_ok(0))
    def _():
        own_left(batches[0])

    if helped:
        @pl.when(is_end)
        def _():
            end_rows(inward).start()
            for d in range(1, G):
                end_piece(d, lax.rem(g + d, G), s, inward).start()

        @pl.when(s == last - 1)
        def _():
            own_right(batches[1])
            if L > 1:
                own_right(batches[2])

        @pl.when(s == 1)
        def _():
            own_left(batches[1])
            if L > 1:
                own_left(batches[2])

    @pl.when((s == 0) & (s < n - 1))
    def _():
        for b in batches[1:]:
            own_right(b)

    @pl.when((s == n - 1) & (s > 0))
    def _():
        for b in batches[1:]:
            own_left(b)

    x_state[...] = tokens_f32(tokens, xg, t)
    drains = []

    for layer in range(L):
        first, second = 2 * layer, 2 * layer + 1
        if layer == 0:
            relay(first, 0, 1)
        else:
            relay(first, 1, 2)
        drains.append(spreads[layer][1]())
        if helped and layer == 0:
            @pl.when(jnp.logical_not(is_end))
            def _():
                normalize(layer, layer, 0)
        else:
            normalize(layer, layer, 0)
        relay(first, 1 if layer == 0 else 2, n)
        begin, finish = spread(xg, L, x_send, x_recv)
        if helped and layer == 0:
            @pl.when(helper)
            def _():
                end_rows(end).wait_recv()
                begin()

        relay(second, 0, 1)

        def put(h, value):
            pad[layer, PAD:PAD + rows, h * half:(h + 1) * half] = value

        def put_out(h, value):
            glu_out[:, h * half:(h + 1) * half] = value

        if helped and layer == 0:
            @pl.when(helper)
            def _():
                drain = finish()
                normalize(0, L, 1)
                for d in range(1, G):
                    end_piece(d, lax.rem(g + d, G), end, end).wait_recv()
                drain()

            wait_across(first)

            @pl.when(helper)
            def _():
                project(0, 1, put_out)
                end_glu(end).start()

            @pl.when(jnp.logical_not(is_end))
            def _():
                project(0, 0, put)

            @pl.when(helper)
            def _():
                end_glu(end).wait_send()

            @pl.when(is_end)
            def _():
                end_rows(inward).wait_send()
                for d in range(1, G):
                    end_piece(d, lax.rem(g + d, G), s, inward).wait_send()
                end_glu(inward).wait_recv()
        else:
            wait_across(first)
            project(layer, 0, put)

        def to_right():
            return pltpu.make_async_remote_copy(
                src_ref=pad.at[layer, pl.ds(rows, PAD), :], dst_ref=pad.at[layer, pl.ds(0, PAD), :],
                send_sem=h_send.at[layer, 0], recv_sem=h_recv.at[layer, 0],
                device_id={"sp": s + 1}, device_id_type=MESH)

        def to_left():
            return pltpu.make_async_remote_copy(
                src_ref=pad.at[layer, pl.ds(PAD, PAD), :], dst_ref=pad.at[layer, pl.ds(PAD + rows, PAD), :],
                send_sem=h_send.at[layer, 1], recv_sem=h_recv.at[layer, 1],
                device_id={"sp": s - 1}, device_id_type=MESH)

        @pl.when(s < n - 1)
        def _():
            to_right().start()

        @pl.when(s > 0)
        def _():
            to_left().start()

        @pl.when(s == 0)
        def _():
            pad[layer, 0:PAD, :] = jnp.zeros((PAD, chans), bf16)

        @pl.when(s == n - 1)
        def _():
            pad[layer, PAD + rows:, :] = jnp.zeros((PAD, chans), bf16)

        relay(second, 1, 2)

        @pl.when(s > 0)
        def _():
            to_right().wait_recv()

        @pl.when(s < n - 1)
        def _():
            to_left().wait_recv()

        padf[...] = pad[layer].astype(f32)
        block = 64
        sums, squares = [], []
        for r in range(0, rows, block):
            total = jnp.zeros((block, chans), f32)
            for k in range(n_taps):
                start = r + PAD - reach + k
                total = total + taps[layer, k][None, :] * padf[start:start + block, :]
            conv[r:r + block, :] = total
            sums.append(jnp.sum(total, axis=1, keepdims=True))
            squares.append(jnp.sum(total * total, axis=1, keepdims=True))
        totals = exchange(layer, [jnp.concatenate(sums, 0), jnp.concatenate(squares, 0)])
        relay(second, 2, n)
        if layer + 1 < L:
            relay(second + 1, 0, 1)
        total, square = totals()
        center = total / C
        spread_ = square / C - center * center
        normal = (conv[...] - center) * lax.rsqrt(spread_ + 1e-05)
        actg[layer, t] = jax.nn.silu(normal * cgain[layer][None, :]).astype(bf16)
        act_begin, act_finish = spread(actg, layer, a_send, a_recv)
        act_begin()
        drains.append(act_finish())
        wait_across(second)
        for h in range(G):
            part = None
            for j in range(T):
                term = jnp.dot(actg[layer, j], wo[layer, h, j * chans:(j + 1) * chans, :], preferred_element_type=f32)
                part = term if part is None else part + term
            cols = slice(h * out_half, (h + 1) * out_half)
            x_state[:, cols] = (x_state[:, cols] + part).astype(bf16).astype(f32)
        if layer + 1 < L:
            xg[layer + 1, t] = x_state[...].astype(bf16)
            spreads[layer + 1][0]()

        @pl.when(s < n - 1)
        def _():
            to_right().wait_send()

        @pl.when(s > 0)
        def _():
            to_left().wait_send()

    xf = x_state[...]
    totals = exchange(L, [jnp.sum(xf * xf, axis=1, keepdims=True)])

    for drain in drains:
        drain()

    def drain_step(j, carry):
        for p in range(L * pieces):
            came = (j == s) | takes(p)

            @pl.when((j <= s) & to_right_ok(p) & came)
            def _():
                right(p, j).wait_send()

            @pl.when((j >= s) & to_left_ok(p) & came)
            def _():
                left(p, j).wait_send()

            @pl.when(by_grp(p, j))
            def _():
                for d in range(1, G):
                    across(p, j, d, g).wait_send()
        return carry
    lax.fori_loop(0, n, drain_step, 0)

    (total,) = totals()
    scale = lax.rsqrt(total / D + 1e-06)
    result[...] = (x_state[...] * scale * fgain[...]).astype(bf16)


QC = 4
RC = 4
EPILOGUE = 2


def quad_kernel(
    G, n, T, L,
    tokens, gain_hbm, value_w, gate_w, taps_hbm, cgain_hbm, out_w,
    x_out, scale_out,
    wvg, wo, xg, xn, glu_out, acc, pad, padf, convg, act, stat, x_state, leaving, gain, taps, cgain,
    local_sem, recv_z, recv_o, send_w, x_sem, e_sem, c_sem, s_sem, h_sem, hs_sem, g_sem, f_sem, o_sem,
):
    g, s, t = lax.axis_index("grp"), lax.axis_index("sp"), lax.axis_index("tp")
    rows, width = tokens.shape
    depth, chans = value_w.shape[1:]
    out_rows = out_w.shape[1]
    half = chans // G
    out_half = width // G
    n_taps = taps.shape[0]
    reach = n_taps // 2
    D = width * T
    C = chans * T
    full = rows + 2 * PAD
    pieces = QC + RC
    size = {"vg": depth // QC, "wo": out_rows // RC}
    count = {"vg": QC, "wo": RC}
    shared_from = QC - 1
    f32, bf16 = jnp.float32, jnp.bfloat16
    last = n - 1
    low = s < n // 2
    is_end = (s == 0) | (s == last)
    is_mid = jnp.logical_not(is_end)
    inner = jnp.where(low, s + 1, s - 1)
    outer = jnp.where(low, s - 1, s + 1)
    edge, mine, near, far = (jnp.where(low, a, last - a) for a in (0, 1, n - 2, n - 1))
    other = lax.rem(g + 1, G)
    x_chunks = QC
    x_rows = rows // x_chunks
    own = pl.ds(PAD, rows)
    first_vg, first_wo, second_vg, second_wo = (0, "vg"), (0, "wo"), (1, "vg"), (1, "wo")
    after = (first_wo, second_vg, second_wo)
    scope = jax.named_scope
    IN, OUT, Y, YE, UN = range(5)

    def index(stage, q):
        layer, kind = stage
        return layer * pieces + (0 if kind == "vg" else QC) + q

    def order_of(stage):
        return stage[0] * 2 + (0 if stage[1] == "vg" else 1)

    def place(j):
        return jnp.where(j == near, 1, jnp.where(j == far, 2, 0))

    def piece(stage, q, h, j):
        layer, kind = stage
        step = size[kind]
        per = depth if kind == "vg" else out_rows
        ref = wvg if kind == "vg" else wo
        return ref.at[layer, h, pl.ds(pl.multiple_of(j * per + q * step, step), step), :]

    def wait_bytes(ref, sem):
        pltpu.make_async_copy(ref, ref, sem).wait()

    own_rows = pl.ds(pl.multiple_of(s * depth, depth), depth)
    own_out = pl.ds(pl.multiple_of(s * out_rows, out_rows), out_rows)

    def stage_in(stage):
        layer, kind = stage
        sem = local_sem.at[order_of(stage)]
        for h in range(G):
            if kind == "vg":
                for k, w in enumerate((value_w, gate_w)):
                    pltpu.make_async_copy(
                        w.at[layer, :, pl.ds(h * half, half)],
                        wvg.at[layer, h, own_rows, pl.ds(k * half, half)], sem).start()
            else:
                pltpu.make_async_copy(
                    out_w.at[layer, :, pl.ds(h * out_half, out_half)],
                    wo.at[layer, h, own_out, :], sem).start()

    def staged(stage):
        layer, kind = stage
        ref = wvg.at[layer, :, own_rows] if kind == "vg" else wo.at[layer, :, own_out]
        wait_bytes(ref, local_sem.at[order_of(stage)])

    token_copy = pltpu.make_async_copy(tokens, xg.at[0, t, own], local_sem.at[2 * L])
    gain_copy = pltpu.make_async_copy(cgain_hbm, cgain.at[t], local_sem.at[2 * L + 1])
    small = [
        pltpu.make_async_copy(gain_hbm, gain, local_sem.at[2 * L + 2]),
        pltpu.make_async_copy(taps_hbm, taps, local_sem.at[2 * L + 3]),
    ]
    stage_in(first_vg)
    token_copy.start()
    gain_copy.start()
    for stage in after:
        stage_in(stage)
    for c in small:
        c.start()

    barrier = pltpu.get_barrier_semaphore()
    for d in range(1, T):
        pl.semaphore_signal(barrier, inc=1, device_id={"tp": lax.rem(t + d, T)}, device_id_type=MESH)
    pl.semaphore_signal(barrier, inc=1, device_id={"grp": other}, device_id_type=MESH)

    @pl.when(s > 0)
    def _():
        pl.semaphore_signal(barrier, inc=1, device_id={"sp": s - 1}, device_id_type=MESH)

    @pl.when(s < last)
    def _():
        pl.semaphore_signal(barrier, inc=1, device_id={"sp": s + 1}, device_id_type=MESH)

    blank = jnp.zeros((T, PAD, width), bf16)

    @pl.when(s < n // 2)
    def _():
        xg[0, :, 0:PAD, :] = blank

    @pl.when(s >= n // 2)
    def _():
        xg[0, :, PAD + rows:, :] = blank

    @pl.when(s == 0)
    def _():
        xg[1, :, 0:PAD, :] = blank

    @pl.when(s == last)
    def _():
        xg[1, :, PAD + rows:, :] = blank

    sides = jnp.where(s > 0, 1, 0) + jnp.where(s < last, 1, 0)
    pl.semaphore_wait(barrier, (T - 1) + (G - 1) + sides)

    def arrived(stage, q, j):
        wait_bytes(piece(stage, q, g, j), recv_z.at[index(stage, q), place(j)])

    def inward(stage, q, j):
        r, p = piece(stage, q, g, j), index(stage, q)
        there = jnp.where(is_end, 0, jnp.where(j == mine, 1, 2))
        return pltpu.make_async_remote_copy(
            src_ref=r, dst_ref=r, send_sem=send_w.at[IN], recv_sem=recv_z.at[p, there],
            device_id={"sp": inner}, device_id_type=MESH)

    def outward(stage, q, j):
        r, p = piece(stage, q, g, j), index(stage, q)
        return pltpu.make_async_remote_copy(
            src_ref=r, dst_ref=r, send_sem=send_w.at[OUT], recv_sem=recv_z.at[p, place(j)],
            device_id={"sp": outer}, device_id_type=MESH)

    def across(stage, q, j, send=Y):
        r = piece(stage, q, g, j)
        return pltpu.make_async_remote_copy(
            src_ref=r, dst_ref=r, send_sem=send_w.at[send], recv_sem=recv_o.at[order_of(stage)],
            device_id={"grp": other}, device_id_type=MESH)

    def direct(stage, q):
        r = piece(stage, q, other, edge)
        return pltpu.make_async_remote_copy(
            src_ref=r, dst_ref=r, send_sem=send_w.at[UN], recv_sem=recv_o.at[order_of(stage)],
            device_id={"sp": inner}, device_id_type=MESH)

    def others_arrived(stage):
        layer, kind = stage
        per = depth if kind == "vg" else out_rows
        ref = wvg if kind == "vg" else wo
        wait_bytes(ref.at[layer, 0, pl.ds(0, (n - 1) * per)], recv_o.at[order_of(stage)])

    def end_rows(c, target):
        src = pl.ds(pl.multiple_of(PAD + c * x_rows, PAD), x_rows)
        return pltpu.make_async_remote_copy(
            src_ref=xg.at[0, t, src], dst_ref=xg.at[L, t, src], send_sem=f_sem.at[0], recv_sem=f_sem.at[2 + c],
            device_id={"sp": target}, device_id_type=MESH)

    def end_glu(target):
        return pltpu.make_async_remote_copy(
            src_ref=glu_out, dst_ref=pad.at[0], send_sem=f_sem.at[1], recv_sem=f_sem.at[2 + x_chunks],
            device_id={"sp": target}, device_id_type=MESH)

    def each(low_, high_, body):
        def step(q, carry):
            body(q)
            return carry
        lax.fori_loop(low_, high_, step, 0)

    def from_inner(stage, q, j, over_y=True):
        def serve():
            with scope("w_inner"):
                arrived(stage, q, j)
            if stage != first_vg:
                @pl.when(is_mid)
                def _():
                    outward(stage, q, j).start()
            if over_y:
                across(stage, q, j).start()
        if stage == first_vg:
            pl.when(is_mid)(serve)
        else:
            serve()

    def from_edge(stage, q):
        @pl.when(is_mid)
        def _():
            with scope("w_edge"):
                arrived(stage, q, edge)
            inward(stage, q, edge).start()
            if stage == first_vg:
                @pl.when(q >= shared_from)
                def _():
                    across(stage, q, edge, YE).start()

    def push_in(stage, lo, hi):
        @pl.when(is_mid)
        def _():
            each(lo, hi, lambda q: inward(stage, q, mine).start())

    class Spread:
        def __init__(self, view, three, two, sems):
            self.view, self.three, self.two, self.sems = view, three, two, sems

        def copy(self, j, bit, k):
            block = self.view(j)
            return pltpu.make_async_remote_copy(
                src_ref=block, dst_ref=block, send_sem=self.sems(2), recv_sem=self.sems(k),
                device_id={"tp": t ^ bit}, device_id_type=MESH)

        def begin(self):
            self.copy(t, T // 2, 0).start()
            self.copy(t, 1, 1).start()

        def relay(self):
            wait_bytes(self.view(t), self.sems(0))
            self.copy(t ^ (T // 2), 1, 1).start()

        def complete(self):
            wait_bytes(self.two, self.sems(1))

        def drain(self):
            wait_bytes(self.three, self.sems(2))

    def half_columns(h):
        return pl.ds(pl.multiple_of(h * out_half, out_half), out_half)

    def x_spread():
        return Spread(lambda j: xg.at[0, j, own], xg.at[0, pl.ds(0, 3), own], xg.at[0, pl.ds(0, 2), own],
                      lambda k: x_sem.at[0, k])

    def half_spread(h, turn):
        cols = half_columns(h)
        return Spread(lambda j: xg.at[1, j, own, cols], xg.at[1, pl.ds(0, 3), own, cols],
                      xg.at[1, pl.ds(0, 2), own, cols], lambda k: x_sem.at[1 + turn, k])

    def edge_spread(c):
        part = pl.ds(pl.multiple_of(PAD + c * x_rows, PAD), x_rows)
        return Spread(lambda j: xg.at[L, j, part], xg.at[L, pl.ds(0, 3), part], xg.at[L, pl.ds(0, 2), part],
                      lambda k: e_sem.at[c, k])

    def halo_spread(layer, side):
        part = pl.ds(0 if side == 0 else PAD + rows, PAD)
        return Spread(lambda j: xg.at[layer, j, part], xg.at[layer, pl.ds(0, 3), part], xg.at[layer, pl.ds(0, 2), part],
                      lambda k: hs_sem.at[layer, side, k])

    def conv_spread(layer, part_):
        part = pl.ds(part_ * (rows // 2), rows // 2)
        return Spread(lambda j: convg.at[layer, j, part], convg.at[layer, pl.ds(0, 3), part],
                      convg.at[layer, pl.ds(0, 2), part], lambda k: c_sem.at[layer, part_, k])

    def to_peers(buf, sem, k):
        for d in range(1, T):
            pltpu.make_async_remote_copy(
                src_ref=buf.at[0], dst_ref=buf.at[d], send_sem=sem.at[k], recv_sem=sem.at[k + 1],
                device_id={"tp": lax.rem(t + d, T)}, device_id_type=MESH).start()

    def columns_of(index_):
        wait_bytes(stat.at[index_, pl.ds(0, T - 1)], s_sem.at[2 * index_ + 1])
        got = jnp.concatenate([stat[index_, d] for d in range(T)] + [jnp.zeros((128 - 8 * T, rows), f32)], axis=0)
        return got.T

    def share(index_, columns):
        lane = lax.broadcasted_iota(jnp.int32, (rows, 128), 1)
        tile = jnp.zeros((rows, 128), f32)
        for i, column in enumerate(columns):
            tile = jnp.where(lane == i, column, tile)
        stat[index_, 0] = tile.T[:8, :]
        to_peers(stat.at[index_], s_sem, 2 * index_)

    def normalize(layer, held, into, start, size_):
        def squares(j, total):
            part = xg[held, j, start:start + size_, :].astype(f32)
            return total + jnp.sum(part * part, axis=1, keepdims=True)
        mean = lax.fori_loop(0, T, squares, jnp.zeros((size_, 1), f32)) / D
        scale = lax.rsqrt(mean + 1e-06)

        def body(j, carry):
            by = gain[pl.ds(layer, 1), pl.ds(pl.multiple_of(j * width, width), width)]
            xn[into, j, start:start + size_, :] = (
                xg[held, j, start:start + size_, :].astype(f32) * scale * by).astype(bf16)
            return carry
        lax.fori_loop(0, T, body, 0)

    def project(layer, held, start, size_, into, h):
        def body(j, carry):
            block = wvg[layer, h, pl.ds(pl.multiple_of(j * width, width), width), :]
            part = jnp.dot(xn[held, j, start:start + size_, :], block, preferred_element_type=f32)

            @pl.when(j == 0)
            def _():
                acc[start:start + size_, :] = part

            @pl.when(j > 0)
            def _():
                acc[start:start + size_, :] += part
            return carry
        lax.fori_loop(0, T, body, 0)
        glu = acc[start:start + size_, :half] * jax.nn.sigmoid(acc[start:start + size_, half:])
        into[start:start + size_, pl.ds(pl.multiple_of(h * half, half), half)] = glu.astype(bf16)

    def x_right(layer):
        return pltpu.make_async_remote_copy(
            src_ref=xg.at[layer, t, pl.ds(rows, PAD)], dst_ref=xg.at[layer, t, pl.ds(0, PAD)],
            send_sem=h_sem.at[layer, 0], recv_sem=h_sem.at[layer, 2],
            device_id={"sp": s + 1}, device_id_type=MESH)

    def x_left(layer):
        return pltpu.make_async_remote_copy(
            src_ref=xg.at[layer, t, pl.ds(PAD, PAD)], dst_ref=xg.at[layer, t, pl.ds(PAD + rows, PAD)],
            send_sem=h_sem.at[layer, 1], recv_sem=h_sem.at[layer, 3],
            device_id={"sp": s - 1}, device_id_type=MESH)

    def sides_of(layer):
        if layer == 0:
            return s == 1, s == last - 1, s == last - 1, s == 1
        return s < last, s > 0, s > 0, s < last

    def halo(layer, do):
        sends_right, sends_left, from_left, from_right = sides_of(layer)
        if do == "send":
            pl.when(sends_right)(lambda: x_right(layer).start())
            pl.when(sends_left)(lambda: x_left(layer).start())
        elif do == "begin":
            @pl.when(from_left)
            def _():
                wait_bytes(xg.at[layer, t, pl.ds(0, PAD)], h_sem.at[layer, 2])
                halo_spread(layer, 0).begin()

            @pl.when(from_right)
            def _():
                wait_bytes(xg.at[layer, t, pl.ds(0, PAD)], h_sem.at[layer, 3])
                halo_spread(layer, 1).begin()
        elif do == "drain":
            @pl.when(sends_right)
            def _():
                wait_bytes(xg.at[layer, t, pl.ds(0, PAD)], h_sem.at[layer, 0])

            @pl.when(sends_left)
            def _():
                wait_bytes(xg.at[layer, t, pl.ds(0, PAD)], h_sem.at[layer, 1])
            pl.when(from_left)(lambda: halo_spread(layer, 0).drain())
            pl.when(from_right)(lambda: halo_spread(layer, 1).drain())
        else:
            pl.when(from_left)(lambda: getattr(halo_spread(layer, 0), do)())
            pl.when(from_right)(lambda: getattr(halo_spread(layer, 1), do)())

    def convolve(layer, between):
        padf[...] = pad[layer].astype(f32)
        block = 64
        sums, squares = [], []
        for r in range(0, rows, block):
            total = jnp.zeros((block, chans), f32)
            for k in range(n_taps):
                start = r + PAD - reach + k
                total = total + taps[k, layer:layer + 1, :] * padf[start:start + block, :]
            mean = jnp.sum(total, axis=1, keepdims=True) / chans
            shifted = total - mean
            convg[layer, t, r:r + block, :] = shifted.astype(bf16)
            sums.append(mean)
            squares.append(jnp.sum(shifted * shifted, axis=1, keepdims=True))
            if r + block == rows // 2:
                conv_spread(layer, 0).begin()
                between()
        share(layer, [jnp.concatenate(sums, 0), jnp.concatenate(squares, 0)])
        conv_spread(layer, 1).begin()

    def activate(layer):
        got = columns_of(layer)
        means = [got[:, 8 * d:8 * d + 1] for d in range(T)]
        center = sum(means[1:], means[0]) / T
        apart = [m - center for m in means]
        square = sum((got[:, 8 * d + 1:8 * d + 2] + chans * (apart[d] * apart[d]) for d in range(T)), jnp.zeros((rows, 1), f32))
        scale = lax.rsqrt(square / C + 1e-05)
        for d in range(T):
            j = lax.rem(t + T - d, T)
            by = cgain[j, layer:layer + 1, :]
            normal = (convg[layer, j].astype(f32) + apart[d]) * scale
            act[j] = jax.nn.silu(normal * by).astype(bf16)

    def add_branch(layer, h):
        part = None
        for j in range(T):
            term = jnp.dot(act[j], wo[layer, h, j * chans:(j + 1) * chans, :], preferred_element_type=f32)
            part = term if part is None else part + term
        cols = half_columns(h)
        x_state[:, cols] = (x_state[:, cols] + part).astype(bf16).astype(f32)

    with scope("stage_wait"):
        staged(first_vg)
    token_copy.wait()
    halo(0, "send")
    each(0, QC, lambda q: inward(first_vg, q, s).start())

    @pl.when(is_end)
    def _():
        each(0, x_chunks, lambda c: end_rows(c, inner).start())

    @pl.when(is_mid)
    def _():
        x_spread().begin()

    with scope("stage_wait2"):
        for stage in after:
            staged(stage)

    def end_sends(what, stage, lo, hi):
        @pl.when(is_end)
        def _():
            if what == "in":
                each(lo, hi, lambda q: inward(stage, q, edge).start())
            else:
                each(lo, hi, lambda q: direct(stage, q).start())

    end_sends("direct", first_vg, 0, shared_from)

    @pl.when(is_mid)
    def _():
        for stage in after:
            each(0, count[stage[1]], lambda q: outward(stage, q, mine).start())

    gain_copy.wait()
    for c in small:
        c.wait()
    for d in range(1, T):
        pltpu.make_async_remote_copy(
            src_ref=cgain.at[t], dst_ref=cgain.at[t], send_sem=g_sem.at[0], recv_sem=g_sem.at[1],
            device_id={"tp": lax.rem(t + d, T)}, device_id_type=MESH).start()
    x_state[...] = xg[0, t, own, :].astype(f32)
    with scope("halo0_begin"):
        halo(0, "begin")

    def first_chunks(q):
        from_inner(first_vg, q, near)
        from_edge(first_vg, q)
    with scope("A_vg0_near_edge"):
        each(0, QC, first_chunks)
    push_in(first_wo, 0, RC)
    push_in(second_vg, 0, QC // 2)

    @pl.when(is_end)
    def _():
        def pass_on(stage):
            def body(q):
                arrived(stage, q, mine)
                across(stage, q, mine).start()
            each(0, count[stage[1]], body)
        for stage in after:
            with scope("end_pass_on"):
                pass_on(stage)
            if stage == first_wo:
                end_sends("in", first_wo, 0, RC)
                end_sends("in", second_vg, 0, QC // 2)
            elif stage == second_vg:
                end_sends("direct", first_wo, 0, RC)

    def edge_relays(lo, hi):
        @pl.when(is_mid)
        def _():
            with scope("edge_relay"):
                each(lo, hi, lambda c: edge_spread(c).relay())

    halo(0, "relay")

    @pl.when(is_mid)
    def _():
        with scope("x0_finish"):
            x_spread().relay()
            x_spread().complete()
    halo(0, "complete")

    @pl.when(is_mid)
    def _():
        with scope("norm0"):
            normalize(0, 0, 0, 0, full)

    def second_chunks(q):
        from_inner(first_vg, q, far)

        @pl.when(is_mid)
        def _():
            wait_bytes(xg.at[0, t, pl.ds(0, x_rows)], f_sem.at[2 + q])
            edge_spread(q).begin()
    with scope("B_vg0_far"):
        each(0, QC, second_chunks)

    @pl.when(is_mid)
    def _():
        with scope("proj0_g"):
            project(0, 0, 0, full, pad.at[0], g)
    edge_relays(0, x_chunks // 2)
    with scope("C1_wo0_near"):
        each(0, RC // 2, lambda q: from_inner(first_wo, q, near))
    edge_relays(x_chunks // 2, x_chunks - 1)
    with scope("C1_wo0_near"):
        each(RC // 2, RC, lambda q: from_inner(first_wo, q, near))
    edge_relays(x_chunks - 1, x_chunks)
    push_in(second_vg, QC // 2, QC // 2 + 1)
    end_sends("in", second_vg, QC // 2, QC)

    @pl.when(is_mid)
    def _():
        with scope("edge_complete"):
            each(0, x_chunks, lambda c: edge_spread(c).complete())
        with scope("norm_e"):
            normalize(0, L, 1, PAD, rows)
        with scope("proj0e_g"):
            project(0, 1, PAD, rows, glu_out, g)

    with scope("D1_vg1_near"):
        from_inner(second_vg, 0, near)

    @pl.when(is_mid)
    def _():
        with scope("wait_vg0"):
            others_arrived(first_vg)
        with scope("proj0e"):
            project(0, 1, PAD, rows, glu_out, other)
    with scope("C2_wo0_edge"):
        each(0, RC // 2, lambda q: from_edge(first_wo, q))

    @pl.when(is_mid)
    def _():
        with scope("proj0"):
            project(0, 0, 0, full, pad.at[0], other)

    sends_right, sends_left, _, _ = sides_of(0)

    @pl.when(sends_right)
    def _():
        glu_out[0:PAD, :] = jnp.zeros((PAD, chans), bf16)
        glu_out[PAD + rows:, :] = pad[0, PAD:2 * PAD, :]
        pad[0, 0:PAD, :] = glu_out[rows:rows + PAD, :]

    @pl.when(sends_left)
    def _():
        glu_out[0:PAD, :] = pad[0, rows:rows + PAD, :]
        glu_out[PAD + rows:, :] = jnp.zeros((PAD, chans), bf16)
        pad[0, PAD + rows:, :] = glu_out[PAD:2 * PAD, :]

    @pl.when(is_mid)
    def _():
        end_glu(edge).start()

    with scope("D1_vg1_near"):
        each(1, QC // 2, lambda q: from_inner(second_vg, q, near))
    with scope("C2_wo0_edge"):
        each(RC // 2, RC, lambda q: from_edge(first_wo, q))
    push_in(second_vg, QC // 2 + 1, QC)
    end_sends("in", second_wo, 0, RC)

    @pl.when(is_end)
    def _():
        with scope("end_glu_wait"):
            wait_bytes(glu_out, f_sem.at[2 + x_chunks])

    with scope("conv0"):
        convolve(0, lambda: None)
    with scope("D2_vg1_edge"):
        from_edge(second_vg, 0)
    with scope("C3_wo0_far"):
        each(0, RC // 2, lambda q: from_inner(first_wo, q, far))
    with scope("conv0_relay"):
        conv_spread(0, 0).relay()
    with scope("C3_wo0_far"):
        pl.when(is_end)(lambda: each(RC // 2, RC, lambda q: from_inner(first_wo, q, far)))
    with scope("conv0_relay"):
        conv_spread(0, 1).relay()
    with scope("C3_wo0_far"):
        pl.when(is_mid)(lambda: each(RC // 2, RC, lambda q: from_inner(first_wo, q, far)))
    with scope("conv0_complete"):
        conv_spread(0, 0).complete()
        conv_spread(0, 1).complete()
        wait_bytes(cgain.at[pl.ds(0, T - 1)], g_sem.at[1])
    with scope("act0"):
        activate(0)
    with scope("D2_vg1_edge"):
        from_edge(second_vg, 1)
    push_in(second_wo, 0, RC // 2)

    def next_x(h, turn):
        add_branch(0, h)
        cols = half_columns(h)
        xg[1, t, own, cols] = x_state[:, cols].astype(bf16)
        half_spread(h, turn).begin()
    with scope("out0_g"):
        next_x(g, 0)
    with scope("D2_vg1_near"):
        from_inner(second_vg, QC // 2, near)
    with scope("wait_wo0"):
        others_arrived(first_wo)
    with scope("out0"):
        next_x(other, 1)
    halo(1, "send")
    end_sends("direct", second_vg, 0, QC)
    end_sends("direct", second_wo, 0, RC)
    with scope("D3_vg1_near"):
        each(QC // 2 + 1, QC, lambda q: from_inner(second_vg, q, near))
    with scope("D3_vg1_edge"):
        from_edge(second_vg, 2)
    with scope("D4_vg1_far"):
        from_inner(second_vg, 0, far)
    with scope("D3_vg1_edge"):
        each(3, QC, lambda q: from_edge(second_vg, q))
    push_in(second_wo, RC // 2, RC)
    with scope("D4_vg1_far"):
        from_inner(second_vg, 1, far)
    with scope("x1_relay"):
        half_spread(g, 0).relay()
    with scope("halo1_begin"):
        pl.when(is_end)(lambda: halo(1, "begin"))
    with scope("D4_vg1_far"):
        from_inner(second_vg, 2, far)
    with scope("x1_relay"):
        pl.when(is_end)(half_spread(other, 1).relay)
    with scope("halo1_relay"):
        pl.when(is_end)(lambda: halo(1, "relay"))
    with scope("E1_wo1_edge"):
        each(0, RC // 2, lambda q: from_edge(second_wo, q))
    with scope("D4_vg1_far"):
        each(3, QC, lambda q: from_inner(second_vg, q, far))
    with scope("E1_wo1_edge"):
        each(RC // 2, RC, lambda q: from_edge(second_wo, q))
    with scope("halo1_begin"):
        pl.when(is_mid)(lambda: halo(1, "begin"))
    with scope("x1_relay"):
        pl.when(is_mid)(half_spread(other, 1).relay)
    with scope("E1_wo1_near"):
        pl.when(is_mid)(lambda: each(0, RC // 2, lambda q: from_inner(second_wo, q, near)))
    with scope("halo1_relay"):
        pl.when(is_mid)(lambda: halo(1, "relay"))
    with scope("x1_complete"):
        half_spread(g, 0).complete()
        half_spread(other, 1).complete()
        halo(1, "complete")
    with scope("norm1"):
        normalize(1, 1, 0, 0, full)
    with scope("E1_wo1_near"):
        pl.when(is_mid)(lambda: each(RC // 2, RC, lambda q: from_inner(second_wo, q, near)))
    with scope("proj1_g"):
        project(1, 0, 0, full, pad.at[1], g)
    with scope("E2_m"):
        pl.when(is_mid)(lambda: each(0, RC // 2, lambda q: from_inner(second_wo, q, far)))
    with scope("E1_e"):
        pl.when(is_end)(lambda: each(0, RC // 2, lambda q: from_inner(second_wo, q, near)))
    with scope("wait_vg1"):
        others_arrived(second_vg)
    with scope("proj1"):
        project(1, 0, 0, full, pad.at[1], other)
    with scope("E1_e"):
        pl.when(is_end)(lambda: each(RC // 2, RC, lambda q: from_inner(second_wo, q, near)))
    with scope("E2_m"):
        pl.when(is_mid)(lambda: each(RC // 2, RC, lambda q: from_inner(second_wo, q, far)))
    with scope("conv1"):
        convolve(1, lambda: None)
    with scope("E2_e"):
        pl.when(is_end)(lambda: each(0, RC // 2, lambda q: from_inner(second_wo, q, far)))
    with scope("conv1_relay"):
        conv_spread(1, 0).relay()
    with scope("E2_e"):
        pl.when(is_end)(lambda: each(RC // 2, RC, lambda q: from_inner(second_wo, q, far)))
    with scope("conv1_relay"):
        conv_spread(1, 1).relay()
    with scope("conv1_gather"):
        conv_spread(1, 0).complete()
        conv_spread(1, 1).complete()
    with scope("act1"):
        activate(1)

    def last_x(h, turn):
        add_branch(1, h)
        cols = half_columns(h)
        leaving[:, cols] = x_state[:, cols].astype(bf16)
        pltpu.make_async_copy(leaving.at[:, cols], x_out.at[:, cols], o_sem.at[turn]).start()
    with scope("out1_g"):
        last_x(g, 0)
    with scope("wait_wo1"):
        others_arrived(second_wo)
    with scope("out1"):
        last_x(other, 1)
    xf = x_state[...]
    share(L, [jnp.sum(xf * xf, axis=1, keepdims=True)])

    halo(0, "drain")
    halo(1, "drain")
    for layer in range(L):
        for part_ in range(2):
            conv_spread(layer, part_).drain()
    half_spread(g, 0).drain()
    half_spread(other, 1).drain()
    wait_bytes(cgain.at[pl.ds(0, T - 1)], g_sem.at[0])
    whole = L * (depth + out_rows * out_half // (2 * half))
    later = whole - depth

    def sent(length, k):
        wait_bytes(wvg.at[0, 0, pl.ds(0, length)], send_w.at[k])

    def sent_twice(length, k):
        wait_bytes(wvg.at[0, :, pl.ds(0, length)], send_w.at[k])

    def sent_all(k):
        sent_twice(later * (n - 1) // G, k)

    @pl.when(is_mid)
    def _():
        x_spread().drain()
        each(0, x_chunks, lambda c: edge_spread(c).drain())
        wait_bytes(glu_out, f_sem.at[1])
        sent_twice(whole, IN)
        sent_twice(3 * later // 2, OUT)
        sent((QC - shared_from) * size["vg"], YE)
        sent_twice(whole, Y)

    @pl.when(is_end)
    def _():
        wait_bytes(xg.at[0, t, own], f_sem.at[0])
        sent(whole, IN)
        sent(later + shared_from * size["vg"], UN)
        sent_twice(3 * later // 2, Y)

    with scope("final_stat"):
        got = columns_of(L)
        for index_ in range(L + 1):
            wait_bytes(stat.at[index_, pl.ds(0, T - 1)], s_sem.at[2 * index_])
    total = sum((got[:, 8 * d:8 * d + 1] for d in range(1, T)), got[:, 0:1])
    scale_out[...] = lax.rsqrt(total / D + 1e-06)
    for turn in range(G):
        wait_bytes(leaving.at[:, pl.ds(0, out_half)], o_sem.at[turn])


def scale_rows(x, scale, gain, out):
    out[...] = (x[...].astype(jnp.float32) * scale[...] * gain[...]).astype(out.dtype)


def quad_on_device(G, n, T, tokens, norm_gain, value_w, gate_w, taps, cgain, out_w, fgain):
    L = norm_gain.shape[0]
    if L != 2:
        return on_device(G, n, T, tokens, norm_gain, value_w, gate_w, taps, cgain, out_w, fgain)
    rows, width = tokens.shape
    depth, chans = value_w.shape[1:]
    D, C = width * T, chans * T
    bf16, f32 = jnp.bfloat16, jnp.float32
    dma = pltpu.SemaphoreType.DMA
    vmem = pl.BlockSpec(memory_space=pltpu.VMEM)
    hbm = pl.BlockSpec(memory_space=pltpu.HBM)
    full = rows + 2 * PAD
    x, scale = pl.pallas_call(
        functools.partial(quad_kernel, G, n, T, L),
        out_shape=(jax.ShapeDtypeStruct((rows, width), bf16), jax.ShapeDtypeStruct((rows, 1), f32)),
        in_specs=[hbm] * 7,
        out_specs=(pl.BlockSpec(memory_space=pl.ANY), vmem),
        scratch_shapes=[
            pltpu.VMEM((L, G, D, 2 * chans // G), bf16),
            pltpu.VMEM((L, G, C, width // G), bf16),
            pltpu.VMEM((L + 1, T, full, width), bf16),
            pltpu.VMEM((2, T, full, width), bf16),
            pltpu.VMEM((full, chans), bf16),
            pltpu.VMEM((full, 2 * chans // G), f32),
            pltpu.VMEM((L, full, chans), bf16),
            pltpu.VMEM((full, chans), f32),
            pltpu.VMEM((L, T, rows, chans), bf16),
            pltpu.VMEM((T, rows, chans), bf16),
            pltpu.VMEM((L + 1, T, 8, rows), f32),
            pltpu.VMEM((rows, width), f32),
            pltpu.VMEM((rows, width), bf16),
            pltpu.VMEM(norm_gain.shape, f32),
            pltpu.VMEM((taps.shape[1], L, chans), f32),
            pltpu.VMEM((T,) + cgain.shape, f32),
            dma((2 * L + 4,)),
            dma((L * (QC + RC), 3)), dma((2 * L,)), dma((5,)),
            dma((1 + G, 3)), dma((QC, 3)), dma((L, 2, 3)), dma((2 * (L + 1),)),
            dma((L, 4)), dma((L, 2, 3)), dma((2,)), dma((QC + 3,)), dma((G,)),
        ],
        compiler_params=pltpu.CompilerParams(
            collective_id=0, has_side_effects=True, vmem_limit_bytes=56 * 2**20
        ),
    )(tokens, norm_gain, value_w, gate_w, taps.transpose(1, 0, 2), cgain, out_w)
    step = rows // EPILOGUE
    return pl.pallas_call(
        scale_rows,
        grid=(EPILOGUE,),
        out_shape=jax.ShapeDtypeStruct((rows, width), bf16),
        in_specs=[
            pl.BlockSpec((step, width), lambda i: (i, 0)),
            pl.BlockSpec((step, 1), lambda i: (i, 0)),
            pl.BlockSpec((1, width), lambda i: (0, 0)),
        ],
        out_specs=pl.BlockSpec((step, width), lambda i: (i, 0)),
        compiler_params=pltpu.CompilerParams(vmem_limit_bytes=60 * 2**20),
    )(x, scale, fgain.reshape(1, width))


def tokens_f32(tokens, xg, t):
    return xg[0, t].astype(jnp.float32)


def on_device(G, n, T, tokens, norm_gain, value_w, gate_w, taps, cgain, out_w, fgain):
    L = norm_gain.shape[0]
    rows, width = tokens.shape
    depth, chans = value_w.shape[1:]
    D, C = width * T, chans * T
    bf16, f32 = jnp.bfloat16, jnp.float32
    dma = pltpu.SemaphoreType.DMA
    vmem = pl.BlockSpec(memory_space=pltpu.VMEM)
    hbm = pl.BlockSpec(memory_space=pl.ANY)
    P_ = L * (Q + 1)
    peers = max(G - 1, 1)
    return pl.pallas_call(
        functools.partial(kernel, G, n, T, L),
        out_shape=jax.ShapeDtypeStruct((rows, width), bf16),
        in_specs=[hbm, vmem, hbm, hbm, vmem, vmem, hbm, vmem],
        out_specs=vmem,
        scratch_shapes=[
            pltpu.VMEM((L, G, D, 2 * chans // G), bf16),
            pltpu.VMEM((L, G, C, width // G), bf16),
            pltpu.VMEM((L + 1, T, rows, width), bf16),
            pltpu.VMEM((2, T, rows, width), bf16),
            pltpu.VMEM((rows, chans), bf16),
            pltpu.VMEM((rows, 2 * chans // G), f32),
            pltpu.VMEM((L, rows + 2 * PAD, chans), bf16),
            pltpu.VMEM((rows + 2 * PAD, chans), f32),
            pltpu.VMEM((rows, chans), f32),
            pltpu.VMEM((L + 1, T, 8, rows), f32),
            pltpu.VMEM((L, T, rows, chans), bf16),
            pltpu.VMEM((rows, width), f32),
            dma((1 + L * G * 3,)),
            dma((P_, n)), dma((P_, n)), dma((P_, n)),
            dma((P_, n, peers)), dma((P_, n, peers)),
            dma((L + 1, T)), dma((L + 1, T)), dma((L, T)), dma((L, T)),
            dma((L + 1, T)), dma((L + 1, T)),
            dma((L, 2)), dma((L, 2)),
            dma((G + 1,)), dma((G + 1,)),
        ],
        compiler_params=pltpu.CompilerParams(
            collective_id=0, has_side_effects=True, vmem_limit_bytes=56 * 2**20
        ),
    )(tokens, norm_gain.reshape(L * T, width), value_w, gate_w, taps, cgain, out_w, fgain.reshape(1, width))


def solution(mesh):
    placed = (
        P(("grp", "sp"), "tp"),
        P(),
        P(None, "sp", "tp"),
        P(None, "sp", "tp"),
        P(None, None, "tp"),
        P(None, "tp"),
        P(None, "sp", "tp"),
        P("tp"),
    )
    G, n, T = (mesh.shape[a] for a in ("grp", "sp", "tp"))
    paired = G == 2 and n == T == 2 * G
    return jax.shard_map(
        functools.partial(quad_on_device if paired else on_device, G, n, T),
        mesh=mesh, in_specs=placed, out_specs=P(("grp", "sp"), "tp"), check_vma=False,
    )
```

```python
import functools

import jax
import jax.numpy as jnp
from jax import lax
from jax.experimental import pallas as pl
from jax.experimental.pallas import tpu as pltpu
from jax.sharding import PartitionSpec as P

MESH = pl.DeviceIdType.MESH
Q = 2
PAD = 16


def kernel(
    G, n, T, L,
    tokens, gain, value_w, gate_w, taps, cgain, out_w, fgain,
    result,
    wvg, wo, xg, xn, glu_out, acc, pad, padf, conv, stat, actg, x_state,
    local_sem, z_recv, right_send, left_send, y_send, y_recv,
    x_send, x_recv, a_send, a_recv, s_send, s_recv, h_send, h_recv, f_send, f_recv,
):
    g, s, t = lax.axis_index("grp"), lax.axis_index("sp"), lax.axis_index("tp")
    rows, width = tokens.shape
    depth, chans = value_w.shape[1:]
    out_rows = out_w.shape[1]
    half = chans // G
    out_half = width // G
    reach = taps.shape[1] // 2
    n_taps = taps.shape[1]
    D = width * T
    C = chans * T
    chunk = depth // Q
    pieces = Q + 1
    f32, bf16 = jnp.float32, jnp.bfloat16
    helped = n >= 4
    last = n - 1
    is_end = (s == 0) | (s == last)
    helper = (s == 1) | (s == last - 1)
    end = jnp.where(s == 1, 0, last)
    inward = jnp.where(s == 0, 1, last - 1)

    def ends_out(p):
        return helped and p < Q

    def to_right_ok(p):
        return s < last - 1 if ends_out(p) else s < last

    def to_left_ok(p):
        return s > 1 if ends_out(p) else s > 0

    def takes(p):
        return jnp.logical_not(is_end) if ends_out(p) else s >= 0

    def by_grp(p, j):
        ok = takes(p) & (j != s)
        if helped and p == 0:
            ok = ok & jnp.logical_not((s == 1) & (j == 0)) & jnp.logical_not((s == last - 1) & (j == last))
        return ok

    def piece(p, h, j):
        layer, q = p // pieces, p % pieces
        if q < Q:
            start = pl.multiple_of(j * depth + q * chunk, chunk)
            return wvg.at[layer, h, pl.ds(start, chunk), :]
        return wo.at[layer, h, pl.ds(pl.multiple_of(j * out_rows, out_rows), out_rows), :]

    locals_ = [pltpu.make_async_copy(tokens, xg.at[0, t], local_sem.at[0])]
    own_rows = pl.ds(pl.multiple_of(s * depth, depth), depth)
    own_out = pl.ds(pl.multiple_of(s * out_rows, out_rows), out_rows)
    count = 1
    per_layer = []
    for layer in range(L):
        group = []
        for h in range(G):
            for k, w in enumerate((value_w, gate_w)):
                group.append(pltpu.make_async_copy(
                    w.at[layer, :, pl.ds(h * half, half)],
                    wvg.at[layer, h, own_rows, pl.ds(k * half, half)],
                    local_sem.at[count]))
                count += 1
            group.append(pltpu.make_async_copy(
                out_w.at[layer, :, pl.ds(h * out_half, out_half)],
                wo.at[layer, h, own_out, :], local_sem.at[count]))
            count += 1
        per_layer.append(group)
    for c in locals_ + sum(per_layer, []):
        c.start()

    barrier = pltpu.get_barrier_semaphore()
    for d in range(1, T):
        pl.semaphore_signal(barrier, inc=1, device_id={"tp": lax.rem(t + d, T)}, device_id_type=MESH)
    for d in range(1, G):
        pl.semaphore_signal(barrier, inc=1, device_id={"grp": lax.rem(g + d, G)}, device_id_type=MESH)

    @pl.when(s > 0)
    def _():
        pl.semaphore_signal(barrier, inc=1, device_id={"sp": s - 1}, device_id_type=MESH)

    @pl.when(s < n - 1)
    def _():
        pl.semaphore_signal(barrier, inc=1, device_id={"sp": s + 1}, device_id_type=MESH)

    sides = jnp.where(s > 0, 1, 0) + jnp.where(s < n - 1, 1, 0)
    pl.semaphore_wait(barrier, (T - 1) + (G - 1) + sides)

    def right(p, j):
        r = piece(p, g, j)
        return pltpu.make_async_remote_copy(
            src_ref=r, dst_ref=r, send_sem=right_send.at[p, j], recv_sem=z_recv.at[p, j],
            device_id={"sp": s + 1}, device_id_type=MESH)

    def left(p, j):
        r = piece(p, g, j)
        return pltpu.make_async_remote_copy(
            src_ref=r, dst_ref=r, send_sem=left_send.at[p, j], recv_sem=z_recv.at[p, j],
            device_id={"sp": s - 1}, device_id_type=MESH)

    def across(p, j, d, h):
        r = piece(p, h, j)
        return pltpu.make_async_remote_copy(
            src_ref=r, dst_ref=r, send_sem=y_send.at[p, j, d - 1], recv_sem=y_recv.at[p, j, d - 1],
            device_id={"grp": lax.rem(g + d, G)}, device_id_type=MESH)

    batches = []
    for layer in range(L):
        base = layer * pieces
        batches += [list(range(base, base + Q)), [base + Q]]

    def own_right(ps):
        for p in ps:
            right(p, s).start()

    def own_left(ps):
        for p in ps:
            left(p, s).start()

    def end_rows(target):
        return pltpu.make_async_remote_copy(
            src_ref=xg.at[0, t], dst_ref=xg.at[L, t], send_sem=f_send.at[0], recv_sem=f_recv.at[0],
            device_id={"sp": target}, device_id_type=MESH)

    def end_piece(d, h, j, target):
        r = piece(0, h, j)
        return pltpu.make_async_remote_copy(
            src_ref=r, dst_ref=r, send_sem=f_send.at[d], recv_sem=f_recv.at[d],
            device_id={"sp": target}, device_id_type=MESH)

    def end_glu(target):
        return pltpu.make_async_remote_copy(
            src_ref=glu_out, dst_ref=pad.at[0, pl.ds(PAD, rows), :],
            send_sem=f_send.at[G], recv_sem=f_recv.at[G],
            device_id={"sp": target}, device_id_type=MESH)

    def relay(b, low, high):
        low, high = min(low, n - 1), min(high, n - 1)
        following = batches[b + 1] if b + 1 < len(batches) else []

        def step(k, carry):
            for p in batches[b]:
                from_left, from_right = s - 1 - k, s + 1 + k

                @pl.when((from_left >= 0) & takes(p))
                def _():
                    j = jnp.maximum(from_left, 0)
                    right(p, j).wait_recv()

                    @pl.when(to_right_ok(p))
                    def _():
                        right(p, j).start()

                    @pl.when(by_grp(p, j))
                    def _():
                        for d in range(1, G):
                            across(p, j, d, g).start()

                @pl.when((from_right < n) & takes(p))
                def _():
                    j = jnp.minimum(from_right, n - 1)
                    left(p, j).wait_recv()

                    @pl.when(to_left_ok(p))
                    def _():
                        left(p, j).start()

                    @pl.when(by_grp(p, j))
                    def _():
                        for d in range(1, G):
                            across(p, j, d, g).start()

            @pl.when((k == s - 1) & (s < (last - 1 if helped and b < 2 else last)))
            def _():
                own_right(following)

            @pl.when((k == n - 2 - s) & (s > (1 if helped and b < 2 else 0)))
            def _():
                own_left(following)

            return carry

        if high > low:
            lax.fori_loop(low, high, step, 0)

    def wait_across(b):
        for p in batches[b]:
            def step(j, carry):
                @pl.when(by_grp(p, j))
                def _():
                    for d in range(1, G):
                        across(p, j, d, lax.rem(g + G - d, G)).wait_recv()
                return carry
            lax.fori_loop(0, n, step, 0)

    def spread(buf, layer, send, recv):
        def copy(bit, m):
            block = buf.at[layer, t ^ m]
            return pltpu.make_async_remote_copy(
                src_ref=block, dst_ref=block, send_sem=send.at[layer, bit + m], recv_sem=recv.at[layer, bit + m],
                device_id={"tp": t ^ bit}, device_id_type=MESH)

        def arrival(bit, m):
            block = buf.at[layer, t ^ bit ^ m]
            return pltpu.make_async_remote_copy(
                src_ref=block, dst_ref=block, send_sem=send.at[layer, bit + m], recv_sem=recv.at[layer, bit + m],
                device_id={"tp": t ^ bit}, device_id_type=MESH)

        bits = []
        bit = T // 2
        while bit >= 1:
            bits.append(bit)
            bit //= 2

        def begin():
            for bit in bits:
                copy(bit, 0).start()

        def finish():
            have, sent = [0], []
            for i, bit in enumerate(bits):
                for m in have:
                    arrival(bit, m).wait_recv()
                    sent.append((bit, m))
                    for lower in bits[i + 1:]:
                        copy(lower, m ^ bit).start()
                have = have + [m ^ bit for m in have]
            return lambda: [copy(bit, m).wait_send() for bit, m in sent]

        return begin, finish

    def exchange(index, columns):
        lane = lax.broadcasted_iota(jnp.int32, (rows, 128), 1)
        tile = jnp.zeros((rows, 128), f32)
        for i, column in enumerate(columns):
            tile = jnp.where(lane == i, column, tile)
        stat[index, 0] = tile.T[:8, :]

        def copy(d):
            return pltpu.make_async_remote_copy(
                src_ref=stat.at[index, 0], dst_ref=stat.at[index, d],
                send_sem=s_send.at[index, d - 1], recv_sem=s_recv.at[index, d - 1],
                device_id={"tp": lax.rem(t + d, T)}, device_id_type=MESH)

        for d in range(1, T):
            copy(d).start()

        def total():
            for d in range(1, T):
                copy(d).wait_recv()
            sums = stat[index, 0]
            for d in range(1, T):
                sums = sums + stat[index, d]
            wide = jnp.concatenate([sums, jnp.zeros((120, rows), f32)], axis=0).T
            for d in range(1, T):
                copy(d).wait_send()
            return [wide[:, i:i + 1] for i in range(len(columns))]

        return total

    def normalize(layer, held, into):
        def squares(j, total):
            part = xg[held, j].astype(f32)
            return total + jnp.sum(part * part, axis=1, keepdims=True)
        mean = lax.fori_loop(0, T, squares, jnp.zeros((rows, 1), f32)) / D
        scale = lax.rsqrt(mean + 1e-06)

        def body(j, carry):
            xn[into, j] = (xg[held, j].astype(f32) * scale * gain[layer * T + j][None, :]).astype(bf16)
            return carry
        lax.fori_loop(0, T, body, 0)

    def project(layer, held, put):
        for h in range(G):
            def body(j, carry):
                block = wvg[layer, h, pl.ds(pl.multiple_of(j * width, width), width), :]
                part = jnp.dot(xn[held, j], block, preferred_element_type=f32)

                @pl.when(j == 0)
                def _():
                    acc[...] = part

                @pl.when(j > 0)
                def _():
                    acc[...] += part
                return carry
            lax.fori_loop(0, T, body, 0)
            glu = acc[:, :half] * jax.nn.sigmoid(acc[:, half:])
            put(h, glu.astype(bf16))

    for c in locals_:
        c.wait()
    spreads = [spread(xg, layer, x_send, x_recv) for layer in range(L)]
    spreads[0][0]()
    for c in sum(per_layer, []):
        c.wait()

    @pl.when(to_right_ok(0))
    def _():
        own_right(batches[0])

    @pl.when(to_left_ok(0))
    def _():
        own_left(batches[0])

    if helped:
        @pl.when(is_end)
        def _():
            end_rows(inward).start()
            for d in range(1, G):
                end_piece(d, lax.rem(g + d, G), s, inward).start()

        @pl.when(s == last - 1)
        def _():
            own_right(batches[1])
            if L > 1:
                own_right(batches[2])

        @pl.when(s == 1)
        def _():
            own_left(batches[1])
            if L > 1:
                own_left(batches[2])

    @pl.when((s == 0) & (s < n - 1))
    def _():
        for b in batches[1:]:
            own_right(b)

    @pl.when((s == n - 1) & (s > 0))
    def _():
        for b in batches[1:]:
            own_left(b)

    x_state[...] = tokens_f32(tokens, xg, t)
    drains = []

    for layer in range(L):
        first, second = 2 * layer, 2 * layer + 1
        if layer == 0:
            relay(first, 0, 1)
        else:
            relay(first, 1, 2)
        drains.append(spreads[layer][1]())
        if helped and layer == 0:
            @pl.when(jnp.logical_not(is_end))
            def _():
                normalize(layer, layer, 0)
        else:
            normalize(layer, layer, 0)
        relay(first, 1 if layer == 0 else 2, n)
        begin, finish = spread(xg, L, x_send, x_recv)
        if helped and layer == 0:
            @pl.when(helper)
            def _():
                end_rows(end).wait_recv()
                begin()

        relay(second, 0, 1)

        def put(h, value):
            pad[layer, PAD:PAD + rows, h * half:(h + 1) * half] = value

        def put_out(h, value):
            glu_out[:, h * half:(h + 1) * half] = value

        if helped and layer == 0:
            @pl.when(helper)
            def _():
                drain = finish()
                normalize(0, L, 1)
                for d in range(1, G):
                    end_piece(d, lax.rem(g + d, G), end, end).wait_recv()
                drain()

            wait_across(first)

            @pl.when(helper)
            def _():
                project(0, 1, put_out)
                end_glu(end).start()

            @pl.when(jnp.logical_not(is_end))
            def _():
                project(0, 0, put)

            @pl.when(helper)
            def _():
                end_glu(end).wait_send()

            @pl.when(is_end)
            def _():
                end_rows(inward).wait_send()
                for d in range(1, G):
                    end_piece(d, lax.rem(g + d, G), s, inward).wait_send()
                end_glu(inward).wait_recv()
        else:
            wait_across(first)
            project(layer, 0, put)

        def to_right():
            return pltpu.make_async_remote_copy(
                src_ref=pad.at[layer, pl.ds(rows, PAD), :], dst_ref=pad.at[layer, pl.ds(0, PAD), :],
                send_sem=h_send.at[layer, 0], recv_sem=h_recv.at[layer, 0],
                device_id={"sp": s + 1}, device_id_type=MESH)

        def to_left():
            return pltpu.make_async_remote_copy(
                src_ref=pad.at[layer, pl.ds(PAD, PAD), :], dst_ref=pad.at[layer, pl.ds(PAD + rows, PAD), :],
                send_sem=h_send.at[layer, 1], recv_sem=h_recv.at[layer, 1],
                device_id={"sp": s - 1}, device_id_type=MESH)

        @pl.when(s < n - 1)
        def _():
            to_right().start()

        @pl.when(s > 0)
        def _():
            to_left().start()

        @pl.when(s == 0)
        def _():
            pad[layer, 0:PAD, :] = jnp.zeros((PAD, chans), bf16)

        @pl.when(s == n - 1)
        def _():
            pad[layer, PAD + rows:, :] = jnp.zeros((PAD, chans), bf16)

        relay(second, 1, 2)

        @pl.when(s > 0)
        def _():
            to_right().wait_recv()

        @pl.when(s < n - 1)
        def _():
            to_left().wait_recv()

        padf[...] = pad[layer].astype(f32)
        block = 64
        sums, squares = [], []
        for r in range(0, rows, block):
            total = jnp.zeros((block, chans), f32)
            for k in range(n_taps):
                start = r + PAD - reach + k
                total = total + taps[layer, k][None, :] * padf[start:start + block, :]
            conv[r:r + block, :] = total
            sums.append(jnp.sum(total, axis=1, keepdims=True))
            squares.append(jnp.sum(total * total, axis=1, keepdims=True))
        totals = exchange(layer, [jnp.concatenate(sums, 0), jnp.concatenate(squares, 0)])
        relay(second, 2, n)
        if layer + 1 < L:
            relay(second + 1, 0, 1)
        total, square = totals()
        center = total / C
        spread_ = square / C - center * center
        normal = (conv[...] - center) * lax.rsqrt(spread_ + 1e-05)
        actg[layer, t] = jax.nn.silu(normal * cgain[layer][None, :]).astype(bf16)
        act_begin, act_finish = spread(actg, layer, a_send, a_recv)
        act_begin()
        drains.append(act_finish())
        wait_across(second)
        for h in range(G):
            part = None
            for j in range(T):
                term = jnp.dot(actg[layer, j], wo[layer, h, j * chans:(j + 1) * chans, :], preferred_element_type=f32)
                part = term if part is None else part + term
            cols = slice(h * out_half, (h + 1) * out_half)
            x_state[:, cols] = (x_state[:, cols] + part).astype(bf16).astype(f32)
        if layer + 1 < L:
            xg[layer + 1, t] = x_state[...].astype(bf16)
            spreads[layer + 1][0]()

        @pl.when(s < n - 1)
        def _():
            to_right().wait_send()

        @pl.when(s > 0)
        def _():
            to_left().wait_send()

    xf = x_state[...]
    totals = exchange(L, [jnp.sum(xf * xf, axis=1, keepdims=True)])

    for drain in drains:
        drain()

    def drain_step(j, carry):
        for p in range(L * pieces):
            came = (j == s) | takes(p)

            @pl.when((j <= s) & to_right_ok(p) & came)
            def _():
                right(p, j).wait_send()

            @pl.when((j >= s) & to_left_ok(p) & came)
            def _():
                left(p, j).wait_send()

            @pl.when(by_grp(p, j))
            def _():
                for d in range(1, G):
                    across(p, j, d, g).wait_send()
        return carry
    lax.fori_loop(0, n, drain_step, 0)

    (total,) = totals()
    scale = lax.rsqrt(total / D + 1e-06)
    result[...] = (x_state[...] * scale * fgain[...]).astype(bf16)


QC = 8
RC = 4
XC = 4
EPILOGUE = 2


def quad_kernel(
    G, n, T, L,
    tokens, gain_hbm, value_w, gate_w, taps_hbm, cgain_hbm, out_w,
    x_out, scale_out,
    wvg, wo, xg, xn, glu_out, acc, pad, padf, convg, act, column, stat, x_state, leaving, gain, taps, cgain,
    local_sem, recv_z, recv_o, send_w, x_sem, e_sem, c_sem, s_sem, h_sem, hs_sem, g_sem, f_sem, o_sem,
):
    g, s, t = lax.axis_index("grp"), lax.axis_index("sp"), lax.axis_index("tp")
    rows, width = tokens.shape
    depth, chans = value_w.shape[1:]
    out_rows = out_w.shape[1]
    half = chans // G
    out_half = width // G
    n_taps = taps.shape[0]
    reach = n_taps // 2
    D = width * T
    C = chans * T
    full = rows + 2 * PAD
    pieces = QC + RC
    size = {"vg": depth // QC, "wo": out_rows // RC}
    count = {"vg": QC, "wo": RC}
    shared_from = 3 * QC // 4
    f32, bf16 = jnp.float32, jnp.bfloat16
    last = n - 1
    low = s < n // 2
    is_end = (s == 0) | (s == last)
    is_mid = jnp.logical_not(is_end)
    inner = jnp.where(low, s + 1, s - 1)
    outer = jnp.where(low, s - 1, s + 1)
    edge, mine, near, far = (jnp.where(low, a, last - a) for a in (0, 1, n - 2, n - 1))
    other = lax.rem(g + 1, G)
    x_chunks = XC
    x_rows = rows // x_chunks
    own = pl.ds(PAD, rows)
    first_vg, first_wo, second_vg, second_wo = (0, "vg"), (0, "wo"), (1, "vg"), (1, "wo")
    after = (first_wo, second_vg, second_wo)
    scope = jax.named_scope
    IN, OUT, Y, YE, UN = range(5)

    def index(stage, q):
        layer, kind = stage
        return layer * pieces + (0 if kind == "vg" else QC) + q

    def order_of(stage):
        return stage[0] * 2 + (0 if stage[1] == "vg" else 1)

    def place(j):
        return jnp.where(j == near, 1, jnp.where(j == far, 2, 0))

    def piece(stage, q, h, j):
        layer, kind = stage
        step = size[kind]
        per = depth if kind == "vg" else out_rows
        ref = wvg if kind == "vg" else wo
        return ref.at[layer, h, pl.ds(pl.multiple_of(j * per + q * step, step), step), :]

    def wait_bytes(ref, sem):
        pltpu.make_async_copy(ref, ref, sem).wait()

    own_rows = pl.ds(pl.multiple_of(s * depth, depth), depth)
    own_out = pl.ds(pl.multiple_of(s * out_rows, out_rows), out_rows)

    def stage_in(stage):
        layer, kind = stage
        sem = local_sem.at[order_of(stage)]
        for h in range(G):
            if kind == "vg":
                for k, w in enumerate((value_w, gate_w)):
                    pltpu.make_async_copy(
                        w.at[layer, :, pl.ds(h * half, half)],
                        wvg.at[layer, h, own_rows, pl.ds(k * half, half)], sem).start()
            else:
                pltpu.make_async_copy(
                    out_w.at[layer, :, pl.ds(h * out_half, out_half)],
                    wo.at[layer, h, own_out, :], sem).start()

    def staged(stage):
        layer, kind = stage
        ref = wvg.at[layer, :, own_rows] if kind == "vg" else wo.at[layer, :, own_out]
        wait_bytes(ref, local_sem.at[order_of(stage)])

    token_copy = pltpu.make_async_copy(tokens, xg.at[0, t, own], local_sem.at[2 * L])
    gain_copy = pltpu.make_async_copy(cgain_hbm, cgain.at[t], local_sem.at[2 * L + 1])
    small = [
        pltpu.make_async_copy(gain_hbm, gain, local_sem.at[2 * L + 2]),
        pltpu.make_async_copy(taps_hbm, taps, local_sem.at[2 * L + 3]),
    ]
    stage_in(first_vg)
    token_copy.start()
    gain_copy.start()
    for stage in after:
        stage_in(stage)
    for c in small:
        c.start()

    barrier = pltpu.get_barrier_semaphore()
    for d in range(1, T):
        pl.semaphore_signal(barrier, inc=1, device_id={"tp": lax.rem(t + d, T)}, device_id_type=MESH)
    pl.semaphore_signal(barrier, inc=1, device_id={"grp": other}, device_id_type=MESH)

    @pl.when(s > 0)
    def _():
        pl.semaphore_signal(barrier, inc=1, device_id={"sp": s - 1}, device_id_type=MESH)

    @pl.when(s < last)
    def _():
        pl.semaphore_signal(barrier, inc=1, device_id={"sp": s + 1}, device_id_type=MESH)

    blank = jnp.zeros((T, PAD, width), bf16)

    @pl.when(s < n // 2)
    def _():
        xg[0, :, 0:PAD, :] = blank

    @pl.when(s >= n // 2)
    def _():
        xg[0, :, PAD + rows:, :] = blank

    @pl.when(s == 0)
    def _():
        xg[1, :, 0:PAD, :] = blank

    @pl.when(s == last)
    def _():
        xg[1, :, PAD + rows:, :] = blank

    sides = jnp.where(s > 0, 1, 0) + jnp.where(s < last, 1, 0)
    pl.semaphore_wait(barrier, (T - 1) + (G - 1) + sides)

    def arrived(stage, q, j):
        wait_bytes(piece(stage, q, g, j), recv_z.at[index(stage, q), place(j)])

    def inward(stage, q, j):
        r, p = piece(stage, q, g, j), index(stage, q)
        there = jnp.where(is_end, 0, jnp.where(j == mine, 1, 2))
        return pltpu.make_async_remote_copy(
            src_ref=r, dst_ref=r, send_sem=send_w.at[IN], recv_sem=recv_z.at[p, there],
            device_id={"sp": inner}, device_id_type=MESH)

    def outward(stage, q, j):
        r, p = piece(stage, q, g, j), index(stage, q)
        return pltpu.make_async_remote_copy(
            src_ref=r, dst_ref=r, send_sem=send_w.at[OUT], recv_sem=recv_z.at[p, place(j)],
            device_id={"sp": outer}, device_id_type=MESH)

    def across(stage, q, j, send=Y):
        r = piece(stage, q, g, j)
        return pltpu.make_async_remote_copy(
            src_ref=r, dst_ref=r, send_sem=send_w.at[send],
            recv_sem=recv_o.at[2 * L if stage == second_vg and j is far else order_of(stage)],
            device_id={"grp": other}, device_id_type=MESH)

    def direct(stage, q):
        r = piece(stage, q, other, edge)
        return pltpu.make_async_remote_copy(
            src_ref=r, dst_ref=r, send_sem=send_w.at[UN], recv_sem=recv_o.at[order_of(stage)],
            device_id={"sp": inner}, device_id_type=MESH)

    def others_arrived(stage):
        layer, kind = stage
        per = depth if kind == "vg" else out_rows
        ref = wvg if kind == "vg" else wo
        blocks = n - 2 if stage == second_vg else n - 1
        wait_bytes(ref.at[layer, 0, pl.ds(0, blocks * per)], recv_o.at[order_of(stage)])

    def far_arrived():
        wait_bytes(wvg.at[1, 0, pl.ds(0, depth)], recv_o.at[2 * L])

    def end_rows(c, target):
        src = pl.ds(pl.multiple_of(PAD + c * x_rows, PAD), x_rows)
        return pltpu.make_async_remote_copy(
            src_ref=xg.at[0, t, src], dst_ref=xg.at[L, t, src], send_sem=f_sem.at[0], recv_sem=f_sem.at[2 + c],
            device_id={"sp": target}, device_id_type=MESH)

    def end_glu(target):
        return pltpu.make_async_remote_copy(
            src_ref=glu_out, dst_ref=pad.at[0], send_sem=f_sem.at[1], recv_sem=f_sem.at[2 + x_chunks],
            device_id={"sp": target}, device_id_type=MESH)

    def each(low_, high_, body):
        def step(q, carry):
            body(q)
            return carry
        lax.fori_loop(low_, high_, step, 0)

    def from_inner(stage, q, j, over_y=True):
        def serve():
            with scope("w_inner"):
                arrived(stage, q, j)
            if stage != first_vg:
                @pl.when(is_mid)
                def _():
                    outward(stage, q, j).start()
            if over_y:
                across(stage, q, j).start()
        if stage == first_vg:
            pl.when(is_mid)(serve)
        else:
            serve()

    def from_edge(stage, q):
        @pl.when(is_mid)
        def _():
            with scope("w_edge"):
                arrived(stage, q, edge)
            inward(stage, q, edge).start()
            if stage == first_vg:
                @pl.when(q >= shared_from)
                def _():
                    across(stage, q, edge, YE).start()

    def push_in(stage, lo, hi):
        @pl.when(is_mid)
        def _():
            each(lo, hi, lambda q: inward(stage, q, mine).start())

    class Spread:
        def __init__(self, view, three, two, sems):
            self.view, self.three, self.two, self.sems = view, three, two, sems

        def copy(self, j, bit, k):
            block = self.view(j)
            return pltpu.make_async_remote_copy(
                src_ref=block, dst_ref=block, send_sem=self.sems(2), recv_sem=self.sems(k),
                device_id={"tp": t ^ bit}, device_id_type=MESH)

        def begin(self):
            self.copy(t, T // 2, 0).start()
            self.copy(t, 1, 1).start()

        def relay(self):
            wait_bytes(self.view(t), self.sems(0))
            self.copy(t ^ (T // 2), 1, 1).start()

        def complete(self):
            wait_bytes(self.two, self.sems(1))

        def drain(self):
            wait_bytes(self.three, self.sems(2))

    def half_columns(h):
        return pl.ds(pl.multiple_of(h * out_half, out_half), out_half)

    def x_spread():
        return Spread(lambda j: xg.at[0, j, own], xg.at[0, pl.ds(0, 3), own], xg.at[0, pl.ds(0, 2), own],
                      lambda k: x_sem.at[0, k])

    def half_spread(h, turn):
        cols = half_columns(h)
        return Spread(lambda j: xg.at[1, j, own, cols], xg.at[1, pl.ds(0, 3), own, cols],
                      xg.at[1, pl.ds(0, 2), own, cols], lambda k: x_sem.at[1 + turn, k])

    def edge_spread(c):
        part = pl.ds(pl.multiple_of(PAD + c * x_rows, PAD), x_rows)
        return Spread(lambda j: xg.at[L, j, part], xg.at[L, pl.ds(0, 3), part], xg.at[L, pl.ds(0, 2), part],
                      lambda k: e_sem.at[c, k])

    def halo_spread(layer, side):
        part = pl.ds(0 if side == 0 else PAD + rows, PAD)
        return Spread(lambda j: xg.at[layer, j, part], xg.at[layer, pl.ds(0, 3), part], xg.at[layer, pl.ds(0, 2), part],
                      lambda k: hs_sem.at[layer, side, k])

    def conv_spread(layer, part_):
        cols = channels_of(g if part_ == 0 else other)
        return Spread(lambda j: convg.at[layer, j, :, cols], convg.at[layer, pl.ds(0, 3), :, cols],
                      convg.at[layer, pl.ds(0, 2), :, cols], lambda k: c_sem.at[layer, part_, k])

    def to_peers(buf, sem, k):
        for d in range(1, T):
            pltpu.make_async_remote_copy(
                src_ref=buf.at[0], dst_ref=buf.at[d], send_sem=sem.at[k], recv_sem=sem.at[k + 1],
                device_id={"tp": lax.rem(t + d, T)}, device_id_type=MESH).start()

    def share(index_, tile):
        stat[index_, 0] = tile.T[:8, :]
        to_peers(stat.at[index_], s_sem, 2 * index_)

    def normalize(layer, held, into, start, size_):
        def squares(j, total):
            part = xg[held, j, start:start + size_, :].astype(f32)
            return total + jnp.sum(part * part, axis=1, keepdims=True)
        mean = lax.fori_loop(0, T, squares, jnp.zeros((size_, 1), f32)) / D
        scale = lax.rsqrt(mean + 1e-06)

        def body(j, carry):
            by = gain[pl.ds(layer, 1), pl.ds(pl.multiple_of(j * width, width), width)]
            xn[into, j, start:start + size_, :] = (
                xg[held, j, start:start + size_, :].astype(f32) * scale * by).astype(bf16)
            return carry
        lax.fori_loop(0, T, body, 0)

    def project(layer, held, start, size_, into, h, part="whole"):
        def body(k, carry):
            j = lax.rem(far + 1 + k, T)
            block = wvg[layer, h, pl.ds(pl.multiple_of(j * width, width), width), :]
            term = jnp.dot(xn[held, j, start:start + size_, :], block, preferred_element_type=f32)

            @pl.when(k == 0)
            def _():
                acc[start:start + size_, :] = term

            @pl.when(k > 0)
            def _():
                acc[start:start + size_, :] += term
            return carry
        lax.fori_loop(T - 1 if part == "late" else 0, T - 1 if part == "early" else T, body, 0)
        if part != "early":
            glu = acc[start:start + size_, :half] * jax.nn.sigmoid(acc[start:start + size_, half:])
            into[start:start + size_, pl.ds(pl.multiple_of(h * half, half), half)] = glu.astype(bf16)

    def x_right(layer):
        return pltpu.make_async_remote_copy(
            src_ref=xg.at[layer, t, pl.ds(rows, PAD)], dst_ref=xg.at[layer, t, pl.ds(0, PAD)],
            send_sem=h_sem.at[layer, 0], recv_sem=h_sem.at[layer, 2],
            device_id={"sp": s + 1}, device_id_type=MESH)

    def x_left(layer):
        return pltpu.make_async_remote_copy(
            src_ref=xg.at[layer, t, pl.ds(PAD, PAD)], dst_ref=xg.at[layer, t, pl.ds(PAD + rows, PAD)],
            send_sem=h_sem.at[layer, 1], recv_sem=h_sem.at[layer, 3],
            device_id={"sp": s - 1}, device_id_type=MESH)

    def sides_of(layer):
        if layer == 0:
            return s == 1, s == last - 1, s == last - 1, s == 1
        return s < last, s > 0, s > 0, s < last

    def halo(layer, do):
        sends_right, sends_left, from_left, from_right = sides_of(layer)
        if do == "send":
            pl.when(sends_right)(lambda: x_right(layer).start())
            pl.when(sends_left)(lambda: x_left(layer).start())
        elif do == "begin":
            @pl.when(from_left)
            def _():
                wait_bytes(xg.at[layer, t, pl.ds(0, PAD)], h_sem.at[layer, 2])
                halo_spread(layer, 0).begin()

            @pl.when(from_right)
            def _():
                wait_bytes(xg.at[layer, t, pl.ds(0, PAD)], h_sem.at[layer, 3])
                halo_spread(layer, 1).begin()
        elif do == "drain":
            @pl.when(sends_right)
            def _():
                wait_bytes(xg.at[layer, t, pl.ds(0, PAD)], h_sem.at[layer, 0])

            @pl.when(sends_left)
            def _():
                wait_bytes(xg.at[layer, t, pl.ds(0, PAD)], h_sem.at[layer, 1])
            pl.when(from_left)(lambda: halo_spread(layer, 0).drain())
            pl.when(from_right)(lambda: halo_spread(layer, 1).drain())
        else:
            pl.when(from_left)(lambda: getattr(halo_spread(layer, 0), do)())
            pl.when(from_right)(lambda: getattr(halo_spread(layer, 1), do)())

    def channels_of(h):
        return pl.ds(pl.multiple_of(h * half, half), half)

    def convolve(layer, h, turn):
        @pl.when(s >= 0)
        def _():
            rows_of(layer, h, turn)
        if turn == G - 1:
            share(layer, column[...])
        conv_spread(layer, turn).begin()

    def rows_of(layer, h, turn):
        cols = channels_of(h)
        padf[...] = pad[layer, :, cols].astype(f32)
        block = 64
        for r in range(0, rows, block):
            total = jnp.zeros((block, half), f32)
            for k in range(n_taps):
                start = r + PAD - reach + k
                total = total + taps[k, layer:layer + 1, cols] * padf[start:start + block, :]
            mean = jnp.sum(total, axis=1, keepdims=True) / half
            shifted = total - mean
            convg[layer, t, r:r + block, cols] = shifted.astype(bf16)
            lane = lax.broadcasted_iota(jnp.int32, (block, 128), 1)
            before = column[r:r + block, :] if turn else jnp.zeros((block, 128), f32)
            squares = jnp.sum(shifted * shifted, axis=1, keepdims=True)
            column[r:r + block, :] = jnp.where(lane == 2 * h, mean, jnp.where(lane == 2 * h + 1, squares, before))

    def activate(layer):
        wait_bytes(stat.at[layer, pl.ds(0, T - 1)], s_sem.at[2 * layer + 1])
        got = [stat[layer, d] for d in range(T)]
        pairs = [(rows_[2 * h:2 * h + 1, :], rows_[2 * h + 1:2 * h + 2, :]) for rows_ in got for h in range(G)]
        center = sum((m for m, _ in pairs[1:]), pairs[0][0]) / (T * G)
        away = [m - center for m, _ in pairs]
        square = jnp.zeros((1, rows), f32)
        for a, (_, sq) in zip(away, pairs):
            square = square + (sq + half * (a * a))
        lines = away + [lax.rsqrt(square / C + 1e-05)]
        table = jnp.concatenate(lines + [jnp.zeros((128 - len(lines), rows), f32)], axis=0).T
        scale = table[:, T * G:T * G + 1]
        for d in range(T):
            j = lax.rem(t + T - d, T)
            by = cgain[j, layer:layer + 1, :]
            apart = jnp.concatenate(
                [jnp.broadcast_to(table[:, i:i + 1], (rows, half)) for i in range(G * d, G * (d + 1))], axis=1)
            normal = (convg[layer, j].astype(f32) + apart) * scale
            act[j] = jax.nn.silu(normal * by).astype(bf16)

    def add_branch(layer, h):
        part = None
        for j in range(T):
            term = jnp.dot(act[j], wo[layer, h, j * chans:(j + 1) * chans, :], preferred_element_type=f32)
            part = term if part is None else part + term
        cols = half_columns(h)
        x_state[:, cols] = (x_state[:, cols] + part).astype(bf16).astype(f32)

    with scope("stage_wait"):
        staged(first_vg)
    token_copy.wait()
    halo(0, "send")
    each(0, QC, lambda q: inward(first_vg, q, s).start())

    @pl.when(is_end)
    def _():
        each(0, x_chunks, lambda c: end_rows(c, inner).start())

    @pl.when(is_mid)
    def _():
        x_spread().begin()

    with scope("stage_wait2"):
        for stage in after:
            staged(stage)

    def end_sends(what, stage, lo, hi):
        @pl.when(is_end)
        def _():
            if what == "in":
                each(lo, hi, lambda q: inward(stage, q, edge).start())
            else:
                each(lo, hi, lambda q: direct(stage, q).start())

    end_sends("direct", first_vg, 0, shared_from)

    @pl.when(is_mid)
    def _():
        for stage in after:
            each(0, count[stage[1]], lambda q: outward(stage, q, mine).start())

    gain_copy.wait()
    for c in small:
        c.wait()
    for d in range(1, T):
        pltpu.make_async_remote_copy(
            src_ref=cgain.at[t], dst_ref=cgain.at[t], send_sem=g_sem.at[0], recv_sem=g_sem.at[1],
            device_id={"tp": lax.rem(t + d, T)}, device_id_type=MESH).start()
    x_state[...] = xg[0, t, own, :].astype(f32)
    with scope("halo0_begin"):
        halo(0, "begin")

    def first_chunks(q):
        from_inner(first_vg, q, near)
        from_edge(first_vg, q)
    with scope("A_vg0_near_edge"):
        each(0, QC, first_chunks)
    push_in(first_wo, 0, RC)
    push_in(second_vg, 0, QC // 2)

    @pl.when(is_end)
    def _():
        def pass_on(stage):
            def body(q):
                arrived(stage, q, mine)
                across(stage, q, mine).start()
            each(0, count[stage[1]], body)
        for stage in after:
            with scope("end_pass_on"):
                pass_on(stage)
            if stage == first_wo:
                end_sends("in", first_wo, 0, RC)
                end_sends("in", second_vg, 0, QC // 2)
            elif stage == second_vg:
                end_sends("direct", first_wo, 0, RC)

    def edge_relays(lo, hi):
        @pl.when(is_mid)
        def _():
            with scope("edge_relay"):
                each(lo, hi, lambda c: edge_spread(c).relay())

    halo(0, "relay")

    @pl.when(is_mid)
    def _():
        with scope("x0_finish"):
            x_spread().relay()
            x_spread().complete()
    halo(0, "complete")

    @pl.when(is_mid)
    def _():
        with scope("norm0"):
            normalize(0, 0, 0, 0, full)

    def second_chunks(q):
        each(q * QC // x_chunks, (q + 1) * QC // x_chunks, lambda k: from_inner(first_vg, k, far))

        @pl.when(is_mid)
        def _():
            wait_bytes(xg.at[0, t, pl.ds(0, x_rows)], f_sem.at[2 + q])
            edge_spread(q).begin()
    with scope("B_vg0_far"):
        each(0, x_chunks, second_chunks)

    @pl.when(is_mid)
    def _():
        with scope("proj0_g"):
            project(0, 0, 0, full, pad.at[0], g)
    edge_relays(0, x_chunks // 2)
    with scope("C1_wo0_near"):
        each(0, RC // 2, lambda q: from_inner(first_wo, q, near))
    edge_relays(x_chunks // 2, x_chunks - 1)
    with scope("C1_wo0_near"):
        each(RC // 2, RC, lambda q: from_inner(first_wo, q, near))
    edge_relays(x_chunks - 1, x_chunks)
    push_in(second_vg, QC // 2, 3 * QC // 4)
    end_sends("in", second_vg, QC // 2, QC)

    @pl.when(is_mid)
    def _():
        with scope("edge_complete"):
            each(0, x_chunks, lambda c: edge_spread(c).complete())
        with scope("norm_e"):
            normalize(0, L, 1, PAD, rows)
    with scope("D1_vg1_near"):
        each(0 * QC // 4, (0 + 1) * QC // 4, lambda q: from_inner(second_vg, q, near))

    @pl.when(is_mid)
    def _():
        with scope("proj0e_g"):
            project(0, 1, PAD, rows, glu_out, g)

    @pl.when(is_mid)
    def _():
        with scope("wait_vg0"):
            others_arrived(first_vg)
        with scope("proj0e"):
            project(0, 1, PAD, rows, glu_out, other)
    with scope("C2_wo0_edge"):
        each(0, RC // 2, lambda q: from_edge(first_wo, q))
    with scope("D1_vg1_near"):
        each(QC // 4, QC // 2, lambda q: from_inner(second_vg, q, near))

    @pl.when(is_mid)
    def _():
        with scope("proj0"):
            project(0, 0, 0, full, pad.at[0], other)

    sends_right, sends_left, _, _ = sides_of(0)

    @pl.when(sends_right)
    def _():
        glu_out[0:PAD, :] = jnp.zeros((PAD, chans), bf16)
        glu_out[PAD + rows:, :] = pad[0, PAD:2 * PAD, :]
        pad[0, 0:PAD, :] = glu_out[rows:rows + PAD, :]

    @pl.when(sends_left)
    def _():
        glu_out[0:PAD, :] = pad[0, rows:rows + PAD, :]
        glu_out[PAD + rows:, :] = jnp.zeros((PAD, chans), bf16)
        pad[0, PAD + rows:, :] = glu_out[PAD:2 * PAD, :]

    @pl.when(is_mid)
    def _():
        end_glu(edge).start()

    with scope("C2_wo0_edge"):
        each(RC // 2, RC, lambda q: from_edge(first_wo, q))
    push_in(second_vg, 3 * QC // 4, QC)
    end_sends("in", second_wo, 0, RC)

    @pl.when(is_end)
    def _():
        with scope("end_glu_wait"):
            wait_bytes(glu_out, f_sem.at[2 + x_chunks])

    with scope("conv0"):
        convolve(0, g, 0)
        convolve(0, other, 1)
    with scope("D2_vg1_edge"):
        each(0 * QC // 4, (0 + 1) * QC // 4, lambda q: from_edge(second_vg, q))
    with scope("C3_wo0_far"):
        each(0, RC // 2, lambda q: from_inner(first_wo, q, far))
    with scope("conv0_relay"):
        conv_spread(0, 0).relay()
    with scope("C3_wo0_far"):
        pl.when(is_end)(lambda: each(RC // 2, RC, lambda q: from_inner(first_wo, q, far)))
    with scope("conv0_relay"):
        conv_spread(0, 1).relay()
    with scope("C3_wo0_far"):
        pl.when(is_mid)(lambda: each(RC // 2, RC, lambda q: from_inner(first_wo, q, far)))
    with scope("conv0_complete"):
        conv_spread(0, 0).complete()
        conv_spread(0, 1).complete()
        wait_bytes(cgain.at[pl.ds(0, T - 1)], g_sem.at[1])
    with scope("act0"):
        activate(0)
    with scope("D2_vg1_edge"):
        each(1 * QC // 4, (1 + 1) * QC // 4, lambda q: from_edge(second_vg, q))
    push_in(second_wo, 0, RC // 2)

    def next_x(h, turn):
        add_branch(0, h)
        cols = half_columns(h)
        xg[1, t, own, cols] = x_state[:, cols].astype(bf16)
        half_spread(h, turn).begin()
    with scope("out0_g"):
        next_x(g, 0)
    with scope("D2_vg1_near"):
        each(QC // 2, 3 * QC // 4, lambda q: from_inner(second_vg, q, near))
    with scope("wait_wo0"):
        others_arrived(first_wo)
    with scope("out0"):
        next_x(other, 1)
    halo(1, "send")
    end_sends("direct", second_vg, 0, QC)
    end_sends("direct", second_wo, 0, RC)
    with scope("D3_vg1_near"):
        each(3 * QC // 4, QC, lambda q: from_inner(second_vg, q, near))
    with scope("D3_vg1_edge"):
        each(2 * QC // 4, (2 + 1) * QC // 4, lambda q: from_edge(second_vg, q))
    with scope("D4_vg1_far"):
        each(0 * QC // 4, (0 + 1) * QC // 4, lambda q: from_inner(second_vg, q, far))
    with scope("D3_vg1_edge"):
        each(3 * QC // 4, QC, lambda q: from_edge(second_vg, q))
    push_in(second_wo, RC // 2, RC)
    with scope("D4_vg1_far"):
        each(1 * QC // 4, (1 + 1) * QC // 4, lambda q: from_inner(second_vg, q, far))
    with scope("x1_relay"):
        half_spread(g, 0).relay()
    with scope("E1_near"):
        each(0, RC // 2, lambda q: from_inner(second_wo, q, near))
    with scope("halo1_begin"):
        pl.when(is_end)(lambda: halo(1, "begin"))
    with scope("D4_vg1_far"):
        each(2 * QC // 4, (2 + 1) * QC // 4, lambda q: from_inner(second_vg, q, far))
    with scope("x1_relay"):
        pl.when(is_end)(half_spread(other, 1).relay)
    with scope("halo1_relay"):
        pl.when(is_end)(lambda: halo(1, "relay"))
    with scope("E1_wo1_edge"):
        each(0, RC // 2, lambda q: from_edge(second_wo, q))
    with scope("D4_vg1_far"):
        pl.when(is_mid)(lambda: each(3 * QC // 4, QC, lambda q: from_inner(second_vg, q, far)))
    with scope("E1_wo1_edge"):
        each(RC // 2, RC, lambda q: from_edge(second_wo, q))
    with scope("halo1_begin"):
        pl.when(is_mid)(lambda: halo(1, "begin"))
    with scope("x1_relay"):
        pl.when(is_mid)(half_spread(other, 1).relay)
    with scope("E1_near"):
        pl.when(is_mid)(lambda: each(RC // 2, RC, lambda q: from_inner(second_wo, q, near)))
    with scope("halo1_relay"):
        pl.when(is_mid)(lambda: halo(1, "relay"))
    with scope("x1_complete"):
        half_spread(g, 0).complete()
        half_spread(other, 1).complete()
        halo(1, "complete")
    with scope("norm1"):
        normalize(1, 1, 0, 0, full)
    with scope("D4_vg1_far"):
        pl.when(is_end)(lambda: each(3 * QC // 4, QC, lambda q: from_inner(second_vg, q, far)))
    with scope("E2_m"):
        pl.when(is_mid)(lambda: each(0, RC // 2, lambda q: from_inner(second_wo, q, far)))
    with scope("proj1_g"):
        project(1, 0, 0, full, pad.at[1], g)
    with scope("conv1_g"):
        convolve(1, g, 0)
    with scope("E2_m"):
        pl.when(is_mid)(lambda: each(RC // 2, RC, lambda q: from_inner(second_wo, q, far)))
    with scope("E1_e"):
        pl.when(is_end)(lambda: each(RC // 2, 3 * RC // 4, lambda q: from_inner(second_wo, q, near)))
    with scope("wait_vg1"):
        others_arrived(second_vg)
    with scope("proj1"):
        project(1, 0, 0, full, pad.at[1], other, "early")
    with scope("E1_e"):
        pl.when(is_end)(lambda: each(3 * RC // 4, RC, lambda q: from_inner(second_wo, q, near)))
    def far_chunk(k):
        with scope("E2_e"):
            pl.when(is_end)(lambda: each(k * RC // 4, (k + 1) * RC // 4, lambda q: from_inner(second_wo, q, far)))
    far_chunk(0)
    with scope("wait_vg1_far"):
        far_arrived()
    far_chunk(1)
    with scope("proj1_far"):
        project(1, 0, 0, full, pad.at[1], other, "late")
    with scope("conv1"):
        convolve(1, other, 1)
    far_chunk(2)
    far_chunk(3)
    with scope("conv1_relay"):
        conv_spread(1, 0).relay()
    with scope("conv1_relay"):
        conv_spread(1, 1).relay()
    with scope("conv1_gather"):
        conv_spread(1, 0).complete()
        conv_spread(1, 1).complete()
    with scope("act1"):
        activate(1)

    def last_x(h, turn):
        add_branch(1, h)
        cols = half_columns(h)
        leaving[:, cols] = x_state[:, cols].astype(bf16)
        pltpu.make_async_copy(leaving.at[:, cols], x_out.at[:, cols], o_sem.at[turn]).start()
    with scope("out1_g"):
        last_x(g, 0)
    with scope("wait_wo1"):
        others_arrived(second_wo)
    with scope("out1"):
        last_x(other, 1)
    xf = x_state[...]
    share(L, jnp.broadcast_to(jnp.sum(xf * xf, axis=1, keepdims=True), (rows, 128)))

    halo(0, "drain")
    halo(1, "drain")
    for layer in range(L):
        for part_ in range(2):
            conv_spread(layer, part_).drain()
    half_spread(g, 0).drain()
    half_spread(other, 1).drain()
    wait_bytes(cgain.at[pl.ds(0, T - 1)], g_sem.at[0])
    whole = L * (depth + out_rows * out_half // (2 * half))
    later = whole - depth

    def sent(length, k):
        wait_bytes(wvg.at[0, 0, pl.ds(0, length)], send_w.at[k])

    def sent_twice(length, k):
        wait_bytes(wvg.at[0, :, pl.ds(0, length)], send_w.at[k])

    def sent_all(k):
        sent_twice(later * (n - 1) // G, k)

    @pl.when(is_mid)
    def _():
        x_spread().drain()
        each(0, x_chunks, lambda c: edge_spread(c).drain())
        wait_bytes(glu_out, f_sem.at[1])
        sent_twice(whole, IN)
        sent_twice(3 * later // 2, OUT)
        sent((QC - shared_from) * size["vg"], YE)
        sent_twice(whole, Y)

    @pl.when(is_end)
    def _():
        wait_bytes(xg.at[0, t, own], f_sem.at[0])
        sent(whole, IN)
        sent(later + shared_from * size["vg"], UN)
        sent_twice(3 * later // 2, Y)

    with scope("final_stat"):
        wait_bytes(stat.at[L, pl.ds(0, T - 1)], s_sem.at[2 * L + 1])
        for index_ in range(L + 1):
            wait_bytes(stat.at[index_, pl.ds(0, T - 1)], s_sem.at[2 * index_])
    line = sum((stat[L, d, 0:1, :] for d in range(1, T)), stat[L, 0, 0:1, :])
    total = jnp.broadcast_to(line, (128, rows)).T[:, 0:1]
    scale_out[...] = lax.rsqrt(total / D + 1e-06)
    for turn in range(G):
        wait_bytes(leaving.at[:, pl.ds(0, out_half)], o_sem.at[turn])


def scale_rows(x, scale, gain, out):
    out[...] = (x[...].astype(jnp.float32) * scale[...] * gain[...]).astype(out.dtype)


def quad_on_device(G, n, T, tokens, norm_gain, value_w, gate_w, taps, cgain, out_w, fgain):
    L = norm_gain.shape[0]
    if L != 2:
        return on_device(G, n, T, tokens, norm_gain, value_w, gate_w, taps, cgain, out_w, fgain)
    rows, width = tokens.shape
    depth, chans = value_w.shape[1:]
    D, C = width * T, chans * T
    bf16, f32 = jnp.bfloat16, jnp.float32
    dma = pltpu.SemaphoreType.DMA
    vmem = pl.BlockSpec(memory_space=pltpu.VMEM)
    hbm = pl.BlockSpec(memory_space=pltpu.HBM)
    full = rows + 2 * PAD
    x, scale = pl.pallas_call(
        functools.partial(quad_kernel, G, n, T, L),
        out_shape=(jax.ShapeDtypeStruct((rows, width), bf16), jax.ShapeDtypeStruct((rows, 1), f32)),
        in_specs=[hbm] * 7,
        out_specs=(pl.BlockSpec(memory_space=pl.ANY), vmem),
        scratch_shapes=[
            pltpu.VMEM((L, G, D, 2 * chans // G), bf16),
            pltpu.VMEM((L, G, C, width // G), bf16),
            pltpu.VMEM((L + 1, T, full, width), bf16),
            pltpu.VMEM((2, T, full, width), bf16),
            pltpu.VMEM((full, chans), bf16),
            pltpu.VMEM((full, 2 * chans // G), f32),
            pltpu.VMEM((L, full, chans), bf16),
            pltpu.VMEM((full, chans // G), f32),
            pltpu.VMEM((L, T, rows, chans), bf16),
            pltpu.VMEM((T, rows, chans), bf16),
            pltpu.VMEM((rows, 128), f32),
            pltpu.VMEM((L + 1, T, 8, rows), f32),
            pltpu.VMEM((rows, width), f32),
            pltpu.VMEM((rows, width), bf16),
            pltpu.VMEM(norm_gain.shape, f32),
            pltpu.VMEM((taps.shape[1], L, chans), f32),
            pltpu.VMEM((T,) + cgain.shape, f32),
            dma((2 * L + 4,)),
            dma((L * (QC + RC), 3)), dma((2 * L + 1,)), dma((5,)),
            dma((1 + G, 3)), dma((XC, 3)), dma((L, 2, 3)), dma((2 * (L + 1),)),
            dma((L, 4)), dma((L, 2, 3)), dma((2,)), dma((XC + 3,)), dma((G,)),
        ],
        compiler_params=pltpu.CompilerParams(
            collective_id=0, has_side_effects=True, vmem_limit_bytes=56 * 2**20
        ),
    )(tokens, norm_gain, value_w, gate_w, taps.transpose(1, 0, 2), cgain, out_w)
    step = rows // EPILOGUE
    return pl.pallas_call(
        scale_rows,
        grid=(EPILOGUE,),
        out_shape=jax.ShapeDtypeStruct((rows, width), bf16),
        in_specs=[
            pl.BlockSpec((step, width), lambda i: (i, 0)),
            pl.BlockSpec((step, 1), lambda i: (i, 0)),
            pl.BlockSpec((1, width), lambda i: (0, 0)),
        ],
        out_specs=pl.BlockSpec((step, width), lambda i: (i, 0)),
        compiler_params=pltpu.CompilerParams(vmem_limit_bytes=60 * 2**20),
    )(x, scale, fgain.reshape(1, width))


def tokens_f32(tokens, xg, t):
    return xg[0, t].astype(jnp.float32)


def on_device(G, n, T, tokens, norm_gain, value_w, gate_w, taps, cgain, out_w, fgain):
    L = norm_gain.shape[0]
    rows, width = tokens.shape
    depth, chans = value_w.shape[1:]
    D, C = width * T, chans * T
    bf16, f32 = jnp.bfloat16, jnp.float32
    dma = pltpu.SemaphoreType.DMA
    vmem = pl.BlockSpec(memory_space=pltpu.VMEM)
    hbm = pl.BlockSpec(memory_space=pl.ANY)
    P_ = L * (Q + 1)
    peers = max(G - 1, 1)
    return pl.pallas_call(
        functools.partial(kernel, G, n, T, L),
        out_shape=jax.ShapeDtypeStruct((rows, width), bf16),
        in_specs=[hbm, vmem, hbm, hbm, vmem, vmem, hbm, vmem],
        out_specs=vmem,
        scratch_shapes=[
            pltpu.VMEM((L, G, D, 2 * chans // G), bf16),
            pltpu.VMEM((L, G, C, width // G), bf16),
            pltpu.VMEM((L + 1, T, rows, width), bf16),
            pltpu.VMEM((2, T, rows, width), bf16),
            pltpu.VMEM((rows, chans), bf16),
            pltpu.VMEM((rows, 2 * chans // G), f32),
            pltpu.VMEM((L, rows + 2 * PAD, chans), bf16),
            pltpu.VMEM((rows + 2 * PAD, chans), f32),
            pltpu.VMEM((rows, chans), f32),
            pltpu.VMEM((L + 1, T, 8, rows), f32),
            pltpu.VMEM((L, T, rows, chans), bf16),
            pltpu.VMEM((rows, width), f32),
            dma((1 + L * G * 3,)),
            dma((P_, n)), dma((P_, n)), dma((P_, n)),
            dma((P_, n, peers)), dma((P_, n, peers)),
            dma((L + 1, T)), dma((L + 1, T)), dma((L, T)), dma((L, T)),
            dma((L + 1, T)), dma((L + 1, T)),
            dma((L, 2)), dma((L, 2)),
            dma((G + 1,)), dma((G + 1,)),
        ],
        compiler_params=pltpu.CompilerParams(
            collective_id=0, has_side_effects=True, vmem_limit_bytes=56 * 2**20
        ),
    )(tokens, norm_gain.reshape(L * T, width), value_w, gate_w, taps, cgain, out_w, fgain.reshape(1, width))


def solution(mesh):
    placed = (
        P(("grp", "sp"), "tp"),
        P(),
        P(None, "sp", "tp"),
        P(None, "sp", "tp"),
        P(None, None, "tp"),
        P(None, "tp"),
        P(None, "sp", "tp"),
        P("tp"),
    )
    G, n, T = (mesh.shape[a] for a in ("grp", "sp", "tp"))
    paired = G == 2 and n == T == 2 * G
    return jax.shard_map(
        functools.partial(quad_on_device if paired else on_device, G, n, T),
        mesh=mesh, in_specs=placed, out_specs=P(("grp", "sp"), "tp"), check_vma=False,
    )
```

```python
import functools

import jax
import jax.numpy as jnp
from jax import lax
from jax.experimental import pallas as pl
from jax.experimental.pallas import tpu as pltpu
from jax.sharding import PartitionSpec as P

MESH = pl.DeviceIdType.MESH
Q = 2
PAD = 16


def kernel(
    G, n, T, L,
    tokens, gain, value_w, gate_w, taps, cgain, out_w, fgain,
    result,
    wvg, wo, xg, xn, glu_out, acc, pad, padf, conv, stat, actg, x_state,
    local_sem, z_recv, right_send, left_send, y_send, y_recv,
    x_send, x_recv, a_send, a_recv, s_send, s_recv, h_send, h_recv, f_send, f_recv,
):
    g, s, t = lax.axis_index("grp"), lax.axis_index("sp"), lax.axis_index("tp")
    rows, width = tokens.shape
    depth, chans = value_w.shape[1:]
    out_rows = out_w.shape[1]
    half = chans // G
    out_half = width // G
    reach = taps.shape[1] // 2
    n_taps = taps.shape[1]
    D = width * T
    C = chans * T
    chunk = depth // Q
    pieces = Q + 1
    f32, bf16 = jnp.float32, jnp.bfloat16
    helped = n >= 4
    last = n - 1
    is_end = (s == 0) | (s == last)
    helper = (s == 1) | (s == last - 1)
    end = jnp.where(s == 1, 0, last)
    inward = jnp.where(s == 0, 1, last - 1)

    def ends_out(p):
        return helped and p < Q

    def to_right_ok(p):
        return s < last - 1 if ends_out(p) else s < last

    def to_left_ok(p):
        return s > 1 if ends_out(p) else s > 0

    def takes(p):
        return jnp.logical_not(is_end) if ends_out(p) else s >= 0

    def by_grp(p, j):
        ok = takes(p) & (j != s)
        if helped and p == 0:
            ok = ok & jnp.logical_not((s == 1) & (j == 0)) & jnp.logical_not((s == last - 1) & (j == last))
        return ok

    def piece(p, h, j):
        layer, q = p // pieces, p % pieces
        if q < Q:
            start = pl.multiple_of(j * depth + q * chunk, chunk)
            return wvg.at[layer, h, pl.ds(start, chunk), :]
        return wo.at[layer, h, pl.ds(pl.multiple_of(j * out_rows, out_rows), out_rows), :]

    locals_ = [pltpu.make_async_copy(tokens, xg.at[0, t], local_sem.at[0])]
    own_rows = pl.ds(pl.multiple_of(s * depth, depth), depth)
    own_out = pl.ds(pl.multiple_of(s * out_rows, out_rows), out_rows)
    count = 1
    per_layer = []
    for layer in range(L):
        group = []
        for h in range(G):
            for k, w in enumerate((value_w, gate_w)):
                group.append(pltpu.make_async_copy(
                    w.at[layer, :, pl.ds(h * half, half)],
                    wvg.at[layer, h, own_rows, pl.ds(k * half, half)],
                    local_sem.at[count]))
                count += 1
            group.append(pltpu.make_async_copy(
                out_w.at[layer, :, pl.ds(h * out_half, out_half)],
                wo.at[layer, h, own_out, :], local_sem.at[count]))
            count += 1
        per_layer.append(group)
    for c in locals_ + sum(per_layer, []):
        c.start()

    barrier = pltpu.get_barrier_semaphore()
    for d in range(1, T):
        pl.semaphore_signal(barrier, inc=1, device_id={"tp": lax.rem(t + d, T)}, device_id_type=MESH)
    for d in range(1, G):
        pl.semaphore_signal(barrier, inc=1, device_id={"grp": lax.rem(g + d, G)}, device_id_type=MESH)

    @pl.when(s > 0)
    def _():
        pl.semaphore_signal(barrier, inc=1, device_id={"sp": s - 1}, device_id_type=MESH)

    @pl.when(s < n - 1)
    def _():
        pl.semaphore_signal(barrier, inc=1, device_id={"sp": s + 1}, device_id_type=MESH)

    sides = jnp.where(s > 0, 1, 0) + jnp.where(s < n - 1, 1, 0)
    pl.semaphore_wait(barrier, (T - 1) + (G - 1) + sides)

    def right(p, j):
        r = piece(p, g, j)
        return pltpu.make_async_remote_copy(
            src_ref=r, dst_ref=r, send_sem=right_send.at[p, j], recv_sem=z_recv.at[p, j],
            device_id={"sp": s + 1}, device_id_type=MESH)

    def left(p, j):
        r = piece(p, g, j)
        return pltpu.make_async_remote_copy(
            src_ref=r, dst_ref=r, send_sem=left_send.at[p, j], recv_sem=z_recv.at[p, j],
            device_id={"sp": s - 1}, device_id_type=MESH)

    def across(p, j, d, h):
        r = piece(p, h, j)
        return pltpu.make_async_remote_copy(
            src_ref=r, dst_ref=r, send_sem=y_send.at[p, j, d - 1], recv_sem=y_recv.at[p, j, d - 1],
            device_id={"grp": lax.rem(g + d, G)}, device_id_type=MESH)

    batches = []
    for layer in range(L):
        base = layer * pieces
        batches += [list(range(base, base + Q)), [base + Q]]

    def own_right(ps):
        for p in ps:
            right(p, s).start()

    def own_left(ps):
        for p in ps:
            left(p, s).start()

    def end_rows(target):
        return pltpu.make_async_remote_copy(
            src_ref=xg.at[0, t], dst_ref=xg.at[L, t], send_sem=f_send.at[0], recv_sem=f_recv.at[0],
            device_id={"sp": target}, device_id_type=MESH)

    def end_piece(d, h, j, target):
        r = piece(0, h, j)
        return pltpu.make_async_remote_copy(
            src_ref=r, dst_ref=r, send_sem=f_send.at[d], recv_sem=f_recv.at[d],
            device_id={"sp": target}, device_id_type=MESH)

    def end_glu(target):
        return pltpu.make_async_remote_copy(
            src_ref=glu_out, dst_ref=pad.at[0, pl.ds(PAD, rows), :],
            send_sem=f_send.at[G], recv_sem=f_recv.at[G],
            device_id={"sp": target}, device_id_type=MESH)

    def relay(b, low, high):
        low, high = min(low, n - 1), min(high, n - 1)
        following = batches[b + 1] if b + 1 < len(batches) else []

        def step(k, carry):
            for p in batches[b]:
                from_left, from_right = s - 1 - k, s + 1 + k

                @pl.when((from_left >= 0) & takes(p))
                def _():
                    j = jnp.maximum(from_left, 0)
                    right(p, j).wait_recv()

                    @pl.when(to_right_ok(p))
                    def _():
                        right(p, j).start()

                    @pl.when(by_grp(p, j))
                    def _():
                        for d in range(1, G):
                            across(p, j, d, g).start()

                @pl.when((from_right < n) & takes(p))
                def _():
                    j = jnp.minimum(from_right, n - 1)
                    left(p, j).wait_recv()

                    @pl.when(to_left_ok(p))
                    def _():
                        left(p, j).start()

                    @pl.when(by_grp(p, j))
                    def _():
                        for d in range(1, G):
                            across(p, j, d, g).start()

            @pl.when((k == s - 1) & (s < (last - 1 if helped and b < 2 else last)))
            def _():
                own_right(following)

            @pl.when((k == n - 2 - s) & (s > (1 if helped and b < 2 else 0)))
            def _():
                own_left(following)

            return carry

        if high > low:
            lax.fori_loop(low, high, step, 0)

    def wait_across(b):
        for p in batches[b]:
            def step(j, carry):
                @pl.when(by_grp(p, j))
                def _():
                    for d in range(1, G):
                        across(p, j, d, lax.rem(g + G - d, G)).wait_recv()
                return carry
            lax.fori_loop(0, n, step, 0)

    def spread(buf, layer, send, recv):
        def copy(bit, m):
            block = buf.at[layer, t ^ m]
            return pltpu.make_async_remote_copy(
                src_ref=block, dst_ref=block, send_sem=send.at[layer, bit + m], recv_sem=recv.at[layer, bit + m],
                device_id={"tp": t ^ bit}, device_id_type=MESH)

        def arrival(bit, m):
            block = buf.at[layer, t ^ bit ^ m]
            return pltpu.make_async_remote_copy(
                src_ref=block, dst_ref=block, send_sem=send.at[layer, bit + m], recv_sem=recv.at[layer, bit + m],
                device_id={"tp": t ^ bit}, device_id_type=MESH)

        bits = []
        bit = T // 2
        while bit >= 1:
            bits.append(bit)
            bit //= 2

        def begin():
            for bit in bits:
                copy(bit, 0).start()

        def finish():
            have, sent = [0], []
            for i, bit in enumerate(bits):
                for m in have:
                    arrival(bit, m).wait_recv()
                    sent.append((bit, m))
                    for lower in bits[i + 1:]:
                        copy(lower, m ^ bit).start()
                have = have + [m ^ bit for m in have]
            return lambda: [copy(bit, m).wait_send() for bit, m in sent]

        return begin, finish

    def exchange(index, columns):
        lane = lax.broadcasted_iota(jnp.int32, (rows, 128), 1)
        tile = jnp.zeros((rows, 128), f32)
        for i, column in enumerate(columns):
            tile = jnp.where(lane == i, column, tile)
        stat[index, 0] = tile.T[:8, :]

        def copy(d):
            return pltpu.make_async_remote_copy(
                src_ref=stat.at[index, 0], dst_ref=stat.at[index, d],
                send_sem=s_send.at[index, d - 1], recv_sem=s_recv.at[index, d - 1],
                device_id={"tp": lax.rem(t + d, T)}, device_id_type=MESH)

        for d in range(1, T):
            copy(d).start()

        def total():
            for d in range(1, T):
                copy(d).wait_recv()
            sums = stat[index, 0]
            for d in range(1, T):
                sums = sums + stat[index, d]
            wide = jnp.concatenate([sums, jnp.zeros((120, rows), f32)], axis=0).T
            for d in range(1, T):
                copy(d).wait_send()
            return [wide[:, i:i + 1] for i in range(len(columns))]

        return total

    def normalize(layer, held, into):
        def squares(j, total):
            part = xg[held, j].astype(f32)
            return total + jnp.sum(part * part, axis=1, keepdims=True)
        mean = lax.fori_loop(0, T, squares, jnp.zeros((rows, 1), f32)) / D
        scale = lax.rsqrt(mean + 1e-06)

        def body(j, carry):
            xn[into, j] = (xg[held, j].astype(f32) * scale * gain[layer * T + j][None, :]).astype(bf16)
            return carry
        lax.fori_loop(0, T, body, 0)

    def project(layer, held, put):
        for h in range(G):
            def body(j, carry):
                block = wvg[layer, h, pl.ds(pl.multiple_of(j * width, width), width), :]
                part = jnp.dot(xn[held, j], block, preferred_element_type=f32)

                @pl.when(j == 0)
                def _():
                    acc[...] = part

                @pl.when(j > 0)
                def _():
                    acc[...] += part
                return carry
            lax.fori_loop(0, T, body, 0)
            glu = acc[:, :half] * jax.nn.sigmoid(acc[:, half:])
            put(h, glu.astype(bf16))

    for c in locals_:
        c.wait()
    spreads = [spread(xg, layer, x_send, x_recv) for layer in range(L)]
    spreads[0][0]()
    for c in sum(per_layer, []):
        c.wait()

    @pl.when(to_right_ok(0))
    def _():
        own_right(batches[0])

    @pl.when(to_left_ok(0))
    def _():
        own_left(batches[0])

    if helped:
        @pl.when(is_end)
        def _():
            end_rows(inward).start()
            for d in range(1, G):
                end_piece(d, lax.rem(g + d, G), s, inward).start()

        @pl.when(s == last - 1)
        def _():
            own_right(batches[1])
            if L > 1:
                own_right(batches[2])

        @pl.when(s == 1)
        def _():
            own_left(batches[1])
            if L > 1:
                own_left(batches[2])

    @pl.when((s == 0) & (s < n - 1))
    def _():
        for b in batches[1:]:
            own_right(b)

    @pl.when((s == n - 1) & (s > 0))
    def _():
        for b in batches[1:]:
            own_left(b)

    x_state[...] = tokens_f32(tokens, xg, t)
    drains = []

    for layer in range(L):
        first, second = 2 * layer, 2 * layer + 1
        if layer == 0:
            relay(first, 0, 1)
        else:
            relay(first, 1, 2)
        drains.append(spreads[layer][1]())
        if helped and layer == 0:
            @pl.when(jnp.logical_not(is_end))
            def _():
                normalize(layer, layer, 0)
        else:
            normalize(layer, layer, 0)
        relay(first, 1 if layer == 0 else 2, n)
        begin, finish = spread(xg, L, x_send, x_recv)
        if helped and layer == 0:
            @pl.when(helper)
            def _():
                end_rows(end).wait_recv()
                begin()

        relay(second, 0, 1)

        def put(h, value):
            pad[layer, PAD:PAD + rows, h * half:(h + 1) * half] = value

        def put_out(h, value):
            glu_out[:, h * half:(h + 1) * half] = value

        if helped and layer == 0:
            @pl.when(helper)
            def _():
                drain = finish()
                normalize(0, L, 1)
                for d in range(1, G):
                    end_piece(d, lax.rem(g + d, G), end, end).wait_recv()
                drain()

            wait_across(first)

            @pl.when(helper)
            def _():
                project(0, 1, put_out)
                end_glu(end).start()

            @pl.when(jnp.logical_not(is_end))
            def _():
                project(0, 0, put)

            @pl.when(helper)
            def _():
                end_glu(end).wait_send()

            @pl.when(is_end)
            def _():
                end_rows(inward).wait_send()
                for d in range(1, G):
                    end_piece(d, lax.rem(g + d, G), s, inward).wait_send()
                end_glu(inward).wait_recv()
        else:
            wait_across(first)
            project(layer, 0, put)

        def to_right():
            return pltpu.make_async_remote_copy(
                src_ref=pad.at[layer, pl.ds(rows, PAD), :], dst_ref=pad.at[layer, pl.ds(0, PAD), :],
                send_sem=h_send.at[layer, 0], recv_sem=h_recv.at[layer, 0],
                device_id={"sp": s + 1}, device_id_type=MESH)

        def to_left():
            return pltpu.make_async_remote_copy(
                src_ref=pad.at[layer, pl.ds(PAD, PAD), :], dst_ref=pad.at[layer, pl.ds(PAD + rows, PAD), :],
                send_sem=h_send.at[layer, 1], recv_sem=h_recv.at[layer, 1],
                device_id={"sp": s - 1}, device_id_type=MESH)

        @pl.when(s < n - 1)
        def _():
            to_right().start()

        @pl.when(s > 0)
        def _():
            to_left().start()

        @pl.when(s == 0)
        def _():
            pad[layer, 0:PAD, :] = jnp.zeros((PAD, chans), bf16)

        @pl.when(s == n - 1)
        def _():
            pad[layer, PAD + rows:, :] = jnp.zeros((PAD, chans), bf16)

        relay(second, 1, 2)

        @pl.when(s > 0)
        def _():
            to_right().wait_recv()

        @pl.when(s < n - 1)
        def _():
            to_left().wait_recv()

        padf[...] = pad[layer].astype(f32)
        block = 64
        sums, squares = [], []
        for r in range(0, rows, block):
            total = jnp.zeros((block, chans), f32)
            for k in range(n_taps):
                start = r + PAD - reach + k
                total = total + taps[layer, k][None, :] * padf[start:start + block, :]
            conv[r:r + block, :] = total
            sums.append(jnp.sum(total, axis=1, keepdims=True))
            squares.append(jnp.sum(total * total, axis=1, keepdims=True))
        totals = exchange(layer, [jnp.concatenate(sums, 0), jnp.concatenate(squares, 0)])
        relay(second, 2, n)
        if layer + 1 < L:
            relay(second + 1, 0, 1)
        total, square = totals()
        center = total / C
        spread_ = square / C - center * center
        normal = (conv[...] - center) * lax.rsqrt(spread_ + 1e-05)
        actg[layer, t] = jax.nn.silu(normal * cgain[layer][None, :]).astype(bf16)
        act_begin, act_finish = spread(actg, layer, a_send, a_recv)
        act_begin()
        drains.append(act_finish())
        wait_across(second)
        for h in range(G):
            part = None
            for j in range(T):
                term = jnp.dot(actg[layer, j], wo[layer, h, j * chans:(j + 1) * chans, :], preferred_element_type=f32)
                part = term if part is None else part + term
            cols = slice(h * out_half, (h + 1) * out_half)
            x_state[:, cols] = (x_state[:, cols] + part).astype(bf16).astype(f32)
        if layer + 1 < L:
            xg[layer + 1, t] = x_state[...].astype(bf16)
            spreads[layer + 1][0]()

        @pl.when(s < n - 1)
        def _():
            to_right().wait_send()

        @pl.when(s > 0)
        def _():
            to_left().wait_send()

    xf = x_state[...]
    totals = exchange(L, [jnp.sum(xf * xf, axis=1, keepdims=True)])

    for drain in drains:
        drain()

    def drain_step(j, carry):
        for p in range(L * pieces):
            came = (j == s) | takes(p)

            @pl.when((j <= s) & to_right_ok(p) & came)
            def _():
                right(p, j).wait_send()

            @pl.when((j >= s) & to_left_ok(p) & came)
            def _():
                left(p, j).wait_send()

            @pl.when(by_grp(p, j))
            def _():
                for d in range(1, G):
                    across(p, j, d, g).wait_send()
        return carry
    lax.fori_loop(0, n, drain_step, 0)

    (total,) = totals()
    scale = lax.rsqrt(total / D + 1e-06)
    result[...] = (x_state[...] * scale * fgain[...]).astype(bf16)


QC = 8
RC = 4
XC = 4
EPILOGUE = 2


def quad_kernel(
    G, n, T, L,
    tokens, gain_hbm, value_w, gate_w, taps_hbm, cgain_hbm, out_w,
    x_out, scale_out,
    wvg, wo, xg, xn, glu_out, acc, pad, padf, convg, act, column, stat, x_state, leaving, gain, taps, cgain,
    local_sem, recv_z, recv_o, send_w, x_sem, e_sem, c_sem, s_sem, h_sem, hs_sem, g_sem, f_sem, o_sem,
):
    g, s, t = lax.axis_index("grp"), lax.axis_index("sp"), lax.axis_index("tp")
    rows, width = tokens.shape
    depth, chans = value_w.shape[1:]
    out_rows = out_w.shape[1]
    half = chans // G
    out_half = width // G
    n_taps = taps.shape[0]
    reach = n_taps // 2
    D = width * T
    C = chans * T
    full = rows + 2 * PAD
    pieces = QC + RC
    size = {"vg": depth // QC, "wo": out_rows // RC}
    count = {"vg": QC, "wo": RC}
    shared_from = 3 * QC // 4
    f32, bf16 = jnp.float32, jnp.bfloat16
    last = n - 1
    low = s < n // 2
    is_end = (s == 0) | (s == last)
    is_mid = jnp.logical_not(is_end)
    inner = jnp.where(low, s + 1, s - 1)
    outer = jnp.where(low, s - 1, s + 1)
    edge, mine, near, far = (jnp.where(low, a, last - a) for a in (0, 1, n - 2, n - 1))
    other = lax.rem(g + 1, G)
    x_chunks = XC
    x_rows = rows // x_chunks
    own = pl.ds(PAD, rows)
    first_vg, first_wo, second_vg, second_wo = (0, "vg"), (0, "wo"), (1, "vg"), (1, "wo")
    after = (first_wo, second_vg, second_wo)
    scope = jax.named_scope
    IN, OUT, Y, YE, UN = range(5)

    def index(stage, q):
        layer, kind = stage
        return layer * pieces + (0 if kind == "vg" else QC) + q

    def order_of(stage):
        return stage[0] * 2 + (0 if stage[1] == "vg" else 1)

    def place(j):
        return jnp.where(j == near, 1, jnp.where(j == far, 2, 0))

    def piece(stage, q, h, j):
        layer, kind = stage
        step = size[kind]
        per = depth if kind == "vg" else out_rows
        ref = wvg if kind == "vg" else wo
        return ref.at[layer, h, pl.ds(pl.multiple_of(j * per + q * step, step), step), :]

    def wait_bytes(ref, sem):
        pltpu.make_async_copy(ref, ref, sem).wait()

    own_rows = pl.ds(pl.multiple_of(s * depth, depth), depth)
    own_out = pl.ds(pl.multiple_of(s * out_rows, out_rows), out_rows)

    def stage_in(stage):
        layer, kind = stage
        sem = local_sem.at[order_of(stage)]
        for h in range(G):
            if kind == "vg":
                for k, w in enumerate((value_w, gate_w)):
                    pltpu.make_async_copy(
                        w.at[layer, :, pl.ds(h * half, half)],
                        wvg.at[layer, h, own_rows, pl.ds(k * half, half)], sem).start()
            else:
                pltpu.make_async_copy(
                    out_w.at[layer, :, pl.ds(h * out_half, out_half)],
                    wo.at[layer, h, own_out, :], sem).start()

    def staged(stage):
        layer, kind = stage
        ref = wvg.at[layer, :, own_rows] if kind == "vg" else wo.at[layer, :, own_out]
        wait_bytes(ref, local_sem.at[order_of(stage)])

    token_copy = pltpu.make_async_copy(tokens, xg.at[0, t, own], local_sem.at[2 * L])
    gain_copy = pltpu.make_async_copy(cgain_hbm, cgain.at[t], local_sem.at[2 * L + 1])
    small = [
        pltpu.make_async_copy(gain_hbm, gain, local_sem.at[2 * L + 2]),
        pltpu.make_async_copy(taps_hbm, taps, local_sem.at[2 * L + 3]),
    ]
    stage_in(first_vg)
    token_copy.start()
    gain_copy.start()
    for stage in after:
        stage_in(stage)
    for c in small:
        c.start()

    barrier = pltpu.get_barrier_semaphore()
    for d in range(1, T):
        pl.semaphore_signal(barrier, inc=1, device_id={"tp": lax.rem(t + d, T)}, device_id_type=MESH)
    pl.semaphore_signal(barrier, inc=1, device_id={"grp": other}, device_id_type=MESH)

    @pl.when(s > 0)
    def _():
        pl.semaphore_signal(barrier, inc=1, device_id={"sp": s - 1}, device_id_type=MESH)

    @pl.when(s < last)
    def _():
        pl.semaphore_signal(barrier, inc=1, device_id={"sp": s + 1}, device_id_type=MESH)

    blank = jnp.zeros((T, PAD, width), bf16)

    @pl.when(s < n // 2)
    def _():
        xg[0, :, 0:PAD, :] = blank

    @pl.when(s >= n // 2)
    def _():
        xg[0, :, PAD + rows:, :] = blank

    @pl.when(s == 0)
    def _():
        xg[1, :, 0:PAD, :] = blank

    @pl.when(s == last)
    def _():
        xg[1, :, PAD + rows:, :] = blank

    sides = jnp.where(s > 0, 1, 0) + jnp.where(s < last, 1, 0)
    pl.semaphore_wait(barrier, (T - 1) + (G - 1) + sides)

    def arrived(stage, q, j):
        wait_bytes(piece(stage, q, g, j), recv_z.at[index(stage, q), place(j)])

    def inward(stage, q, j):
        r, p = piece(stage, q, g, j), index(stage, q)
        there = jnp.where(is_end, 0, jnp.where(j == mine, 1, 2))
        return pltpu.make_async_remote_copy(
            src_ref=r, dst_ref=r, send_sem=send_w.at[IN], recv_sem=recv_z.at[p, there],
            device_id={"sp": inner}, device_id_type=MESH)

    def outward(stage, q, j):
        r, p = piece(stage, q, g, j), index(stage, q)
        return pltpu.make_async_remote_copy(
            src_ref=r, dst_ref=r, send_sem=send_w.at[OUT], recv_sem=recv_z.at[p, place(j)],
            device_id={"sp": outer}, device_id_type=MESH)

    def across(stage, q, j, send=Y):
        r = piece(stage, q, g, j)
        return pltpu.make_async_remote_copy(
            src_ref=r, dst_ref=r, send_sem=send_w.at[send],
            recv_sem=recv_o.at[2 * L if stage == second_vg and j is far else order_of(stage)],
            device_id={"grp": other}, device_id_type=MESH)

    def direct(stage, q):
        r = piece(stage, q, other, edge)
        return pltpu.make_async_remote_copy(
            src_ref=r, dst_ref=r, send_sem=send_w.at[UN], recv_sem=recv_o.at[order_of(stage)],
            device_id={"sp": inner}, device_id_type=MESH)

    def others_arrived(stage):
        layer, kind = stage
        per = depth if kind == "vg" else out_rows
        ref = wvg if kind == "vg" else wo
        blocks = n - 2 if stage == second_vg else n - 1
        wait_bytes(ref.at[layer, 0, pl.ds(0, blocks * per)], recv_o.at[order_of(stage)])

    def far_arrived():
        wait_bytes(wvg.at[1, 0, pl.ds(0, depth)], recv_o.at[2 * L])

    def end_rows(c, target):
        src = pl.ds(pl.multiple_of(PAD + c * x_rows, PAD), x_rows)
        return pltpu.make_async_remote_copy(
            src_ref=xg.at[0, t, src], dst_ref=xg.at[L, t, src], send_sem=f_sem.at[0], recv_sem=f_sem.at[2 + c],
            device_id={"sp": target}, device_id_type=MESH)

    def end_glu(target):
        return pltpu.make_async_remote_copy(
            src_ref=glu_out, dst_ref=pad.at[0], send_sem=f_sem.at[1], recv_sem=f_sem.at[2 + x_chunks],
            device_id={"sp": target}, device_id_type=MESH)

    def each(low_, high_, body):
        def step(q, carry):
            body(q)
            return carry
        lax.fori_loop(low_, high_, step, 0)

    def from_inner(stage, q, j, over_y=True):
        def serve():
            with scope("w_inner"):
                arrived(stage, q, j)
            if stage != first_vg:
                @pl.when(is_mid)
                def _():
                    outward(stage, q, j).start()
            if over_y:
                across(stage, q, j).start()
        if stage == first_vg:
            pl.when(is_mid)(serve)
        else:
            serve()

    def from_edge(stage, q):
        @pl.when(is_mid)
        def _():
            with scope("w_edge"):
                arrived(stage, q, edge)
            inward(stage, q, edge).start()
            if stage == first_vg:
                @pl.when(q >= shared_from)
                def _():
                    across(stage, q, edge, YE).start()

    def push_in(stage, lo, hi):
        @pl.when(is_mid)
        def _():
            each(lo, hi, lambda q: inward(stage, q, mine).start())

    class Spread:
        def __init__(self, view, three, two, sems):
            self.view, self.three, self.two, self.sems = view, three, two, sems

        def copy(self, j, bit, k):
            block = self.view(j)
            return pltpu.make_async_remote_copy(
                src_ref=block, dst_ref=block, send_sem=self.sems(2), recv_sem=self.sems(k),
                device_id={"tp": t ^ bit}, device_id_type=MESH)

        def begin(self):
            self.copy(t, T // 2, 0).start()
            self.copy(t, 1, 1).start()

        def relay(self):
            wait_bytes(self.view(t), self.sems(0))
            self.copy(t ^ (T // 2), 1, 1).start()

        def complete(self):
            wait_bytes(self.two, self.sems(1))

        def drain(self):
            wait_bytes(self.three, self.sems(2))

    def half_columns(h):
        return pl.ds(pl.multiple_of(h * out_half, out_half), out_half)

    def x_spread():
        return Spread(lambda j: xg.at[0, j, own], xg.at[0, pl.ds(0, 3), own], xg.at[0, pl.ds(0, 2), own],
                      lambda k: x_sem.at[0, k])

    def half_spread(h, turn):
        cols = half_columns(h)
        return Spread(lambda j: xg.at[1, j, own, cols], xg.at[1, pl.ds(0, 3), own, cols],
                      xg.at[1, pl.ds(0, 2), own, cols], lambda k: x_sem.at[1 + turn, k])

    def edge_spread(c):
        part = pl.ds(pl.multiple_of(PAD + c * x_rows, PAD), x_rows)
        return Spread(lambda j: xg.at[L, j, part], xg.at[L, pl.ds(0, 3), part], xg.at[L, pl.ds(0, 2), part],
                      lambda k: e_sem.at[c, k])

    def halo_spread(layer, side):
        part = pl.ds(0 if side == 0 else PAD + rows, PAD)
        return Spread(lambda j: xg.at[layer, j, part], xg.at[layer, pl.ds(0, 3), part], xg.at[layer, pl.ds(0, 2), part],
                      lambda k: hs_sem.at[layer, side, k])

    def conv_spread(layer, part_):
        cols = channels_of(g if part_ == 0 else other)
        return Spread(lambda j: convg.at[layer, j, :, cols], convg.at[layer, pl.ds(0, 3), :, cols],
                      convg.at[layer, pl.ds(0, 2), :, cols], lambda k: c_sem.at[layer, part_, k])

    def to_peers(buf, sem, k):
        for d in range(1, T):
            pltpu.make_async_remote_copy(
                src_ref=buf.at[0], dst_ref=buf.at[d], send_sem=sem.at[k], recv_sem=sem.at[k + 1],
                device_id={"tp": lax.rem(t + d, T)}, device_id_type=MESH).start()

    def share(index_, tile):
        stat[index_, 0] = tile.T[:8, :]
        to_peers(stat.at[index_], s_sem, 2 * index_)

    def normalize(layer, held, into, start, size_):
        def squares(j, total):
            part = xg[held, j, start:start + size_, :].astype(f32)
            return total + jnp.sum(part * part, axis=1, keepdims=True)
        mean = lax.fori_loop(0, T, squares, jnp.zeros((size_, 1), f32)) / D
        scale = lax.rsqrt(mean + 1e-06)

        def body(j, carry):
            by = gain[pl.ds(layer, 1), pl.ds(pl.multiple_of(j * width, width), width)]
            xn[into, j, start:start + size_, :] = (
                xg[held, j, start:start + size_, :].astype(f32) * scale * by).astype(bf16)
            return carry
        lax.fori_loop(0, T, body, 0)

    def project(layer, held, start, size_, into, h, part="whole"):
        def body(k, carry):
            j = lax.rem(far + 1 + k, T)
            block = wvg[layer, h, pl.ds(pl.multiple_of(j * width, width), width), :]
            term = jnp.dot(xn[held, j, start:start + size_, :], block, preferred_element_type=f32)

            @pl.when(k == 0)
            def _():
                acc[start:start + size_, :] = term

            @pl.when(k > 0)
            def _():
                acc[start:start + size_, :] += term
            return carry
        lax.fori_loop(T - 1 if part == "late" else 0, T - 1 if part == "early" else T, body, 0)
        if part != "early":
            glu = acc[start:start + size_, :half] * jax.nn.sigmoid(acc[start:start + size_, half:])
            into[start:start + size_, pl.ds(pl.multiple_of(h * half, half), half)] = glu.astype(bf16)

    def x_right(layer):
        return pltpu.make_async_remote_copy(
            src_ref=xg.at[layer, t, pl.ds(rows, PAD)], dst_ref=xg.at[layer, t, pl.ds(0, PAD)],
            send_sem=h_sem.at[layer, 0], recv_sem=h_sem.at[layer, 2],
            device_id={"sp": s + 1}, device_id_type=MESH)

    def x_left(layer):
        return pltpu.make_async_remote_copy(
            src_ref=xg.at[layer, t, pl.ds(PAD, PAD)], dst_ref=xg.at[layer, t, pl.ds(PAD + rows, PAD)],
            send_sem=h_sem.at[layer, 1], recv_sem=h_sem.at[layer, 3],
            device_id={"sp": s - 1}, device_id_type=MESH)

    def sides_of(layer):
        if layer == 0:
            return s == 1, s == last - 1, s == last - 1, s == 1
        return s < last, s > 0, s > 0, s < last

    def halo(layer, do):
        sends_right, sends_left, from_left, from_right = sides_of(layer)
        if do == "send":
            pl.when(sends_right)(lambda: x_right(layer).start())
            pl.when(sends_left)(lambda: x_left(layer).start())
        elif do == "begin":
            @pl.when(from_left)
            def _():
                wait_bytes(xg.at[layer, t, pl.ds(0, PAD)], h_sem.at[layer, 2])
                halo_spread(layer, 0).begin()

            @pl.when(from_right)
            def _():
                wait_bytes(xg.at[layer, t, pl.ds(0, PAD)], h_sem.at[layer, 3])
                halo_spread(layer, 1).begin()
        elif do == "drain":
            @pl.when(sends_right)
            def _():
                wait_bytes(xg.at[layer, t, pl.ds(0, PAD)], h_sem.at[layer, 0])

            @pl.when(sends_left)
            def _():
                wait_bytes(xg.at[layer, t, pl.ds(0, PAD)], h_sem.at[layer, 1])
            pl.when(from_left)(lambda: halo_spread(layer, 0).drain())
            pl.when(from_right)(lambda: halo_spread(layer, 1).drain())
        else:
            pl.when(from_left)(lambda: getattr(halo_spread(layer, 0), do)())
            pl.when(from_right)(lambda: getattr(halo_spread(layer, 1), do)())

    def channels_of(h):
        return pl.ds(pl.multiple_of(h * half, half), half)

    def convolve(layer, h, turn):
        @pl.when(s >= 0)
        def _():
            rows_of(layer, h, turn)
        if turn == G - 1:
            share(layer, column[...])
        conv_spread(layer, turn).begin()

    def rows_of(layer, h, turn):
        cols = channels_of(h)
        padf[...] = pad[layer, :, cols].astype(f32)
        block = 64
        for r in range(0, rows, block):
            total = jnp.zeros((block, half), f32)
            for k in range(n_taps):
                start = r + PAD - reach + k
                total = total + taps[k, layer:layer + 1, cols] * padf[start:start + block, :]
            mean = jnp.sum(total, axis=1, keepdims=True) / half
            shifted = total - mean
            convg[layer, t, r:r + block, cols] = shifted.astype(bf16)
            lane = lax.broadcasted_iota(jnp.int32, (block, 128), 1)
            before = column[r:r + block, :] if turn else jnp.zeros((block, 128), f32)
            squares = jnp.sum(shifted * shifted, axis=1, keepdims=True)
            column[r:r + block, :] = jnp.where(lane == 2 * h, mean, jnp.where(lane == 2 * h + 1, squares, before))

    def activate(layer):
        wait_bytes(stat.at[layer, pl.ds(0, T - 1)], s_sem.at[2 * layer + 1])
        got = [stat[layer, d] for d in range(T)]
        pairs = [(rows_[2 * h:2 * h + 1, :], rows_[2 * h + 1:2 * h + 2, :]) for rows_ in got for h in range(G)]
        center = sum((m for m, _ in pairs[1:]), pairs[0][0]) / (T * G)
        away = [m - center for m, _ in pairs]
        square = jnp.zeros((1, rows), f32)
        for a, (_, sq) in zip(away, pairs):
            square = square + (sq + half * (a * a))
        lines = away + [lax.rsqrt(square / C + 1e-05)]
        table = jnp.concatenate(lines + [jnp.zeros((128 - len(lines), rows), f32)], axis=0).T
        scale = table[:, T * G:T * G + 1]
        for d in range(T):
            j = lax.rem(t + T - d, T)
            by = cgain[j, layer:layer + 1, :]
            apart = jnp.concatenate(
                [jnp.broadcast_to(table[:, i:i + 1], (rows, half)) for i in range(G * d, G * (d + 1))], axis=1)
            normal = (convg[layer, j].astype(f32) + apart) * scale
            act[j] = jax.nn.silu(normal * by).astype(bf16)

    def add_branch(layer, h):
        part = None
        for j in range(T):
            term = jnp.dot(act[j], wo[layer, h, j * chans:(j + 1) * chans, :], preferred_element_type=f32)
            part = term if part is None else part + term
        cols = half_columns(h)
        x_state[:, cols] = (x_state[:, cols] + part).astype(bf16).astype(f32)

    with scope("stage_wait"):
        staged(first_vg)
    token_copy.wait()
    halo(0, "send")
    each(0, QC, lambda q: inward(first_vg, q, s).start())

    @pl.when(is_end)
    def _():
        each(0, x_chunks, lambda c: end_rows(c, inner).start())

    @pl.when(is_mid)
    def _():
        x_spread().begin()

    with scope("stage_wait2"):
        for stage in after:
            staged(stage)

    def end_sends(what, stage, lo, hi):
        @pl.when(is_end)
        def _():
            if what == "in":
                each(lo, hi, lambda q: inward(stage, q, edge).start())
            else:
                each(lo, hi, lambda q: direct(stage, q).start())

    end_sends("direct", first_vg, 0, shared_from)

    @pl.when(is_mid)
    def _():
        for stage in after:
            each(0, count[stage[1]], lambda q: outward(stage, q, mine).start())

    gain_copy.wait()
    for c in small:
        c.wait()
    for d in range(1, T):
        pltpu.make_async_remote_copy(
            src_ref=cgain.at[t], dst_ref=cgain.at[t], send_sem=g_sem.at[0], recv_sem=g_sem.at[1],
            device_id={"tp": lax.rem(t + d, T)}, device_id_type=MESH).start()
    x_state[...] = xg[0, t, own, :].astype(f32)
    with scope("halo0_begin"):
        halo(0, "begin")

    def first_chunks(q):
        from_inner(first_vg, q, near)
        from_edge(first_vg, q)
    with scope("A_vg0_near_edge"):
        each(0, QC, first_chunks)
    push_in(first_wo, 0, RC)
    push_in(second_vg, 0, QC // 2)

    @pl.when(is_end)
    def _():
        def pass_on(stage):
            def body(q):
                arrived(stage, q, mine)
                across(stage, q, mine).start()
            each(0, count[stage[1]], body)
        for stage in after:
            with scope("end_pass_on"):
                pass_on(stage)
            if stage == first_wo:
                end_sends("in", first_wo, 0, RC)
                end_sends("in", second_vg, 0, QC // 2)
            elif stage == second_vg:
                end_sends("direct", first_wo, 0, RC)

    def edge_relays(lo, hi):
        @pl.when(is_mid)
        def _():
            with scope("edge_relay"):
                each(lo, hi, lambda c: edge_spread(c).relay())

    halo(0, "relay")

    @pl.when(is_mid)
    def _():
        with scope("x0_finish"):
            x_spread().relay()
            x_spread().complete()
    halo(0, "complete")

    @pl.when(is_mid)
    def _():
        with scope("norm0"):
            normalize(0, 0, 0, 0, full)

    def second_chunks(q):
        each(q * QC // x_chunks, (q + 1) * QC // x_chunks, lambda k: from_inner(first_vg, k, far))

        @pl.when(is_mid)
        def _():
            wait_bytes(xg.at[0, t, pl.ds(0, x_rows)], f_sem.at[2 + q])
            edge_spread(q).begin()
    with scope("B_vg0_far"):
        each(0, x_chunks, second_chunks)

    @pl.when(is_mid)
    def _():
        with scope("proj0_g"):
            project(0, 0, 0, full, pad.at[0], g)
    edge_relays(0, x_chunks // 2)
    with scope("C1_wo0_near"):
        each(0, RC // 2, lambda q: from_inner(first_wo, q, near))
    edge_relays(x_chunks // 2, x_chunks - 1)
    with scope("C1_wo0_near"):
        each(RC // 2, RC, lambda q: from_inner(first_wo, q, near))
    edge_relays(x_chunks - 1, x_chunks)
    push_in(second_vg, QC // 2, 3 * QC // 4)
    end_sends("in", second_vg, QC // 2, QC)

    @pl.when(is_mid)
    def _():
        with scope("edge_complete"):
            each(0, x_chunks, lambda c: edge_spread(c).complete())
        with scope("norm_e"):
            normalize(0, L, 1, PAD, rows)
    with scope("D1_vg1_near"):
        each(0 * QC // 4, (0 + 1) * QC // 4, lambda q: from_inner(second_vg, q, near))

    @pl.when(is_mid)
    def _():
        with scope("proj0e_g"):
            project(0, 1, PAD, rows, glu_out, g)

    @pl.when(is_mid)
    def _():
        with scope("wait_vg0"):
            others_arrived(first_vg)
        with scope("proj0e"):
            project(0, 1, PAD, rows, glu_out, other)
    with scope("C2_wo0_edge"):
        each(0, RC // 2, lambda q: from_edge(first_wo, q))
    with scope("D1_vg1_near"):
        each(QC // 4, QC // 2, lambda q: from_inner(second_vg, q, near))

    @pl.when(is_mid)
    def _():
        with scope("proj0"):
            project(0, 0, 0, full, pad.at[0], other)

    sends_right, sends_left, _, _ = sides_of(0)

    @pl.when(sends_right)
    def _():
        glu_out[0:PAD, :] = jnp.zeros((PAD, chans), bf16)
        glu_out[PAD + rows:, :] = pad[0, PAD:2 * PAD, :]
        pad[0, 0:PAD, :] = glu_out[rows:rows + PAD, :]

    @pl.when(sends_left)
    def _():
        glu_out[0:PAD, :] = pad[0, rows:rows + PAD, :]
        glu_out[PAD + rows:, :] = jnp.zeros((PAD, chans), bf16)
        pad[0, PAD + rows:, :] = glu_out[PAD:2 * PAD, :]

    @pl.when(is_mid)
    def _():
        end_glu(edge).start()

    with scope("C2_wo0_edge"):
        each(RC // 2, RC, lambda q: from_edge(first_wo, q))
    push_in(second_vg, 3 * QC // 4, QC)
    end_sends("in", second_wo, 0, RC)

    @pl.when(is_end)
    def _():
        with scope("end_glu_wait"):
            wait_bytes(glu_out, f_sem.at[2 + x_chunks])

    with scope("conv0"):
        convolve(0, g, 0)
        convolve(0, other, 1)
    with scope("D2_vg1_edge"):
        each(0 * QC // 4, (0 + 1) * QC // 4, lambda q: from_edge(second_vg, q))
    with scope("C3_wo0_far"):
        each(0, RC // 2, lambda q: from_inner(first_wo, q, far))
    with scope("conv0_relay"):
        conv_spread(0, 0).relay()
    with scope("C3_wo0_far"):
        pl.when(is_end)(lambda: each(RC // 2, RC, lambda q: from_inner(first_wo, q, far)))
    with scope("conv0_relay"):
        conv_spread(0, 1).relay()
    with scope("C3_wo0_far"):
        pl.when(is_mid)(lambda: each(RC // 2, RC, lambda q: from_inner(first_wo, q, far)))
    with scope("conv0_complete"):
        conv_spread(0, 0).complete()
        conv_spread(0, 1).complete()
        wait_bytes(cgain.at[pl.ds(0, T - 1)], g_sem.at[1])
    with scope("act0"):
        activate(0)
    with scope("D2_vg1_edge"):
        each(1 * QC // 4, (1 + 1) * QC // 4, lambda q: from_edge(second_vg, q))
    push_in(second_wo, 0, RC // 2)

    def next_x(h, turn):
        add_branch(0, h)
        cols = half_columns(h)
        xg[1, t, own, cols] = x_state[:, cols].astype(bf16)
        half_spread(h, turn).begin()
    with scope("out0_g"):
        next_x(g, 0)
    with scope("D2_vg1_near"):
        each(QC // 2, 3 * QC // 4, lambda q: from_inner(second_vg, q, near))
    with scope("wait_wo0"):
        others_arrived(first_wo)
    with scope("out0"):
        next_x(other, 1)
    halo(1, "send")
    end_sends("direct", second_vg, 0, QC)
    end_sends("direct", second_wo, 0, RC)
    with scope("D3_vg1_near"):
        each(3 * QC // 4, QC, lambda q: from_inner(second_vg, q, near))
    with scope("D3_vg1_edge"):
        each(2 * QC // 4, (2 + 1) * QC // 4, lambda q: from_edge(second_vg, q))
    with scope("D4_vg1_far"):
        each(0 * QC // 4, (0 + 1) * QC // 4, lambda q: from_inner(second_vg, q, far))
    with scope("D3_vg1_edge"):
        each(3 * QC // 4, QC, lambda q: from_edge(second_vg, q))
    push_in(second_wo, RC // 2, RC)
    with scope("D4_vg1_far"):
        each(1 * QC // 4, (1 + 1) * QC // 4, lambda q: from_inner(second_vg, q, far))
    with scope("x1_relay"):
        half_spread(g, 0).relay()
    with scope("E1_near"):
        each(0, RC // 2, lambda q: from_inner(second_wo, q, near))
    with scope("halo1_begin"):
        pl.when(is_end)(lambda: halo(1, "begin"))
    with scope("D4_vg1_far"):
        each(2 * QC // 4, (2 + 1) * QC // 4, lambda q: from_inner(second_vg, q, far))
    with scope("x1_relay"):
        pl.when(is_end)(half_spread(other, 1).relay)
    with scope("halo1_relay"):
        pl.when(is_end)(lambda: halo(1, "relay"))
    with scope("E1_wo1_edge"):
        each(0, RC // 2, lambda q: from_edge(second_wo, q))
    with scope("D4_vg1_far"):
        pl.when(is_mid)(lambda: each(3 * QC // 4, QC, lambda q: from_inner(second_vg, q, far)))
    with scope("E1_wo1_edge"):
        each(RC // 2, RC, lambda q: from_edge(second_wo, q))
    with scope("halo1_begin"):
        pl.when(is_mid)(lambda: halo(1, "begin"))
    with scope("x1_relay"):
        pl.when(is_mid)(half_spread(other, 1).relay)
    with scope("E1_near"):
        pl.when(is_mid)(lambda: each(RC // 2, RC, lambda q: from_inner(second_wo, q, near)))
    with scope("halo1_relay"):
        pl.when(is_mid)(lambda: halo(1, "relay"))
    with scope("x1_complete"):
        half_spread(g, 0).complete()
        half_spread(other, 1).complete()
        halo(1, "complete")
    with scope("norm1"):
        normalize(1, 1, 0, 0, full)
    with scope("D4_vg1_far"):
        pl.when(is_end)(lambda: each(3 * QC // 4, QC, lambda q: from_inner(second_vg, q, far)))
    with scope("E2_m"):
        pl.when(is_mid)(lambda: each(0, RC // 2, lambda q: from_inner(second_wo, q, far)))
    with scope("proj1_g"):
        project(1, 0, 0, full, pad.at[1], g)
    with scope("conv1_g"):
        convolve(1, g, 0)
    with scope("E2_m"):
        pl.when(is_mid)(lambda: each(RC // 2, RC, lambda q: from_inner(second_wo, q, far)))
    with scope("E1_e"):
        pl.when(is_end)(lambda: each(RC // 2, 3 * RC // 4, lambda q: from_inner(second_wo, q, near)))
    with scope("wait_vg1"):
        others_arrived(second_vg)
    with scope("proj1"):
        project(1, 0, 0, full, pad.at[1], other, "early")
    with scope("E1_e"):
        pl.when(is_end)(lambda: each(3 * RC // 4, RC, lambda q: from_inner(second_wo, q, near)))
    def far_chunk(k):
        with scope("E2_e"):
            pl.when(is_end)(lambda: each(k * RC // 4, (k + 1) * RC // 4, lambda q: from_inner(second_wo, q, far)))
    far_chunk(0)
    with scope("wait_vg1_far"):
        far_arrived()
    far_chunk(1)
    with scope("proj1_far"):
        project(1, 0, 0, full, pad.at[1], other, "late")
    with scope("conv1"):
        convolve(1, other, 1)
    far_chunk(2)
    far_chunk(3)
    with scope("conv1_relay"):
        conv_spread(1, 0).relay()
    with scope("conv1_relay"):
        conv_spread(1, 1).relay()
    with scope("conv1_gather"):
        conv_spread(1, 0).complete()
        conv_spread(1, 1).complete()
    with scope("act1"):
        activate(1)

    def last_x(h, turn):
        add_branch(1, h)
        cols = half_columns(h)
        xf = x_state[:, cols]
        leaving[:, cols] = xf.astype(bf16)
        pltpu.make_async_copy(leaving.at[:, cols], x_out.at[:, cols], o_sem.at[turn]).start()
        squares = jnp.broadcast_to(jnp.sum(xf * xf, axis=1, keepdims=True), (rows, 128))
        if turn < G - 1:
            column[...] = squares
        else:
            share(L, column[...] + squares)
    with scope("out1_g"):
        last_x(g, 0)
    with scope("wait_wo1"):
        others_arrived(second_wo)
    with scope("out1"):
        last_x(other, 1)

    halo(0, "drain")
    halo(1, "drain")
    for layer in range(L):
        for part_ in range(2):
            conv_spread(layer, part_).drain()
    half_spread(g, 0).drain()
    half_spread(other, 1).drain()
    wait_bytes(cgain.at[pl.ds(0, T - 1)], g_sem.at[0])
    whole = L * (depth + out_rows * out_half // (2 * half))
    later = whole - depth

    def sent(length, k):
        wait_bytes(wvg.at[0, 0, pl.ds(0, length)], send_w.at[k])

    def sent_twice(length, k):
        wait_bytes(wvg.at[0, :, pl.ds(0, length)], send_w.at[k])

    def sent_all(k):
        sent_twice(later * (n - 1) // G, k)

    @pl.when(is_mid)
    def _():
        x_spread().drain()
        each(0, x_chunks, lambda c: edge_spread(c).drain())
        wait_bytes(glu_out, f_sem.at[1])
        sent_twice(whole, IN)
        sent_twice(3 * later // 2, OUT)
        sent((QC - shared_from) * size["vg"], YE)
        sent_twice(whole, Y)

    @pl.when(is_end)
    def _():
        wait_bytes(xg.at[0, t, own], f_sem.at[0])
        sent(whole, IN)
        sent(later + shared_from * size["vg"], UN)
        sent_twice(3 * later // 2, Y)

    with scope("final_stat"):
        wait_bytes(stat.at[L, pl.ds(0, T - 1)], s_sem.at[2 * L + 1])
        for index_ in range(L + 1):
            wait_bytes(stat.at[index_, pl.ds(0, T - 1)], s_sem.at[2 * index_])
    line = sum((stat[L, d, 0:1, :] for d in range(1, T)), stat[L, 0, 0:1, :])
    total = jnp.broadcast_to(line, (128, rows)).T[:, 0:1]
    scale_out[...] = lax.rsqrt(total / D + 1e-06)
    for turn in range(G):
        wait_bytes(leaving.at[:, pl.ds(0, out_half)], o_sem.at[turn])


def scale_rows(x, scale, gain, out):
    out[...] = (x[...].astype(jnp.float32) * scale[...] * gain[...]).astype(out.dtype)


def quad_on_device(G, n, T, tokens, norm_gain, value_w, gate_w, taps, cgain, out_w, fgain):
    L = norm_gain.shape[0]
    if L != 2:
        return on_device(G, n, T, tokens, norm_gain, value_w, gate_w, taps, cgain, out_w, fgain)
    rows, width = tokens.shape
    depth, chans = value_w.shape[1:]
    D, C = width * T, chans * T
    bf16, f32 = jnp.bfloat16, jnp.float32
    dma = pltpu.SemaphoreType.DMA
    vmem = pl.BlockSpec(memory_space=pltpu.VMEM)
    hbm = pl.BlockSpec(memory_space=pltpu.HBM)
    full = rows + 2 * PAD
    x, scale = pl.pallas_call(
        functools.partial(quad_kernel, G, n, T, L),
        out_shape=(jax.ShapeDtypeStruct((rows, width), bf16), jax.ShapeDtypeStruct((rows, 1), f32)),
        in_specs=[hbm] * 7,
        out_specs=(pl.BlockSpec(memory_space=pl.ANY), vmem),
        scratch_shapes=[
            pltpu.VMEM((L, G, D, 2 * chans // G), bf16),
            pltpu.VMEM((L, G, C, width // G), bf16),
            pltpu.VMEM((L + 1, T, full, width), bf16),
            pltpu.VMEM((2, T, full, width), bf16),
            pltpu.VMEM((full, chans), bf16),
            pltpu.VMEM((full, 2 * chans // G), f32),
            pltpu.VMEM((L, full, chans), bf16),
            pltpu.VMEM((full, chans // G), f32),
            pltpu.VMEM((L, T, rows, chans), bf16),
            pltpu.VMEM((T, rows, chans), bf16),
            pltpu.VMEM((rows, 128), f32),
            pltpu.VMEM((L + 1, T, 8, rows), f32),
            pltpu.VMEM((rows, width), f32),
            pltpu.VMEM((rows, width), bf16),
            pltpu.VMEM(norm_gain.shape, f32),
            pltpu.VMEM((taps.shape[1], L, chans), f32),
            pltpu.VMEM((T,) + cgain.shape, f32),
            dma((2 * L + 4,)),
            dma((L * (QC + RC), 3)), dma((2 * L + 1,)), dma((5,)),
            dma((1 + G, 3)), dma((XC, 3)), dma((L, 2, 3)), dma((2 * (L + 1),)),
            dma((L, 4)), dma((L, 2, 3)), dma((2,)), dma((XC + 3,)), dma((G,)),
        ],
        compiler_params=pltpu.CompilerParams(
            collective_id=0, has_side_effects=True, vmem_limit_bytes=56 * 2**20
        ),
    )(tokens, norm_gain, value_w, gate_w, taps.transpose(1, 0, 2), cgain, out_w)
    step = rows // EPILOGUE
    return pl.pallas_call(
        scale_rows,
        grid=(EPILOGUE,),
        out_shape=jax.ShapeDtypeStruct((rows, width), bf16),
        in_specs=[
            pl.BlockSpec((step, width), lambda i: (i, 0)),
            pl.BlockSpec((step, 1), lambda i: (i, 0)),
            pl.BlockSpec((1, width), lambda i: (0, 0)),
        ],
        out_specs=pl.BlockSpec((step, width), lambda i: (i, 0)),
        compiler_params=pltpu.CompilerParams(vmem_limit_bytes=60 * 2**20),
    )(x, scale, fgain.reshape(1, width))


def tokens_f32(tokens, xg, t):
    return xg[0, t].astype(jnp.float32)


def on_device(G, n, T, tokens, norm_gain, value_w, gate_w, taps, cgain, out_w, fgain):
    L = norm_gain.shape[0]
    rows, width = tokens.shape
    depth, chans = value_w.shape[1:]
    D, C = width * T, chans * T
    bf16, f32 = jnp.bfloat16, jnp.float32
    dma = pltpu.SemaphoreType.DMA
    vmem = pl.BlockSpec(memory_space=pltpu.VMEM)
    hbm = pl.BlockSpec(memory_space=pl.ANY)
    P_ = L * (Q + 1)
    peers = max(G - 1, 1)
    return pl.pallas_call(
        functools.partial(kernel, G, n, T, L),
        out_shape=jax.ShapeDtypeStruct((rows, width), bf16),
        in_specs=[hbm, vmem, hbm, hbm, vmem, vmem, hbm, vmem],
        out_specs=vmem,
        scratch_shapes=[
            pltpu.VMEM((L, G, D, 2 * chans // G), bf16),
            pltpu.VMEM((L, G, C, width // G), bf16),
            pltpu.VMEM((L + 1, T, rows, width), bf16),
            pltpu.VMEM((2, T, rows, width), bf16),
            pltpu.VMEM((rows, chans), bf16),
            pltpu.VMEM((rows, 2 * chans // G), f32),
            pltpu.VMEM((L, rows + 2 * PAD, chans), bf16),
            pltpu.VMEM((rows + 2 * PAD, chans), f32),
            pltpu.VMEM((rows, chans), f32),
            pltpu.VMEM((L + 1, T, 8, rows), f32),
            pltpu.VMEM((L, T, rows, chans), bf16),
            pltpu.VMEM((rows, width), f32),
            dma((1 + L * G * 3,)),
            dma((P_, n)), dma((P_, n)), dma((P_, n)),
            dma((P_, n, peers)), dma((P_, n, peers)),
            dma((L + 1, T)), dma((L + 1, T)), dma((L, T)), dma((L, T)),
            dma((L + 1, T)), dma((L + 1, T)),
            dma((L, 2)), dma((L, 2)),
            dma((G + 1,)), dma((G + 1,)),
        ],
        compiler_params=pltpu.CompilerParams(
            collective_id=0, has_side_effects=True, vmem_limit_bytes=56 * 2**20
        ),
    )(tokens, norm_gain.reshape(L * T, width), value_w, gate_w, taps, cgain, out_w, fgain.reshape(1, width))


def solution(mesh):
    placed = (
        P(("grp", "sp"), "tp"),
        P(),
        P(None, "sp", "tp"),
        P(None, "sp", "tp"),
        P(None, None, "tp"),
        P(None, "tp"),
        P(None, "sp", "tp"),
        P("tp"),
    )
    G, n, T = (mesh.shape[a] for a in ("grp", "sp", "tp"))
    paired = G == 2 and n == T == 2 * G
    return jax.shard_map(
        functools.partial(quad_on_device if paired else on_device, G, n, T),
        mesh=mesh, in_specs=placed, out_specs=P(("grp", "sp"), "tp"), check_vma=False,
    )
```
